256 devices in a mesh: ep: 64 (over z, y, core), tp: 4 (over x).
Axes of the slice: x: 4, y: 4, z: 8, core: 2. Of those that a mesh axis runs over, the one named last changes fastest.
Arguments:
- queries: bfloat16 [12288, 2048], P('ep', 'tp'), may hold values from -5 to 5
- keys: bfloat16 [12288, 512], P('ep', 'tp'), may hold values from -5 to 5
- values: bfloat16 [12288, 512], P('ep', 'tp'), may hold values from -6 to 6
- query_gain: float32 [128], replicated, may hold values from 0.6 to 6
- key_gain: float32 [128], replicated, may hold values from 0.6 to 6
- out_weight: bfloat16 [2048, 2048], P('tp'), may hold values from -0.125 to 0.125
- mixer_gain: float32 [2048], replicated, may hold values from 0.1 to 1.9
- expert_in: bfloat16 [32768, 2048], P(('ep', 'tp')), may hold values from -6 to 6
- routes: int32 [32768, 2], P(('ep', 'tp')), may hold values from 0 to 63, all different within a row; in each aligned block of 128 rows (0 to 127, 128 to 255, ...) at most 6 rows name the same one
- route_weights: float32 [32768, 2], P(('ep', 'tp')), may hold values from 0.2 to 1
- expert_gain: float32 [2048], replicated, may hold values from 0.5 to 4
- gate_w: bfloat16 [64, 2048, 2048], P('ep', None, 'tp'), may hold values from -0.125 to 0.125
- up_w: bfloat16 [64, 2048, 2048], P('ep', None, 'tp'), may hold values from -0.125 to 0.125
- down_w: bfloat16 [64, 2048, 2048], P('ep', 'tp'), may hold values from -0.125 to 0.125
- ffn_out_gain: float32 [2048], replicated, may hold values from 0.1 to 1.9
Outputs:
- mixer_out: bfloat16 [12288, 2048], P(('ep', 'tp'))
- expert_out: bfloat16 [32768, 2048], P(('ep', 'tp'))
The draws below stay inside these ranges and needn't reach their ends.
Inputs may be any that keep to these rules, and one draw needn't show every extreme that they name: `routes`: each row names 2 different experts. Among the rows of one device no expert is named by more than 6 rows, and in every draw some expert is named by exactly 6 rows of some device.
All inputs are finite; a program needn't handle non-finite values.
Results may differ from the reference program's by a relative error of at most 0.015.
The reference program's roundings to bfloat16 on the way count: a program that leaves them out, or rounds other values in their place, can miss the bound.
Values may be sent and summed in bfloat16 or wider, within the bound.
A program may use at most 128 MiB of HBM per device.

```python
import math
import jax
import jax.numpy as jnp
import numpy as np
from jax import lax

D = 2048
HEADS = 16
KV_HEADS = 4
HEAD = 128
QW = 2048
KVW = 512
GRID_W = 64
LEN = 12288
FF = 2048
TOPK = 2
TB_DEV = 128
EXPERTS = 64
CAP = 6
TOKB = 32768
N_EP = 64
N_TP = 4


def plant_pairs(key):
    base_key = jax.random.fold_in(key, 7)
    key_part = jnp.clip(jax.random.normal(jax.random.fold_in(base_key, 1), (LEN, KVW), jnp.float32), -5.0, 5.0)
    query_part = jnp.clip(jax.random.normal(jax.random.fold_in(base_key, 2), (LEN, QW), jnp.float32), -5.0, 5.0)
    return (query_part, key_part)


def draw_queries(key, part):
    return plant_pairs(key)[0].astype(jnp.bfloat16)


def draw_keys(key, part):
    return plant_pairs(key)[1].astype(jnp.bfloat16)


def pair_gain(key, salt):
    base_key = jax.random.fold_in(key, salt)
    return jax.random.uniform(base_key, (HEAD,), jnp.float32, 0.6, 1.4)


def draw_query_gain(key, part):
    return pair_gain(key, 11)


def draw_key_gain(key, part):
    return pair_gain(key, 12)


def steps_of(key, shape, shards, least, top_value):
    def one(dim, blocks):
        heights = jax.random.uniform(jax.random.fold_in(jax.random.fold_in(key, 6), dim), (blocks,), jnp.float32, least / len(shards), top_value / len(shards))
        return jnp.repeat(jnp.exp(heights), shape[dim] // blocks).reshape((-1,) + (1,) * (len(shape) - dim - 1))

    level = one(*shards[0])
    for cut in shards[1:]:
        level = level * one(*cut)
    return level


def routed_block(stream_key, own, number, rows, number_of, top, most, slope):
    order = jax.random.permutation(stream_key, number_of)
    heavy_load, ordinary = shares(number_of, rows * top, most, slope, True), shares(number_of, rows * top, most, slope, False)
    places = jnp.arange(number_of)

    def named(tallies, turn):
        used = int((tallies > 0).sum())
        fixed = max(1, used // 4)
        shifted = fixed + (places - fixed + turn * (used - fixed)) % max(1, number_of - fixed)
        return jnp.zeros((number_of,), jnp.int32).at[order[jnp.where(places < fixed, places, shifted)]].set(jnp.asarray(tallies, jnp.int32))

    tallies = jnp.where(number % 4 == 0, named(heavy_load, number // 4), named(ordinary, number - number // 4 - 1))
    mixed = jax.random.permutation(jax.random.fold_in(own, 3), number_of)
    source_of, receiver = mixed[0:number_of // 2 * 2:2], mixed[1:number_of // 2 * 2:2]
    slack = jnp.minimum(tallies[source_of] - 1, most - tallies[receiver]) // 2
    slack = jnp.where((source_of == order[0]) | (receiver == order[0]) | (tallies[receiver] == 0), 0, jnp.maximum(slack, 0))
    shifted = jax.random.randint(jax.random.fold_in(own, 4), (number_of // 2,), 0, 1 << 20) % (slack + 1)
    tallies = tallies.at[source_of].add(-shifted).at[receiver].add(shifted)
    labels = jnp.searchsorted(jnp.cumsum(tallies), jnp.arange(rows * top), side="right").astype(jnp.int32)
    table = labels.reshape(top, rows).T
    table = table[jax.random.permutation(jax.random.fold_in(own, 1), rows)]
    turn = jax.random.randint(jax.random.fold_in(own, 2), (rows, 1), 0, top)
    return jnp.take_along_axis(table, (jnp.arange(top)[None, :] + turn) % top, axis=1)


def shares(number_of, total, most, lean, full):
    loads = [(1 << 20) // math.isqrt(standing ** lean) + 1 for standing in range(1, number_of + 1)]
    largest = most if full else min(most, max(-(-total // number_of), total * loads[0] // sum(loads)))
    least = 1 if total - largest >= number_of - 1 else 0
    given, spare = [largest] + [least] * (number_of - 1), total - largest - least * (number_of - 1)
    while spare > 0:
        movable = [i for i in range(1, number_of) if given[i] < largest] or [i for i in range(1, number_of) if given[i] < most]
        mass, left = sum([loads[i] for i in movable]), spare
        for i in movable:
            more = min(most - given[i], max(1, left * loads[i] // mass), spare)
            given[i] = given[i] + more
            spare = spare - more
    return np.array(given)


def scatter_about(key, shape, scale, reach, cuts=(), kind=jnp.bfloat16):
    entries = scale * jax.random.normal(key, shape, jnp.float32)
    if cuts:
        entries = entries * steps_of(key, shape, cuts, -0.22, 0.18)
    return jnp.clip(entries, -reach, reach).astype(kind)


def setup_inputs(seed: int = 0) -> dict:
    seeds = jax.random.split(jax.random.key(seed), 16)
    queries = draw_queries(jax.random.fold_in(seeds[15], 71), 0)
    keys = draw_keys(jax.random.fold_in(seeds[15], 71), 0)
    values = scatter_about(seeds[2], (LEN, KVW), 1.0, 6.0, ((0, 64), (1, 4)))
    query_gain = draw_query_gain(jax.random.fold_in(seeds[15], 71), 0)
    key_gain = draw_key_gain(jax.random.fold_in(seeds[15], 71), 0)
    out_weight = scatter_about(seeds[5], (QW, D), QW ** -0.5, 0.125, ((0, 4),))
    mixer_gain = jnp.clip(1.0 + 0.18 * jax.random.normal(seeds[6], (D,), jnp.float32), 0.1, 1.9)
    expert_in = scatter_about(seeds[7], (TOKB, D), 1.0, 6.0, ((0, 256),))
    routes_keys = jax.random.split(jax.random.fold_in(seeds[8], 1), TOKB // TB_DEV)
    routes_turns = jax.random.permutation(jax.random.fold_in(seeds[8], 3), TOKB // TB_DEV)
    routes = jax.vmap(lambda own, number: routed_block(jax.random.fold_in(seeds[8], 2), own, number, TB_DEV, EXPERTS, TOPK, CAP, 1))(routes_keys, routes_turns).reshape((TOKB, TOPK))
    route_weights = jnp.clip(0.2 + 0.8 * jax.random.uniform(seeds[9], (TOKB, TOPK), jnp.float32) ** steps_of(seeds[9], (TOKB, TOPK), ((0, 256),), -0.2, 0.2), 0.2, 1.0)
    expert_gain = jnp.clip(jnp.exp(jax.random.uniform(seeds[10], (D,), jnp.float32, math.log(0.5), math.log(4.0))), 0.5, 4.0)
    gate_w = scatter_about(seeds[11], (EXPERTS, D, FF), D ** -0.5, 0.125, ((0, 64), (2, 4)))
    up_w = scatter_about(seeds[12], (EXPERTS, D, FF), D ** -0.5, 0.125, ((0, 64), (2, 4)))
    down_w = scatter_about(seeds[13], (EXPERTS, FF, D), FF ** -0.5, 0.125, ((0, 64), (1, 4)))
    ffn_out_gain = jnp.clip(1.0 + 0.18 * jax.random.normal(seeds[14], (D,), jnp.float32), 0.1, 1.9)
    return {"queries": queries, "keys": keys, "values": values, "query_gain": query_gain, "key_gain": key_gain, "out_weight": out_weight, "mixer_gain": mixer_gain, "expert_in": expert_in, "routes": routes, "route_weights": route_weights, "expert_gain": expert_gain, "gate_w": gate_w, "up_w": up_w, "down_w": down_w, "ffn_out_gain": ffn_out_gain}


norm_eps = 1e-06
rope_base = 10000.0
clamp_limit = 7.0
sigmoid_slope = 1.702

def rms_scale(values_in, gain):
    return values_in * lax.rsqrt(lax.optimization_barrier(jnp.mean(values_in * values_in, axis=-1, keepdims=True)) + norm_eps) * gain

def turn_pair(halfpart, cosine, sine):
    first_part, second_part = jnp.split(halfpart, 2, axis=-1)
    return jnp.concatenate([first_part * cosine - second_part * sine, second_part * cosine + first_part * sine], axis=-1)

def grid_rotate(field, position):
    half_width = field.shape[-1] // 2
    inverse = rope_base ** (-jnp.arange(0, half_width, 2, dtype=jnp.float32) / half_width)
    grid_row = (position // GRID_W).astype(jnp.float32)
    grid_col = (position % GRID_W).astype(jnp.float32)
    row_angle = (grid_row[:, None] * inverse[None, :])[:, None, :]
    col_angle = (grid_col[:, None] * inverse[None, :])[:, None, :]
    return jnp.concatenate([turn_pair(field[..., :half_width], jnp.cos(row_angle), jnp.sin(row_angle)), turn_pair(field[..., half_width:], jnp.cos(col_angle), jnp.sin(col_angle))], axis=-1)

def clamped_unit(gate_pre, up_pre):
    gate_cut = jnp.minimum(gate_pre, clamp_limit)
    up_cut = jnp.clip(up_pre, -clamp_limit, clamp_limit)
    return ((up_cut + 1.0) * gate_cut * jax.nn.sigmoid(sigmoid_slope * gate_cut)).astype(jnp.bfloat16)

def reference(queries, keys, values, query_gain, key_gain, out_weight, mixer_gain, expert_in, routes, route_weights, expert_gain, gate_w, up_w, down_w, ffn_out_gain):
    group_size = HEADS // KV_HEADS
    position = jnp.arange(LEN, dtype=jnp.int32)
    query_norm = grid_rotate(rms_scale(queries.astype(jnp.float32).reshape(LEN, HEADS, HEAD), query_gain), position).astype(jnp.bfloat16)
    key_norm = grid_rotate(rms_scale(keys.astype(jnp.float32).reshape(LEN, KV_HEADS, HEAD), key_gain), position).astype(jnp.bfloat16)
    key_wide = key_norm.astype(jnp.float32)
    value_wide = values.reshape(LEN, KV_HEADS, HEAD).astype(jnp.float32)
    score_scale = HEAD ** (-0.5)
    query_blocks = query_norm.reshape(LEN // GRID_W, GRID_W, KV_HEADS, group_size, HEAD)

    def attend_block(block_in):
        scores = jnp.einsum('qhgd,khd->hgqk', block_in.astype(jnp.float32), key_wide) * score_scale
        expo = jnp.exp(scores - lax.optimization_barrier(jnp.max(scores, axis=-1, keepdims=True)))
        total = lax.optimization_barrier(jnp.sum(expo, axis=-1))
        probs = lax.optimization_barrier(expo.astype(jnp.bfloat16))
        summed = jnp.einsum('hgqk,khd->qhgd', probs.astype(jnp.float32), value_wide)
        return (summed / jnp.transpose(total, (2, 0, 1))[..., None]).astype(jnp.bfloat16)
    attended = lax.map(attend_block, query_blocks).reshape(LEN, HEADS * HEAD)
    column_span = HEADS * HEAD // N_TP
    projected = jnp.zeros((LEN, D), jnp.float32)
    for member in range(N_TP):
        partial_term = jnp.dot(attended[:, member * column_span:(member + 1) * column_span], out_weight[member * column_span:(member + 1) * column_span], preferred_element_type=jnp.float32).astype(jnp.bfloat16)
        projected = projected + lax.optimization_barrier(partial_term).astype(jnp.float32)
    mixer_out = rms_scale(projected, mixer_gain).astype(jnp.bfloat16)
    normed = rms_scale(expert_in.astype(jnp.float32), expert_gain).astype(jnp.bfloat16)
    padded = jnp.concatenate([normed, jnp.zeros((1, D), jnp.bfloat16)], axis=0)
    pair_expert = routes.reshape(-1)
    pair_count = pair_expert.shape[0]
    pair_weight = jnp.concatenate([route_weights.reshape(-1), jnp.zeros((1,), jnp.float32)], axis=0)
    most_rows = N_EP * N_TP * CAP
    hidden_span = FF // N_TP

    def one_expert(combined_in, expert_id):
        chosen = jnp.nonzero(pair_expert == expert_id, size=most_rows, fill_value=pair_count)[0].astype(jnp.int32)
        token_index = chosen // TOPK
        inputs = padded[token_index]
        hidden = clamped_unit(jnp.dot(inputs, gate_w[expert_id], preferred_element_type=jnp.float32), jnp.dot(inputs, up_w[expert_id], preferred_element_type=jnp.float32))
        down_here = down_w[expert_id]
        result = jnp.zeros((most_rows, D), jnp.float32)
        for member in range(N_TP):
            partial_term = jnp.dot(hidden[:, member * hidden_span:(member + 1) * hidden_span], down_here[member * hidden_span:(member + 1) * hidden_span], preferred_element_type=jnp.float32).astype(jnp.bfloat16)
            result = result + lax.optimization_barrier(partial_term).astype(jnp.float32)
        output_rows = lax.optimization_barrier(result.astype(jnp.bfloat16))
        combined_out = combined_in.at[token_index].add(pair_weight[chosen][:, None] * output_rows.astype(jnp.float32))
        return (combined_out, None)
    combined, unused = lax.scan(one_expert, jnp.zeros((TOKB + 1, D), jnp.float32), jnp.arange(EXPERTS, dtype=jnp.int32))
    expert_out = rms_scale(combined[:TOKB], ffn_out_gain).astype(jnp.bfloat16)
    return (mixer_out, expert_out)
```

```python
import functools

import jax
import jax.numpy as jnp
import numpy as np
from jax import lax
from jax.experimental import pallas as pl
from jax.experimental.pallas import tpu as pltpu
from jax.sharding import Mesh
from jax.sharding import PartitionSpec as P

HEAD = 128
GRID_W = 64
EP = ("ep_0", "ep_1", "ep_2")
EP_TP = ("ep_0", "ep_1", "ep_2", "tp")
MESH = pl.DeviceIdType.MESH
BF = jnp.bfloat16
F32 = jnp.float32

norm_eps = 1e-06
rope_base = 10000.0
clamp_limit = 7.0
sigmoid_slope = 1.702

PL = 8
CAP = 6
SUB = 8
ROWS = PL * CAP


def whole_of(array, axes, dim):
    if not axes:
        return array
    nearer = lax.all_gather(array, axes[-1], axis=dim, tiled=True)
    return whole_of(nearer, axes[:-1], dim)


def in_blocks(array, dim, peers):
    before, after = (array.shape[:dim], array.shape[dim + 1 :])
    return jnp.moveaxis(array.reshape(*before, peers, -1, *after), dim, 0)


def summed_on_arrival(array, axis, dim):
    blocks = in_blocks(array, dim, lax.axis_size(axis))
    arrived = lax.all_to_all(blocks, axis, split_axis=0, concat_axis=0, tiled=True)
    return arrived.astype(jnp.float32).sum(axis=0)


def rms_scale(values_in, gain):
    return (
        values_in
        * lax.rsqrt(jnp.mean(values_in * values_in, axis=-1, keepdims=True) + norm_eps)
        * gain
    )


def turn_pair(halfpart, cosine, sine):
    first_part, second_part = jnp.split(halfpart, 2, axis=-1)
    return jnp.concatenate(
        [first_part * cosine - second_part * sine, second_part * cosine + first_part * sine],
        axis=-1,
    )


def grid_rotate(field, position):
    half_width = field.shape[-1] // 2
    inverse = rope_base ** (-jnp.arange(0, half_width, 2, dtype=jnp.float32) / half_width)
    grid_row = (position // GRID_W).astype(jnp.float32)
    grid_col = (position % GRID_W).astype(jnp.float32)
    row_angle = (grid_row[:, None] * inverse[None, :])[:, None, :]
    col_angle = (grid_col[:, None] * inverse[None, :])[:, None, :]
    return jnp.concatenate(
        [
            turn_pair(field[..., :half_width], jnp.cos(row_angle), jnp.sin(row_angle)),
            turn_pair(field[..., half_width:], jnp.cos(col_angle), jnp.sin(col_angle)),
        ],
        axis=-1,
    )


def mixer_half(queries, keys, values, query_gain, key_gain, out_weight, mixer_gain):
    local_rows = queries.shape[0]
    kv_local = keys.shape[1] // HEAD
    group_size = queries.shape[1] // HEAD // kv_local
    position = lax.axis_index(EP) * local_rows + jnp.arange(local_rows, dtype=jnp.int32)
    query_f = queries.astype(jnp.float32).reshape(local_rows, kv_local * group_size, HEAD)
    query_norm = grid_rotate(rms_scale(query_f, query_gain), position).astype(jnp.bfloat16)
    query_norm = query_norm.reshape(local_rows, kv_local, group_size, HEAD)
    key_f = keys.astype(jnp.float32).reshape(local_rows, kv_local, HEAD)
    key_norm = grid_rotate(rms_scale(key_f, key_gain), position).astype(jnp.bfloat16)
    key_norm = key_norm.reshape(local_rows, kv_local * HEAD)
    score_scale = HEAD ** (-0.5)
    initial = (
        jnp.full((kv_local, group_size, local_rows), -1e30, jnp.float32),
        jnp.zeros((kv_local, group_size, local_rows), jnp.float32),
        jnp.zeros((kv_local, group_size, local_rows, HEAD), jnp.float32),
    )
    key_piece = whole_of(key_norm, ("ep_2", "ep_0", "ep_1"), 0)
    value_piece = whole_of(values, ("ep_2", "ep_0", "ep_1"), 0)
    piece_rows = key_piece.shape[0]
    block_rows = 1024
    key_blocks = key_piece.reshape(piece_rows // block_rows, block_rows, kv_local, HEAD)
    value_blocks = value_piece.reshape(piece_rows // block_rows, block_rows, kv_local, HEAD)

    def one_block(state, blocks_in):
        running_max, running_total, weighted = state
        key_block, value_block = blocks_in
        scores = (
            jnp.einsum("qhgd,khd->hgqk", query_norm, key_block, preferred_element_type=jnp.float32)
            * score_scale
        )
        new_max = jnp.maximum(running_max, jnp.max(scores, axis=-1))
        factor = jnp.exp(running_max - new_max)
        expo = jnp.exp(scores - new_max[..., None])
        new_total = running_total * factor + jnp.sum(expo, axis=-1)
        new_weighted = weighted * factor[..., None] + jnp.einsum(
            "hgqk,khd->hgqd",
            expo.astype(jnp.bfloat16),
            value_block,
            preferred_element_type=jnp.float32,
        )
        return ((new_max, new_total, new_weighted), None)

    state_out, unused = lax.scan(one_block, initial, (key_blocks, value_blocks))
    final_max, final_total, weighted = state_out
    attended = (weighted / final_total[..., None]).astype(jnp.bfloat16)
    attended = jnp.transpose(attended, (2, 0, 1, 3)).reshape(
        local_rows, kv_local * group_size * HEAD
    )
    projected = summed_on_arrival(
        jnp.dot(attended, out_weight, preferred_element_type=jnp.float32).astype(jnp.bfloat16),
        "tp",
        0,
    )
    return rms_scale(projected, mixer_gain).astype(jnp.bfloat16)


def dot(a, b):
    return jnp.dot(a, b, preferred_element_type=F32)


def one_hot(cond):
    return jnp.where(cond, 1.0, 0.0).astype(BF)


def experts_kernel(
    nz,
    x_ref,
    routes_ref,
    routes_t_ref,
    rw_ref,
    eg_ref,
    fg_ref,
    pin_ref,
    pout_ref,
    gate_hbm,
    up_hbm,
    down_hbm,
    out_ref,
    normed,
    outgoing,
    arr,
    xall,
    part,
    rs1,
    rs2,
    ret_out,
    ret_in,
    ret_rows,
    wgu,
    wd,
    combined,
    w_sem,
    d_send,
    d_recv,
    ag_send,
    ag_recv,
    rs_send,
    rs1_recv,
    rs2_recv,
    r_send,
    r_recv,
):
    z = lax.axis_index("ep_0")
    p_me = lax.axis_index("ep_1") * 2 + lax.axis_index("ep_2")
    x_me = lax.axis_index("tp")
    right = {"tp": lax.rem(x_me + 1, 4)}
    left = {"tp": lax.rem(x_me + 3, 4)}
    tok, width = x_ref.shape
    half = width // 2
    sub_w = width // SUB
    ff = wd.shape[0]
    n_exp = nz * PL

    def peer(zz, p):
        return {"ep_0": zz, "ep_1": p // 2, "ep_2": lax.rem(p, 2)}

    def away(i):
        return jnp.where(lax.rem(i, 2) == 1, (i + 1) // 2, -(i // 2))

    def plane(i):
        return lax.rem(z + away(i) + nz, nz)

    def mirror(i):
        other = jnp.where(lax.rem(i, 2) == 1, i + 1, i - 1)
        return jnp.where((i == 0) | (i == nz - 1), i, other)

    barrier = pltpu.get_barrier_semaphore()

    @pl.loop(1, n_exp)
    def _(j):
        to = lax.rem(z * PL + p_me + j, n_exp)
        pl.semaphore_signal(
            barrier, inc=1, device_id=peer(to // PL, lax.rem(to, PL)), device_id_type=MESH
        )

    pl.semaphore_signal(barrier, inc=1, device_id=left, device_id_type=MESH)
    pl.semaphore_signal(barrier, inc=1, device_id=right, device_id_type=MESH)

    w_copies = [
        pltpu.make_async_copy(gate_hbm.at[0], wgu.at[:, pl.ds(0, ff)], w_sem.at[0]),
        pltpu.make_async_copy(up_hbm.at[0], wgu.at[:, pl.ds(ff, ff)], w_sem.at[1]),
        pltpu.make_async_copy(down_hbm.at[0], wd, w_sem.at[2]),
    ]
    for copy in w_copies:
        copy.start()

    xf = x_ref[...].astype(F32)
    normed[...] = rms_scale(xf, eg_ref[...]).astype(BF)

    def base_of(e):
        o = (lax.shift_right_logical(e, 3) - z + nz) & (nz - 1)
        idx = jnp.where(o == 0, 0, jnp.where(o <= nz // 2, 2 * o - 1, 2 * (nz - o)))
        return idx * ROWS + (e & 7) * CAP

    e_rows = lax.broadcasted_iota(jnp.int32, (n_exp, tok), 0)
    t_a = lax.broadcasted_iota(jnp.int32, (tok, tok), 0)
    t_b = lax.broadcasted_iota(jnp.int32, (tok, tok), 1)
    before_t = one_hot(t_a < t_b)
    before = one_hot(t_b < t_a)
    oh0 = e_rows == routes_t_ref[0:1, :]
    oh1 = e_rows == routes_t_ref[1:2, :]
    rank0 = dot(one_hot(oh0), before_t)
    rank1 = dot(one_hot(oh1), before_t) + jnp.sum(
        jnp.where(oh0, 1.0, 0.0), axis=1, keepdims=True
    )
    base = base_of(e_rows).astype(F32)
    place0 = jnp.sum(jnp.where(oh0, base + rank0, 0.0), axis=0, keepdims=True).astype(jnp.int32)
    place1 = jnp.sum(jnp.where(oh1, base + rank1, 0.0), axis=0, keepdims=True).astype(jnp.int32)
    slots = lax.broadcasted_iota(jnp.int32, (nz * ROWS, tok), 0)
    pick = one_hot((slots == place0) | (slots == place1))

    pl.semaphore_wait(barrier, n_exp - 1 + 2)

    def stack_pieces(rows):
        return jnp.concatenate(
            [rows[:, q * sub_w : (q + 1) * sub_w] for q in range(SUB)], axis=0
        )

    def join_pieces(stacked):
        return jnp.concatenate(
            [stacked[q * ROWS : (q + 1) * ROWS, :] for q in range(SUB)], axis=1
        )

    def to_blocks(rows):
        blocks = dot(pout_ref[...], stack_pieces(rows)).astype(BF)
        return blocks.reshape(PL, ROWS, sub_w)

    def to_rows(blocks):
        flat = blocks.reshape(PL * ROWS, sub_w)
        return join_pieces(dot(pin_ref[...], flat).astype(BF))

    def dispatch(i, p):
        return pltpu.make_async_remote_copy(
            src_ref=outgoing.at[i, p],
            dst_ref=arr.at[mirror(i), p_me],
            send_sem=d_send.at[i],
            recv_sem=d_recv.at[mirror(i)],
            device_id=peer(plane(i), p),
            device_id_type=MESH,
        )

    def give_back(i, p):
        return pltpu.make_async_remote_copy(
            src_ref=ret_out.at[i, p],
            dst_ref=ret_in.at[mirror(i), p_me],
            send_sem=r_send.at[i],
            recv_sem=r_recv.at[mirror(i)],
            device_id=peer(plane(i), p),
            device_id_type=MESH,
        )

    def to_plane(i, make):
        @pl.when(i == 0)
        def _():
            @pl.loop(1, PL)
            def _(j):
                make(i, lax.rem(p_me + j, PL)).start()

        @pl.when(i > 0)
        def _():
            @pl.loop(0, PL)
            def _(j):
                make(i, lax.rem(p_me + j, PL)).start()

    def wait_bytes(ref, sem):
        pltpu.make_async_copy(ref, ref, sem).wait()

    def wait_plane(i, ref, sem):
        @pl.when(i == 0)
        def _():
            wait_bytes(ref.at[0, pl.ds(0, PL - 1)], sem.at[0])

        @pl.when(i > 0)
        def _():
            wait_bytes(ref.at[i], sem.at[i])

    for i in range(nz):
        rows = dot(pick[i * ROWS : (i + 1) * ROWS, :], normed[...]).astype(BF)
        outgoing[i] = to_blocks(rows)
        if i == 0:
            arr[0, p_me] = outgoing[0, p_me]
        to_plane(jnp.int32(i), dispatch)

    def x_copy(src, dst, send, recv, to):
        return pltpu.make_async_remote_copy(
            src_ref=src, dst_ref=dst, send_sem=send, recv_sem=recv, device_id=to,
            device_id_type=MESH,
        )

    cols_a, cols_b = pl.ds(0, half), pl.ds(half, half)

    def ag_right(k):
        return x_copy(xall.at[k, 0], xall.at[k, 1], ag_send.at[k, 0], ag_recv.at[k, 0], right)

    def ag_left(k):
        return x_copy(xall.at[k, 0], xall.at[k, 2], ag_send.at[k, 1], ag_recv.at[k, 1], left)

    def fwd_right(k):
        return x_copy(
            xall.at[k, 1, :, cols_a], xall.at[k, 3, :, cols_a],
            ag_send.at[k, 2], ag_recv.at[k, 2], right,
        )

    def fwd_left(k):
        return x_copy(
            xall.at[k, 2, :, cols_b], xall.at[k, 3, :, cols_b],
            ag_send.at[k, 3], ag_recv.at[k, 3], left,
        )

    def rs_far_left(k):
        return x_copy(
            part.at[k, 3, :, cols_a], rs1.at[k, 0], rs_send.at[k, 0], rs1_recv.at[k, 0], left
        )

    def rs_far_right(k):
        return x_copy(
            part.at[k, 3, :, cols_b], rs1.at[k, 1], rs_send.at[k, 1], rs1_recv.at[k, 1], right
        )

    def rs_near_left(k, c, s):
        return x_copy(
            part.at[k, 1, :, c], rs2.at[k, 1, :, c], rs_send.at[k, s], rs2_recv.at[k, s - 2], left
        )

    def rs_near_right(k, c, s):
        return x_copy(
            part.at[k, 2, :, c], rs2.at[k, 0, :, c], rs_send.at[k, s], rs2_recv.at[k, s - 2], right
        )

    def rs_copies(k):
        return (
            rs_far_left(k),
            rs_far_right(k),
            rs_near_left(k, cols_a, 2),
            rs_near_left(k, cols_b, 3),
            rs_near_right(k, cols_a, 4),
            rs_near_right(k, cols_b, 5),
        )

    @pl.loop(0, nz + 5)
    def _(step):
        @pl.when(step < nz)
        def _():
            k = step
            wait_plane(k, arr, d_recv)
            xall[k, 0] = to_rows(arr[k])
            ag_right(k).start()
            ag_left(k).start()

        @pl.when((step >= 1) & (step < nz + 1))
        def _():
            k = step - 1
            ag_right(k).wait_recv()
            fwd_right(k).start()
            ag_left(k).wait_recv()
            fwd_left(k).start()

        @pl.when((step >= 2) & (step < nz + 2))
        def _():
            k = step - 2
            fwd_right(k).wait_recv()
            fwd_left(k).wait_recv()

            @pl.when(step == 2)
            def _():
                for copy in w_copies:
                    copy.wait()

            rows = xall[k].reshape(4 * ROWS, width)
            pre = dot(rows, wgu[...])
            gate_cut = jnp.minimum(pre[:, :ff], clamp_limit)
            up_cut = jnp.clip(pre[:, ff:], -clamp_limit, clamp_limit)
            hidden = (
                (up_cut + 1.0) * gate_cut * (1.0 / (1.0 + jnp.exp(-sigmoid_slope * gate_cut)))
            ).astype(BF)
            part[k] = dot(hidden, wd[...]).astype(BF).reshape(4, ROWS, width)
            rs_far_left(k).start()
            rs_far_right(k).start()
            rs_near_left(k, cols_b, 3).start()
            rs_near_right(k, cols_a, 4).start()

        @pl.when((step >= 3) & (step < nz + 3))
        def _():
            k = step - 3
            rs_far_left(k).wait_recv()
            part[k, 1, :, cols_a] = (
                part[k, 1, :, cols_a].astype(F32) + rs1[k, 0].astype(F32)
            ).astype(BF)
            rs_near_left(k, cols_a, 2).start()
            rs_far_right(k).wait_recv()
            part[k, 2, :, cols_b] = (
                part[k, 2, :, cols_b].astype(F32) + rs1[k, 1].astype(F32)
            ).astype(BF)
            rs_near_right(k, cols_b, 5).start()

        @pl.when((step >= 4) & (step < nz + 4))
        def _():
            k = step - 4
            for copy in rs_copies(k)[2:]:
                copy.wait_recv()
            total = (
                part[k, 0].astype(F32) + rs2[k, 0].astype(F32) + rs2[k, 1].astype(F32)
            ).astype(BF)
            ret_out[k] = to_blocks(total)

            @pl.when(k == 0)
            def _():
                ret_in[0, p_me] = ret_out[0, p_me]

            to_plane(k, give_back)

        @pl.when(step >= 5)
        def _():
            kk = mirror(step - 5)
            wait_plane(kk, ret_in, r_recv)
            ret_rows[kk] = to_rows(ret_in[kk])

    e_lanes = lax.broadcasted_iota(jnp.int32, (tok, n_exp), 1)
    ohc0 = e_lanes == routes_ref[:, 0:1]
    ohc1 = e_lanes == routes_ref[:, 1:2]
    crank0 = dot(before, one_hot(ohc0))
    crank1 = dot(before, one_hot(ohc1)) + jnp.sum(
        jnp.where(ohc0, 1.0, 0.0), axis=0, keepdims=True
    )
    cbase = base_of(e_lanes).astype(F32)
    at0 = jnp.sum(jnp.where(ohc0, cbase + crank0, 0.0), axis=1, keepdims=True).astype(jnp.int32)
    at1 = jnp.sum(jnp.where(ohc1, cbase + crank1, 0.0), axis=1, keepdims=True).astype(jnp.int32)
    lanes = lax.broadcasted_iota(jnp.int32, (tok, nz * ROWS), 1)
    take = jnp.concatenate([one_hot(lanes == at0), one_hot(lanes == at1)], axis=0)
    square = jnp.zeros((tok, 1), F32)
    block = min(512, width)
    for c in range(width // block):
        columns = slice(c * block, (c + 1) * block)
        both = dot(take, ret_rows[:, :, columns].reshape(nz * ROWS, block))
        mixed = rw_ref[:, 0:1] * both[:tok] + rw_ref[:, 1:2] * both[tok:]
        combined[:, columns] = mixed
        square = square + jnp.sum(mixed * mixed, axis=1, keepdims=True)
    scale = lax.rsqrt(square / width + norm_eps)
    out_ref[...] = (combined[...] * scale * fg_ref[...]).astype(BF)

    @pl.loop(0, nz)
    def _(k):
        wait_plane(k, outgoing, d_send)
        wait_plane(k, ret_out, r_send)
        ag_right(k).wait_send()
        ag_left(k).wait_send()
        fwd_right(k).wait_send()
        fwd_left(k).wait_send()
        for copy in rs_copies(k):
            copy.wait_send()


def permutation():
    source, piece, rank = np.meshgrid(
        np.arange(PL), np.arange(SUB), np.arange(CAP), indexing="ij"
    )
    travel = (source * SUB + piece) * CAP + rank
    rowwise = (piece * PL + source) * CAP + rank
    matrix = np.zeros((PL * ROWS, PL * ROWS), np.float32)
    matrix[rowwise.reshape(-1), travel.reshape(-1)] = 1.0
    return matrix


def expert_half(expert_in, routes, route_weights, expert_gain, gate_w, up_w, down_w, ffn_out_gain):
    nz = lax.axis_size("ep_0")
    tok, width = expert_in.shape
    ff = gate_w.shape[2]
    matrix = permutation()
    pin = jnp.asarray(matrix, BF)
    pout = jnp.asarray(matrix.T, BF)
    vmem = pl.BlockSpec(memory_space=pltpu.VMEM)
    hbm = pl.BlockSpec(memory_space=pl.ANY)
    travel = (nz, PL, ROWS, width // SUB)
    dma = pltpu.SemaphoreType.DMA
    return pl.pallas_call(
        functools.partial(experts_kernel, nz),
        out_shape=jax.ShapeDtypeStruct((tok, width), BF),
        in_specs=[vmem] * 8 + [hbm] * 3,
        out_specs=vmem,
        scratch_shapes=[
            pltpu.VMEM((tok, width), BF),
            pltpu.VMEM(travel, BF),
            pltpu.VMEM(travel, BF),
            pltpu.VMEM((nz, 4, ROWS, width), BF),
            pltpu.VMEM((nz, 4, ROWS, width), BF),
            pltpu.VMEM((nz, 2, ROWS, width // 2), BF),
            pltpu.VMEM((nz, 2, ROWS, width), BF),
            pltpu.VMEM(travel, BF),
            pltpu.VMEM(travel, BF),
            pltpu.VMEM((nz, ROWS, width), BF),
            pltpu.VMEM((width, 2 * ff), BF),
            pltpu.VMEM((ff, width), BF),
            pltpu.VMEM((tok, width), F32),
            dma((3,)),
            dma((nz,)),
            dma((nz,)),
            dma((nz, 4)),
            dma((nz, 4)),
            dma((nz, 6)),
            dma((nz, 2)),
            dma((nz, 4)),
            dma((nz,)),
            dma((nz,)),
        ],
        compiler_params=pltpu.CompilerParams(
            collective_id=0, has_side_effects=True, vmem_limit_bytes=60 * 2**20
        ),
        cost_estimate=pl.CostEstimate(
            flops=60 * 10**9, bytes_accessed=8 * 2**20, transcendentals=0
        ),
        name="experts",
    )(
        expert_in,
        routes,
        routes.T,
        route_weights,
        expert_gain[None, :],
        ffn_out_gain[None, :],
        pin,
        pout,
        gate_w,
        up_w,
        down_w,
    )


def local(
    queries,
    keys,
    values,
    query_gain,
    key_gain,
    out_weight,
    mixer_gain,
    expert_in,
    routes,
    route_weights,
    expert_gain,
    gate_w,
    up_w,
    down_w,
    ffn_out_gain,
):
    expert_out = expert_half(
        expert_in, routes, route_weights, expert_gain, gate_w, up_w, down_w, ffn_out_gain
    )
    mixer_out = mixer_half(queries, keys, values, query_gain, key_gain, out_weight, mixer_gain)
    return (mixer_out, expert_out)


def solution(mesh):
    split = Mesh(
        mesh.devices.reshape(mesh.shape["ep"] // 8, 4, 2, mesh.shape["tp"]),
        ("ep_0", "ep_1", "ep_2", "tp"),
    )
    return jax.shard_map(
        local,
        mesh=split,
        in_specs=(
            P(EP, "tp"),
            P(EP, "tp"),
            P(EP, "tp"),
            P(),
            P(),
            P("tp", None),
            P(),
            P(EP_TP, None),
            P(EP_TP, None),
            P(EP_TP, None),
            P(),
            P(EP, None, "tp"),
            P(EP, None, "tp"),
            P(EP, "tp", None),
            P(),
        ),
        out_specs=(P(EP_TP, None), P(EP_TP, None)),
        check_vma=False,
    )
```

```python
import functools

import jax
import jax.numpy as jnp
import numpy as np
from jax import lax
from jax.experimental import pallas as pl
from jax.experimental.pallas import tpu as pltpu
from jax.sharding import Mesh
from jax.sharding import PartitionSpec as P

HEAD = 128
HEADS = 4
GRID_W = 64
TP = 4
EP = ("ep_0", "ep_1", "ep_2")
EP_TP = ("ep_0", "ep_1", "ep_2", "tp")
MESH = pl.DeviceIdType.MESH
BF = jnp.bfloat16
F32 = jnp.float32

norm_eps = 1e-06
rope_base = 10000.0
clamp_limit = 7.0
sigmoid_slope = 1.702

PL = 8
CAP = 6
SUB = 8
ROWS = PL * CAP


def rms_scale(values_in, gain):
    return (
        values_in
        * lax.rsqrt(jnp.mean(values_in * values_in, axis=-1, keepdims=True) + norm_eps)
        * gain
    )


def dot(a, b):
    return jnp.dot(a, b, preferred_element_type=F32)


def one_hot(cond):
    return jnp.where(cond, 1.0, 0.0).astype(BF)


def layer_kernel(
    nz,
    x_ref,
    routes_ref,
    routes_t_ref,
    rw_ref,
    eg_ref,
    fg_ref,
    pin_ref,
    pout_ref,
    q_ref,
    k_ref,
    v_ref,
    qg_ref,
    kg_ref,
    mg_ref,
    cos_row_ref,
    sin_row_ref,
    cos_col_ref,
    sin_col_ref,
    gate_hbm,
    up_hbm,
    down_hbm,
    ow_hbm,
    mix_ref,
    out_ref,
    normed,
    outgoing,
    arr,
    xall,
    part,
    rs1,
    rs2,
    ret_out,
    ret_in,
    ret_rows,
    wgu,
    wd,
    combined,
    ow,
    kv,
    q_s,
    m_s,
    l_s,
    acc_s,
    att_s,
    w_sem,
    d_send,
    d_recv,
    ag_send,
    ag_recv,
    rs_send,
    rs1_recv,
    rs2_recv,
    r_send,
    r_recv,
    kz_send,
    kz_recv,
    ky_send,
    ky_recv,
    kc_send,
    kc_recv,
):
    z = lax.axis_index("ep_0")
    p_me = lax.axis_index("ep_1") * 2 + lax.axis_index("ep_2")
    x_me = lax.axis_index("tp")
    right = {"tp": lax.rem(x_me + 1, 4)}
    left = {"tp": lax.rem(x_me + 3, 4)}
    y_me = lax.axis_index("ep_1")
    y_up = {"ep_1": lax.rem(y_me + 1, 4)}
    y_down = {"ep_1": lax.rem(y_me + 3, 4)}
    other_core = {"ep_2": 1 - lax.axis_index("ep_2")}
    tok, width = x_ref.shape
    half = width // 2
    sub_w = width // SUB
    ff = wd.shape[0]
    n_exp = nz * PL

    def peer(zz, p):
        return {"ep_0": zz, "ep_1": p // 2, "ep_2": lax.rem(p, 2)}

    def away(i):
        return jnp.where(lax.rem(i, 2) == 1, (i + 1) // 2, -(i // 2))

    def plane(i):
        return lax.rem(z + away(i) + nz, nz)

    def mirror(i):
        other = jnp.where(lax.rem(i, 2) == 1, i + 1, i - 1)
        return jnp.where((i == 0) | (i == nz - 1), i, other)

    barrier = pltpu.get_barrier_semaphore()

    @pl.loop(1, n_exp)
    def _(j):
        to = lax.rem(z * PL + p_me + j, n_exp)
        pl.semaphore_signal(
            barrier, inc=1, device_id=peer(to // PL, lax.rem(to, PL)), device_id_type=MESH
        )

    pl.semaphore_signal(barrier, inc=1, device_id=left, device_id_type=MESH)
    pl.semaphore_signal(barrier, inc=1, device_id=right, device_id_type=MESH)

    w_copies = [
        pltpu.make_async_copy(gate_hbm.at[0], wgu.at[:, pl.ds(0, ff)], w_sem.at[0]),
        pltpu.make_async_copy(up_hbm.at[0], wgu.at[:, pl.ds(ff, ff)], w_sem.at[1]),
        pltpu.make_async_copy(down_hbm.at[0], wd, w_sem.at[2]),
        pltpu.make_async_copy(ow_hbm, ow, w_sem.at[3]),
    ]
    for copy in w_copies:
        copy.start()

    xf = x_ref[...].astype(F32)
    normed[...] = rms_scale(xf, eg_ref[...]).astype(BF)

    grid_rows = k_ref.shape[0] // GRID_W
    first_row = (z * PL + p_me) * grid_rows
    cosine = jnp.concatenate(
        [cos_row_ref[pl.ds(first_row + g, 1), :] + cos_col_ref[...] for g in range(grid_rows)],
        axis=0,
    )
    sine = jnp.concatenate(
        [sin_row_ref[pl.ds(first_row + g, 1), :] + sin_col_ref[...] for g in range(grid_rows)],
        axis=0,
    )
    lane = lax.broadcasted_iota(jnp.int32, cosine.shape, 1)
    first_of_pair = (lane & 32) == 0

    def normed_and_turned(head, gain):
        field = rms_scale(head.astype(F32), gain)
        swapped = jnp.where(
            first_of_pair, pltpu.roll(field, HEAD - 32, 1), pltpu.roll(field, 32, 1)
        )
        return (field * cosine + swapped * sine).astype(BF)

    kv[0, 0, 0, 0] = normed_and_turned(k_ref[...], kg_ref[...])
    kv[0, 0, 0, 1] = v_ref[...]
    for h in range(HEADS):
        q_s[h] = normed_and_turned(q_ref[:, h * HEAD : (h + 1) * HEAD], qg_ref[...])
    m_s[...] = jnp.full(m_s.shape, -1e30, F32)
    l_s[...] = jnp.zeros(l_s.shape, F32)
    acc_s[...] = jnp.zeros(acc_s.shape, F32)

    def base_of(e):
        o = (lax.shift_right_logical(e, 3) - z + nz) & (nz - 1)
        idx = jnp.where(o == 0, 0, jnp.where(o <= nz // 2, 2 * o - 1, 2 * (nz - o)))
        return idx * ROWS + (e & 7) * CAP

    e_rows = lax.broadcasted_iota(jnp.int32, (n_exp, tok), 0)
    t_a = lax.broadcasted_iota(jnp.int32, (tok, tok), 0)
    t_b = lax.broadcasted_iota(jnp.int32, (tok, tok), 1)
    before_t = one_hot(t_a < t_b)
    before = one_hot(t_b < t_a)
    oh0 = e_rows == routes_t_ref[0:1, :]
    oh1 = e_rows == routes_t_ref[1:2, :]
    rank0 = dot(one_hot(oh0), before_t)
    rank1 = dot(one_hot(oh1), before_t) + jnp.sum(
        jnp.where(oh0, 1.0, 0.0), axis=1, keepdims=True
    )
    base = base_of(e_rows).astype(F32)
    place0 = jnp.sum(jnp.where(oh0, base + rank0, 0.0), axis=0, keepdims=True).astype(jnp.int32)
    place1 = jnp.sum(jnp.where(oh1, base + rank1, 0.0), axis=0, keepdims=True).astype(jnp.int32)
    slots = lax.broadcasted_iota(jnp.int32, (nz * ROWS, tok), 0)
    pick = one_hot((slots == place0) | (slots == place1))

    pl.semaphore_wait(barrier, n_exp - 1 + 2)

    def stack_pieces(rows):
        return jnp.concatenate(
            [rows[:, q * sub_w : (q + 1) * sub_w] for q in range(SUB)], axis=0
        )

    def join_pieces(stacked):
        return jnp.concatenate(
            [stacked[q * ROWS : (q + 1) * ROWS, :] for q in range(SUB)], axis=1
        )

    def to_blocks(rows):
        blocks = dot(pout_ref[...], stack_pieces(rows)).astype(BF)
        return blocks.reshape(PL, ROWS, sub_w)

    def to_rows(blocks):
        flat = blocks.reshape(PL * ROWS, sub_w)
        return join_pieces(dot(pin_ref[...], flat).astype(BF))

    def dispatch(i, p):
        return pltpu.make_async_remote_copy(
            src_ref=outgoing.at[i, p],
            dst_ref=arr.at[mirror(i), p_me],
            send_sem=d_send.at[i],
            recv_sem=d_recv.at[mirror(i)],
            device_id=peer(plane(i), p),
            device_id_type=MESH,
        )

    def give_back(i, p):
        return pltpu.make_async_remote_copy(
            src_ref=ret_out.at[i, p],
            dst_ref=ret_in.at[mirror(i), p_me],
            send_sem=r_send.at[i],
            recv_sem=r_recv.at[mirror(i)],
            device_id=peer(plane(i), p),
            device_id_type=MESH,
        )

    def x_copy(src, dst, send, recv, to):
        return pltpu.make_async_remote_copy(
            src_ref=src, dst_ref=dst, send_sem=send, recv_sem=recv, device_id=to,
            device_id_type=MESH,
        )

    def kv_plane(i):
        return x_copy(
            kv.at[0, 0, 0], kv.at[mirror(i), 0, 0], kz_send.at[i], kz_recv.at[mirror(i)],
            {"ep_0": plane(i)},
        )

    def kv_up(k):
        return x_copy(kv.at[k, 0, 0], kv.at[k, 0, 1], ky_send.at[k, 0], ky_recv.at[k, 0], y_up)

    def kv_down(k):
        return x_copy(kv.at[k, 0, 0], kv.at[k, 0, 2], ky_send.at[k, 1], ky_recv.at[k, 1], y_down)

    def k_far(k):
        return x_copy(
            kv.at[k, 0, 1, 0], kv.at[k, 0, 3, 0], ky_send.at[k, 2], ky_recv.at[k, 2], y_up
        )

    def v_far(k):
        return x_copy(
            kv.at[k, 0, 2, 1], kv.at[k, 0, 3, 1], ky_send.at[k, 3], ky_recv.at[k, 3], y_down
        )

    def kv_across(k):
        return x_copy(kv.at[k, 0], kv.at[k, 1], kc_send.at[k], kc_recv.at[k], other_core)

    def attend(k):
        keys = kv[k, :, :, 0].reshape(-1, HEAD)
        vals = kv[k, :, :, 1].reshape(-1, HEAD)

        @pl.loop(0, HEADS)
        def _(h):
            scores = lax.dot_general(
                q_s[h], keys, (((1,), (1,)), ((), ())), preferred_element_type=F32
            ) * HEAD ** (-0.5)
            peak = jnp.maximum(m_s[h], jnp.max(scores, axis=1, keepdims=True))
            fade = jnp.exp(m_s[h] - peak)
            expo = jnp.exp(scores - peak[:, :1])
            m_s[h] = peak
            sums = l_s[h] * fade
            for c in range(expo.shape[1] // HEAD):
                sums = sums + expo[:, c * HEAD : (c + 1) * HEAD]
            l_s[h] = sums
            acc_s[h] = acc_s[h] * fade + dot(expo.astype(BF), vals)

    def project():
        for h in range(HEADS):
            total = jnp.sum(l_s[h], axis=1, keepdims=True)
            att_s[:, h * HEAD : (h + 1) * HEAD] = (acc_s[h] / total).astype(BF)
        share = att_s.shape[0] // TP
        ours = jnp.concatenate(
            [
                att_s[pl.ds(pl.multiple_of(lax.rem(x_me + o, TP) * share, share), share), :]
                for o in (0, 3, 1, 2)
            ],
            axis=0,
        )
        return dot(ours, ow[...]).astype(BF).reshape(TP, share, width)

    def to_plane(i, make):
        @pl.when(i == 0)
        def _():
            @pl.loop(1, PL)
            def _(j):
                make(i, lax.rem(p_me + j, PL)).start()

        @pl.when(i > 0)
        def _():
            @pl.loop(0, PL)
            def _(j):
                make(i, lax.rem(p_me + j, PL)).start()

    def wait_bytes(ref, sem):
        pltpu.make_async_copy(ref, ref, sem).wait()

    def wait_plane(i, ref, sem):
        @pl.when(i == 0)
        def _():
            wait_bytes(ref.at[0, pl.ds(0, PL - 1)], sem.at[0])

        @pl.when(i > 0)
        def _():
            wait_bytes(ref.at[i], sem.at[i])

    for i in range(nz):
        rows = dot(pick[i * ROWS : (i + 1) * ROWS, :], normed[...]).astype(BF)
        outgoing[i] = to_blocks(rows)
        if i == 0:
            arr[0, p_me] = outgoing[0, p_me]
        to_plane(jnp.int32(i), dispatch)
        if i > 0:
            kv_plane(jnp.int32(i)).start()

    cols_a, cols_b = pl.ds(0, half), pl.ds(half, half)

    def ag_right(k):
        return x_copy(xall.at[k, 0], xall.at[k, 1], ag_send.at[k, 0], ag_recv.at[k, 0], right)

    def ag_left(k):
        return x_copy(xall.at[k, 0], xall.at[k, 2], ag_send.at[k, 1], ag_recv.at[k, 1], left)

    def fwd_right(k):
        return x_copy(
            xall.at[k, 1, :, cols_a], xall.at[k, 3, :, cols_a],
            ag_send.at[k, 2], ag_recv.at[k, 2], right,
        )

    def fwd_left(k):
        return x_copy(
            xall.at[k, 2, :, cols_b], xall.at[k, 3, :, cols_b],
            ag_send.at[k, 3], ag_recv.at[k, 3], left,
        )

    def rs_far_left(k):
        return x_copy(
            part.at[k, 3, :, cols_a], rs1.at[k, 0], rs_send.at[k, 0], rs1_recv.at[k, 0], left
        )

    def rs_far_right(k):
        return x_copy(
            part.at[k, 3, :, cols_b], rs1.at[k, 1], rs_send.at[k, 1], rs1_recv.at[k, 1], right
        )

    def rs_near_left(k, c, s):
        return x_copy(
            part.at[k, 1, :, c], rs2.at[k, 1, :, c], rs_send.at[k, s], rs2_recv.at[k, s - 2], left
        )

    def rs_near_right(k, c, s):
        return x_copy(
            part.at[k, 2, :, c], rs2.at[k, 0, :, c], rs_send.at[k, s], rs2_recv.at[k, s - 2], right
        )

    def rs_copies(k):
        return (
            rs_far_left(k),
            rs_far_right(k),
            rs_near_left(k, cols_a, 2),
            rs_near_left(k, cols_b, 3),
            rs_near_right(k, cols_a, 4),
            rs_near_right(k, cols_b, 5),
        )

    def rs_start(k):
        rs_far_left(k).start()
        rs_far_right(k).start()
        rs_near_left(k, cols_b, 3).start()
        rs_near_right(k, cols_a, 4).start()

    def rs_total(k):
        for copy in rs_copies(k)[2:]:
            copy.wait_recv()
        return part[k, 0].astype(F32) + rs2[k, 0].astype(F32) + rs2[k, 1].astype(F32)

    @pl.loop(0, nz + 5)
    def _(step):
        @pl.when(step < nz)
        def _():
            k = step
            wait_plane(k, arr, d_recv)
            xall[k, 0] = to_rows(arr[k])
            ag_right(k).start()
            ag_left(k).start()

            @pl.when(k > 0)
            def _():
                wait_bytes(kv.at[k, 0, 0], kz_recv.at[k])

            kv_up(k).start()
            kv_down(k).start()

        @pl.when((step >= 1) & (step < nz + 1))
        def _():
            k = step - 1
            ag_right(k).wait_recv()
            fwd_right(k).start()
            ag_left(k).wait_recv()
            fwd_left(k).start()
            kv_up(k).wait_recv()
            k_far(k).start()
            kv_down(k).wait_recv()
            v_far(k).start()

        @pl.when((step >= 2) & (step < nz + 2))
        def _():
            k = step - 2
            fwd_right(k).wait_recv()
            fwd_left(k).wait_recv()

            @pl.when(step == 2)
            def _():
                for copy in w_copies:
                    copy.wait()

            rows = xall[k].reshape(4 * ROWS, width)
            pre = dot(rows, wgu[...])
            gate_cut = jnp.minimum(pre[:, :ff], clamp_limit)
            up_cut = jnp.clip(pre[:, ff:], -clamp_limit, clamp_limit)
            hidden = (
                (up_cut + 1.0) * gate_cut * (1.0 / (1.0 + jnp.exp(-sigmoid_slope * gate_cut)))
            ).astype(BF)
            part[k] = dot(hidden, wd[...]).astype(BF).reshape(4, ROWS, width)
            rs_start(k)
            k_far(k).wait_recv()
            v_far(k).wait_recv()
            kv_across(k).start()

        @pl.when((step >= 3) & (step < nz + 4))
        def _():
            k = step - 3
            rs_far_left(k).wait_recv()
            part[k, 1, :, cols_a] = (
                part[k, 1, :, cols_a].astype(F32) + rs1[k, 0].astype(F32)
            ).astype(BF)
            rs_near_left(k, cols_a, 2).start()
            rs_far_right(k).wait_recv()
            part[k, 2, :, cols_b] = (
                part[k, 2, :, cols_b].astype(F32) + rs1[k, 1].astype(F32)
            ).astype(BF)
            rs_near_right(k, cols_b, 5).start()

        @pl.when((step >= 4) & (step < nz + 4))
        def _():
            k = step - 4
            ret_out[k] = to_blocks(rs_total(k).astype(BF))

            @pl.when(k == 0)
            def _():
                ret_in[0, p_me] = ret_out[0, p_me]

            to_plane(k, give_back)

        @pl.when(step >= 5)
        def _():
            kk = mirror(step - 5)
            wait_plane(kk, ret_in, r_recv)
            ret_rows[kk] = to_rows(ret_in[kk])

        @pl.when((step >= 3) & (step < nz + 3))
        def _():
            k = step - 3
            kv_across(k).wait_recv()
            attend(k)

        @pl.when(step == nz + 2)
        def _():
            part[nz] = project()
            rs_start(nz)

    mix_ref[...] = rms_scale(rs_total(nz), mg_ref[...]).astype(BF)

    e_lanes = lax.broadcasted_iota(jnp.int32, (tok, n_exp), 1)
    ohc0 = e_lanes == routes_ref[:, 0:1]
    ohc1 = e_lanes == routes_ref[:, 1:2]
    crank0 = dot(before, one_hot(ohc0))
    crank1 = dot(before, one_hot(ohc1)) + jnp.sum(
        jnp.where(ohc0, 1.0, 0.0), axis=0, keepdims=True
    )
    cbase = base_of(e_lanes).astype(F32)
    at0 = jnp.sum(jnp.where(ohc0, cbase + crank0, 0.0), axis=1, keepdims=True).astype(jnp.int32)
    at1 = jnp.sum(jnp.where(ohc1, cbase + crank1, 0.0), axis=1, keepdims=True).astype(jnp.int32)
    lanes = lax.broadcasted_iota(jnp.int32, (tok, nz * ROWS), 1)
    take = jnp.concatenate([one_hot(lanes == at0), one_hot(lanes == at1)], axis=0)
    square = jnp.zeros((tok, 1), F32)
    block = min(512, width)
    for c in range(width // block):
        columns = slice(c * block, (c + 1) * block)
        both = dot(take, ret_rows[:, :, columns].reshape(nz * ROWS, block))
        mixed = rw_ref[:, 0:1] * both[:tok] + rw_ref[:, 1:2] * both[tok:]
        combined[:, columns] = mixed
        square = square + jnp.sum(mixed * mixed, axis=1, keepdims=True)
    scale = lax.rsqrt(square / width + norm_eps)
    out_ref[...] = (combined[...] * scale * fg_ref[...]).astype(BF)

    @pl.loop(0, nz)
    def _(k):
        wait_plane(k, outgoing, d_send)
        wait_plane(k, ret_out, r_send)
        ag_right(k).wait_send()
        ag_left(k).wait_send()
        fwd_right(k).wait_send()
        fwd_left(k).wait_send()
        kv_up(k).wait_send()
        kv_down(k).wait_send()
        k_far(k).wait_send()
        v_far(k).wait_send()
        kv_across(k).wait_send()

        @pl.when(k > 0)
        def _():
            kv_plane(k).wait_send()

    @pl.loop(0, nz + 1)
    def _(k):
        for copy in rs_copies(k):
            copy.wait_send()


def permutation():
    source, piece, rank = np.meshgrid(
        np.arange(PL), np.arange(SUB), np.arange(CAP), indexing="ij"
    )
    travel = (source * SUB + piece) * CAP + rank
    rowwise = (piece * PL + source) * CAP + rank
    matrix = np.zeros((PL * ROWS, PL * ROWS), np.float32)
    matrix[rowwise.reshape(-1), travel.reshape(-1)] = 1.0
    return matrix


def turn_tables(rows):
    quarter = HEAD // 4
    inverse = rope_base ** (-np.arange(quarter, dtype=np.float64) / quarter)

    def table(count, make, at):
        angle = np.arange(count, dtype=np.float64)[:, None] * inverse[None, :]
        out = np.zeros((count, HEAD), np.float32)
        out[:, at : at + 2 * quarter] = make(angle)
        return jnp.asarray(out)

    def cosines(angle):
        return np.concatenate([np.cos(angle), np.cos(angle)], axis=1)

    def sines(angle):
        return np.concatenate([-np.sin(angle), np.sin(angle)], axis=1)

    return (
        table(rows, cosines, 0),
        table(rows, sines, 0),
        table(GRID_W, cosines, HEAD // 2),
        table(GRID_W, sines, HEAD // 2),
    )


def local(
    queries,
    keys,
    values,
    query_gain,
    key_gain,
    out_weight,
    mixer_gain,
    expert_in,
    routes,
    route_weights,
    expert_gain,
    gate_w,
    up_w,
    down_w,
    ffn_out_gain,
):
    nz = lax.axis_size("ep_0")
    tok, width = expert_in.shape
    ff = gate_w.shape[2]
    seq = queries.shape[0]
    tables = turn_tables(nz * PL * seq // GRID_W)
    matrix = permutation()
    pin = jnp.asarray(matrix, BF)
    pout = jnp.asarray(matrix.T, BF)
    vmem = pl.BlockSpec(memory_space=pltpu.VMEM)
    hbm = pl.BlockSpec(memory_space=pl.ANY)
    travel = (nz, PL, ROWS, width // SUB)
    dma = pltpu.SemaphoreType.DMA
    return pl.pallas_call(
        functools.partial(layer_kernel, nz),
        out_shape=(
            jax.ShapeDtypeStruct((seq // TP, width), BF),
            jax.ShapeDtypeStruct((tok, width), BF),
        ),
        in_specs=[vmem] * 18 + [hbm] * 4,
        out_specs=(vmem, vmem),
        scratch_shapes=[
            pltpu.VMEM((tok, width), BF),
            pltpu.VMEM(travel, BF),
            pltpu.VMEM(travel, BF),
            pltpu.VMEM((nz, 4, ROWS, width), BF),
            pltpu.VMEM((nz + 1, 4, ROWS, width), BF),
            pltpu.VMEM((nz + 1, 2, ROWS, width // 2), BF),
            pltpu.VMEM((nz + 1, 2, ROWS, width), BF),
            pltpu.VMEM(travel, BF),
            pltpu.VMEM(travel, BF),
            pltpu.VMEM((nz, ROWS, width), BF),
            pltpu.VMEM((width, 2 * ff), BF),
            pltpu.VMEM((ff, width), BF),
            pltpu.VMEM((tok, width), F32),
            pltpu.VMEM(out_weight.shape, BF),
            pltpu.VMEM((nz, 2, 4, 2, seq, HEAD), BF),
            pltpu.VMEM((HEADS, seq, HEAD), BF),
            pltpu.VMEM((HEADS, seq, HEAD), F32),
            pltpu.VMEM((HEADS, seq, HEAD), F32),
            pltpu.VMEM((HEADS, seq, HEAD), F32),
            pltpu.VMEM((seq, HEADS * HEAD), BF),
            dma((4,)),
            dma((nz,)),
            dma((nz,)),
            dma((nz, 4)),
            dma((nz, 4)),
            dma((nz + 1, 6)),
            dma((nz + 1, 2)),
            dma((nz + 1, 4)),
            dma((nz,)),
            dma((nz,)),
            dma((nz,)),
            dma((nz,)),
            dma((nz, 4)),
            dma((nz, 4)),
            dma((nz,)),
            dma((nz,)),
        ],
        compiler_params=pltpu.CompilerParams(
            collective_id=0, has_side_effects=True, vmem_limit_bytes=62 * 2**20
        ),
        name="layer",
    )(
        expert_in,
        routes,
        routes.T,
        route_weights,
        expert_gain[None, :],
        ffn_out_gain[None, :],
        pin,
        pout,
        queries,
        keys,
        values,
        query_gain[None, :],
        key_gain[None, :],
        mixer_gain[None, :],
        *tables,
        gate_w,
        up_w,
        down_w,
        out_weight,
    )


def solution(mesh):
    split = Mesh(
        mesh.devices.reshape(mesh.shape["ep"] // 8, 4, 2, mesh.shape["tp"]),
        ("ep_0", "ep_1", "ep_2", "tp"),
    )
    return jax.shard_map(
        local,
        mesh=split,
        in_specs=(
            P(EP, "tp"),
            P(EP, "tp"),
            P(EP, "tp"),
            P(),
            P(),
            P("tp", None),
            P(),
            P(EP_TP, None),
            P(EP_TP, None),
            P(EP_TP, None),
            P(),
            P(EP, None, "tp"),
            P(EP, None, "tp"),
            P(EP, "tp", None),
            P(),
        ),
        out_specs=(P(EP_TP, None), P(EP_TP, None)),
        check_vma=False,
    )
```

```python
import functools

import jax
import jax.numpy as jnp
import numpy as np
from jax import lax
from jax.experimental import pallas as pl
from jax.experimental.pallas import tpu as pltpu
from jax.sharding import Mesh
from jax.sharding import PartitionSpec as P

HEAD = 128
HEADS = 4
GRID_W = 64
TP = 4
OPERANDS = 17
EP = ("ep_0", "ep_1", "ep_2")
EP_TP = ("ep_0", "ep_1", "ep_2", "tp")
MESH = pl.DeviceIdType.MESH
BF = jnp.bfloat16
F32 = jnp.float32

norm_eps = 1e-06
rope_base = 10000.0
clamp_limit = 7.0
sigmoid_slope = 1.702

PL = 8
CAP = 6
SUB = 8
ROWS = PL * CAP
AWAY = (0, 1, -3, 3, 4, -2, 2, -1)
NZ = len(AWAY)
FIRST = (0, 1, 2)
LATER = {0: (3,), 1: (5,), 2: (4, 7), 3: (6,)}
INDEX = [[a % NZ for a in AWAY].index(d) for d in range(NZ)]
MIRROR = [INDEX[-a % NZ] for a in AWAY]


def rms_scale(values_in, gain):
    return (
        values_in
        * lax.rsqrt(jnp.mean(values_in * values_in, axis=-1, keepdims=True) + norm_eps)
        * gain
    )


def dot(a, b):
    return jnp.dot(a, b, preferred_element_type=F32)


def one_hot(cond):
    return jnp.where(cond, 1.0, 0.0).astype(BF)


def layer_kernel(nz, *refs):
    ours = refs[:OPERANDS]
    held = refs[OPERANDS + 6 : 2 * OPERANDS + 6]
    sems = refs[-1]
    copies = [
        pltpu.make_async_copy(src, dst, sems.at[i])
        for i, (src, dst) in enumerate(zip(ours, held))
    ]
    for copy in copies:
        copy.start()

    def operands_here():
        for copy in copies:
            copy.wait()

    layer(nz, operands_here, *held, *refs[OPERANDS : OPERANDS + 6], *refs[2 * OPERANDS + 6 : -1])


def layer(
    nz,
    operands_here,
    x_ref,
    routes_t_ref,
    rw_t_ref,
    eg_ref,
    fg_ref,
    pin_ref,
    pout_ref,
    q_ref,
    k_ref,
    v_ref,
    qg_ref,
    kg_ref,
    mg_ref,
    cos_row_ref,
    sin_row_ref,
    cos_col_ref,
    sin_col_ref,
    gate_hbm,
    up_hbm,
    down_hbm,
    ow_hbm,
    mix_ref,
    out_ref,
    normed,
    outgoing,
    arr,
    xall,
    part,
    rs1,
    rs2,
    ret_out,
    ret_in,
    ret_rows,
    wgu,
    wd,
    combined,
    ow,
    kv,
    side,
    q_s,
    m_s,
    l_s,
    acc_s,
    att_s,
    w_sem,
    d_send,
    d_recv,
    ag_send,
    ag_recv,
    rs_send,
    rs1_recv,
    rs2_recv,
    r_send,
    r_recv,
    kz_send,
    kz_recv,
    ky_send,
    ky_recv,
    kc_send,
    kc_recv,
):
    z = lax.axis_index("ep_0")
    p_me = lax.axis_index("ep_1") * 2 + lax.axis_index("ep_2")
    x_me = lax.axis_index("tp")
    right = {"tp": lax.rem(x_me + 1, 4)}
    left = {"tp": lax.rem(x_me + 3, 4)}
    y_me = lax.axis_index("ep_1")
    y_up = {"ep_1": lax.rem(y_me + 1, 4)}
    y_down = {"ep_1": lax.rem(y_me + 3, 4)}
    other_core = {"ep_2": 1 - lax.axis_index("ep_2")}
    tok, width = x_ref.shape
    half = width // 2
    sub_w = width // SUB
    ff = wd.shape[0]
    n_exp = nz * PL

    def peer(zz, p):
        return {"ep_0": zz, "ep_1": p // 2, "ep_2": lax.rem(p, 2)}

    def entry(values, i):
        found = jnp.full(jnp.shape(i), values[0], jnp.int32)
        for j in range(1, nz):
            found = jnp.where(i == j, values[j], found)
        return found

    def plane(i):
        return lax.rem(z + entry([a % nz for a in AWAY], i), nz)

    def mirror(i):
        return entry(MIRROR, i)

    barrier = pltpu.get_barrier_semaphore()

    @pl.loop(1, n_exp)
    def _(j):
        to = lax.rem(z * PL + p_me + j, n_exp)
        pl.semaphore_signal(
            barrier, inc=1, device_id=peer(to // PL, lax.rem(to, PL)), device_id_type=MESH
        )

    pl.semaphore_signal(barrier, inc=1, device_id=left, device_id_type=MESH)
    pl.semaphore_signal(barrier, inc=1, device_id=right, device_id_type=MESH)

    w_copies = [
        pltpu.make_async_copy(gate_hbm.at[0], wgu.at[:, pl.ds(0, ff)], w_sem.at[0]),
        pltpu.make_async_copy(up_hbm.at[0], wgu.at[:, pl.ds(ff, ff)], w_sem.at[1]),
        pltpu.make_async_copy(down_hbm.at[0], wd, w_sem.at[2]),
        pltpu.make_async_copy(ow_hbm, ow, w_sem.at[3]),
    ]
    for copy in w_copies:
        copy.start()

    operands_here()
    xf = x_ref[...].astype(F32)
    normed[...] = rms_scale(xf, eg_ref[...]).astype(BF)

    grid_rows = k_ref.shape[0] // GRID_W
    first_row = (z * PL + p_me) * grid_rows
    cosine = jnp.concatenate(
        [cos_row_ref[pl.ds(first_row + g, 1), :] + cos_col_ref[...] for g in range(grid_rows)],
        axis=0,
    )
    sine = jnp.concatenate(
        [sin_row_ref[pl.ds(first_row + g, 1), :] + sin_col_ref[...] for g in range(grid_rows)],
        axis=0,
    )
    lane = lax.broadcasted_iota(jnp.int32, cosine.shape, 1)
    first_of_pair = (lane & 32) == 0

    def normed_and_turned(head, gain):
        field = rms_scale(head.astype(F32), gain)
        swapped = jnp.where(
            first_of_pair, pltpu.roll(field, HEAD - 32, 1), pltpu.roll(field, 32, 1)
        )
        return (field * cosine + swapped * sine).astype(BF)

    kv[0, 0, 0, 0] = normed_and_turned(k_ref[...], kg_ref[...])
    kv[0, 0, 0, 1] = v_ref[...]
    for h in range(HEADS):
        q_s[h] = normed_and_turned(q_ref[:, h * HEAD : (h + 1) * HEAD], qg_ref[...])
    m_s[...] = jnp.full(m_s.shape, -1e30, F32)
    l_s[...] = jnp.zeros(l_s.shape, F32)
    acc_s[...] = jnp.zeros(acc_s.shape, F32)

    def base_of(e):
        o = (lax.shift_right_logical(e, 3) - z + nz) & (nz - 1)
        return entry(INDEX, o) * ROWS + (e & 7) * CAP

    e_rows = lax.broadcasted_iota(jnp.int32, (n_exp, tok), 0)
    t_a = lax.broadcasted_iota(jnp.int32, (tok, tok), 0)
    t_b = lax.broadcasted_iota(jnp.int32, (tok, tok), 1)
    before_t = one_hot(t_a < t_b)
    oh0 = e_rows == routes_t_ref[0:1, :]
    oh1 = e_rows == routes_t_ref[1:2, :]
    rank0 = dot(one_hot(oh0), before_t)
    rank1 = dot(one_hot(oh1), before_t) + jnp.sum(
        jnp.where(oh0, 1.0, 0.0), axis=1, keepdims=True
    )
    base = base_of(e_rows).astype(F32)
    place0 = jnp.sum(jnp.where(oh0, base + rank0, 0.0), axis=0, keepdims=True)
    place1 = jnp.sum(jnp.where(oh1, base + rank1, 0.0), axis=0, keepdims=True)
    slots = lax.broadcasted_iota(jnp.int32, (nz * ROWS, tok), 0).astype(F32)
    pick = one_hot((slots == place0) | (slots == place1))
    side[...] = jnp.concatenate(
        [place0, place1, rw_t_ref[...], jnp.zeros((4, tok), F32)], axis=0
    )

    def stack_pieces(rows):
        return jnp.concatenate(
            [rows[:, q * sub_w : (q + 1) * sub_w] for q in range(SUB)], axis=0
        )

    def join_pieces(stacked):
        return jnp.concatenate(
            [stacked[q * ROWS : (q + 1) * ROWS, :] for q in range(SUB)], axis=1
        )

    def to_blocks(rows):
        blocks = dot(pout_ref[...], stack_pieces(rows)).astype(BF)
        return blocks.reshape(PL, ROWS, sub_w)

    def to_rows(blocks):
        flat = blocks.reshape(PL * ROWS, sub_w)
        return join_pieces(dot(pin_ref[...], flat).astype(BF))

    def dispatch(i, p):
        return pltpu.make_async_remote_copy(
            src_ref=outgoing.at[i, p],
            dst_ref=arr.at[mirror(i), p_me],
            send_sem=d_send.at[i],
            recv_sem=d_recv.at[mirror(i)],
            device_id=peer(plane(i), p),
            device_id_type=MESH,
        )

    def give_back(i, p):
        return pltpu.make_async_remote_copy(
            src_ref=ret_out.at[i, p],
            dst_ref=ret_in.at[mirror(i), p_me],
            send_sem=r_send.at[i],
            recv_sem=r_recv.at[mirror(i)],
            device_id=peer(plane(i), p),
            device_id_type=MESH,
        )

    def x_copy(src, dst, send, recv, to):
        return pltpu.make_async_remote_copy(
            src_ref=src, dst_ref=dst, send_sem=send, recv_sem=recv, device_id=to,
            device_id_type=MESH,
        )

    z_up = {"ep_0": lax.rem(z + 1, nz)}
    z_down = {"ep_0": lax.rem(z + nz - 1, nz)}

    def kv_z_up(k, to):
        return x_copy(kv.at[k, 0, 0], kv.at[to, 0, 0], kz_send.at[to, 0], kz_recv.at[to, 0], z_up)

    def kv_z_down(k, to):
        return x_copy(
            kv.at[k, 0, 0], kv.at[to, 0, 0], kz_send.at[to, 0], kz_recv.at[to, 0], z_down
        )

    last = nz - 1
    k_z_far = x_copy(
        kv.at[last - 2, 0, 0, 0], kv.at[last, 0, 0, 0], kz_send.at[last, 0], kz_recv.at[last, 0],
        z_up,
    )
    v_z_far = x_copy(
        kv.at[last - 1, 0, 0, 1], kv.at[last, 0, 0, 1], kz_send.at[last, 1], kz_recv.at[last, 1],
        z_down,
    )

    def each_plane(group, act):
        act(jnp.maximum(2 * group - 1, 0))

        @pl.when((group >= 1) & (group < nz // 2))
        def _():
            act(2 * group)

    def kv_up(k):
        return x_copy(kv.at[k, 0, 0], kv.at[k, 0, 1], ky_send.at[k, 0], ky_recv.at[k, 0], y_up)

    def kv_down(k):
        return x_copy(kv.at[k, 0, 0], kv.at[k, 0, 2], ky_send.at[k, 1], ky_recv.at[k, 1], y_down)

    def k_far(k):
        return x_copy(
            kv.at[k, 0, 1, 0], kv.at[k, 0, 3, 0], ky_send.at[k, 2], ky_recv.at[k, 2], y_up
        )

    def v_far(k):
        return x_copy(
            kv.at[k, 0, 2, 1], kv.at[k, 0, 3, 1], ky_send.at[k, 3], ky_recv.at[k, 3], y_down
        )

    def kv_across(k):
        return x_copy(kv.at[k, 0], kv.at[k, 1], kc_send.at[k], kc_recv.at[k], other_core)

    def attend(k):
        keys = kv[k, :, :, 0].reshape(-1, HEAD)
        vals = kv[k, :, :, 1].reshape(-1, HEAD)

        @pl.loop(0, HEADS)
        def _(h):
            scores = lax.dot_general(
                q_s[h], keys, (((1,), (1,)), ((), ())), preferred_element_type=F32
            ) * HEAD ** (-0.5)
            peak = jnp.maximum(m_s[h], jnp.max(scores, axis=1, keepdims=True))
            fade = jnp.exp(m_s[h] - peak)
            expo = jnp.exp(scores - peak[:, :1])
            m_s[h] = peak
            sums = l_s[h] * fade
            for c in range(expo.shape[1] // HEAD):
                sums = sums + expo[:, c * HEAD : (c + 1) * HEAD]
            l_s[h] = sums
            acc_s[h] = acc_s[h] * fade + dot(expo.astype(BF), vals)

    def project():
        for h in range(HEADS):
            total = jnp.sum(l_s[h], axis=1, keepdims=True)
            att_s[:, h * HEAD : (h + 1) * HEAD] = (acc_s[h] / total).astype(BF)
        share = att_s.shape[0] // TP
        ours = jnp.concatenate(
            [
                att_s[pl.ds(pl.multiple_of(lax.rem(x_me + o, TP) * share, share), share), :]
                for o in (0, 3, 1, 2)
            ],
            axis=0,
        )
        return dot(ours, ow[...]).astype(BF).reshape(TP, share, width)

    def to_plane(i, make):
        @pl.when(i == 0)
        def _():
            @pl.loop(1, PL)
            def _(j):
                make(i, lax.rem(p_me + j, PL)).start()

        @pl.when(i > 0)
        def _():
            @pl.loop(0, PL)
            def _(j):
                make(i, lax.rem(p_me + j, PL)).start()

    def wait_bytes(ref, sem):
        pltpu.make_async_copy(ref, ref, sem).wait()

    def wait_plane(i, ref, sem):
        @pl.when(i == 0)
        def _():
            wait_bytes(ref.at[0, pl.ds(0, PL - 1)], sem.at[0])

        @pl.when(i > 0)
        def _():
            wait_bytes(ref.at[i], sem.at[i])

    for i in range(nz):
        rows = dot(pick[i * ROWS : (i + 1) * ROWS, :], normed[...]).astype(BF)
        outgoing[i] = to_blocks(rows)
    arr[0, p_me] = outgoing[0, p_me]

    pl.semaphore_wait(barrier, n_exp - 1 + 2)
    to_plane(jnp.int32(MIRROR[FIRST[0]]), dispatch)
    kv_z_up(0, 1).start()
    kv_z_down(0, 2).start()
    kv_up(0).start()
    kv_down(0).start()

    for i in FIRST[1:]:
        to_plane(jnp.int32(MIRROR[i]), dispatch)

    cols_a, cols_b = pl.ds(0, half), pl.ds(half, half)

    def ag_right(k):
        return x_copy(xall.at[k, 0], xall.at[k, 1], ag_send.at[k, 0], ag_recv.at[k, 0], right)

    def ag_left(k):
        return x_copy(xall.at[k, 0], xall.at[k, 2], ag_send.at[k, 1], ag_recv.at[k, 1], left)

    def fwd_right(k):
        return x_copy(
            xall.at[k, 1, :, cols_a], xall.at[k, 3, :, cols_a],
            ag_send.at[k, 2], ag_recv.at[k, 2], right,
        )

    def fwd_left(k):
        return x_copy(
            xall.at[k, 2, :, cols_b], xall.at[k, 3, :, cols_b],
            ag_send.at[k, 3], ag_recv.at[k, 3], left,
        )

    def rs_far_left(k):
        return x_copy(
            part.at[k, 3, :, cols_a], rs1.at[k, 0], rs_send.at[k, 0], rs1_recv.at[k, 0], left
        )

    def rs_far_right(k):
        return x_copy(
            part.at[k, 3, :, cols_b], rs1.at[k, 1], rs_send.at[k, 1], rs1_recv.at[k, 1], right
        )

    def rs_near_left(k, c, s):
        return x_copy(
            part.at[k, 1, :, c], rs2.at[k, 1, :, c], rs_send.at[k, s], rs2_recv.at[k, s - 2], left
        )

    def rs_near_right(k, c, s):
        return x_copy(
            part.at[k, 2, :, c], rs2.at[k, 0, :, c], rs_send.at[k, s], rs2_recv.at[k, s - 2], right
        )

    def rs_copies(k):
        return (
            rs_far_left(k),
            rs_far_right(k),
            rs_near_left(k, cols_a, 2),
            rs_near_left(k, cols_b, 3),
            rs_near_right(k, cols_a, 4),
            rs_near_right(k, cols_b, 5),
        )

    def rs_start(k):
        rs_far_left(k).start()
        rs_far_right(k).start()
        rs_near_left(k, cols_b, 3).start()
        rs_near_right(k, cols_a, 4).start()

    def rs_total(k):
        for copy in rs_copies(k)[2:]:
            copy.wait_recv()
        return part[k, 0].astype(F32) + rs2[k, 0].astype(F32) + rs2[k, 1].astype(F32)

    def take_back(j):
        kk = mirror(j)
        wait_plane(kk, ret_in, r_recv)
        ret_rows[kk] = to_rows(ret_in[kk])

    @pl.loop(0, nz + 4)
    def _(step):
        @pl.when(step < nz)
        def _():
            k = step
            wait_plane(k, arr, d_recv)
            xall[k, 0] = to_rows(arr[k])
            ag_right(k).start()
            ag_left(k).start()
        @pl.when((step >= 1) & (step < nz + 1))
        def _():
            k = step - 1
            ag_right(k).wait_recv()
            fwd_right(k).start()
            ag_left(k).wait_recv()
            fwd_left(k).start()

        @pl.when((step >= 2) & (step < nz + 2))
        def _():
            k = step - 2
            fwd_right(k).wait_recv()
            fwd_left(k).wait_recv()

            @pl.when(step == 2)
            def _():
                for copy in w_copies:
                    copy.wait()

            rows = xall[k].reshape(4 * ROWS, width)
            pre = dot(rows, wgu[...])
            gate_cut = jnp.minimum(pre[:, :ff], clamp_limit)
            up_cut = jnp.clip(pre[:, ff:], -clamp_limit, clamp_limit)
            hidden = (
                (up_cut + 1.0) * gate_cut * (1.0 / (1.0 + jnp.exp(-sigmoid_slope * gate_cut)))
            ).astype(BF)
            part[k] = dot(hidden, wd[...]).astype(BF).reshape(4, ROWS, width)
            rs_start(k)

        def pass_on(k):
            rs_far_left(k).wait_recv()
            part[k, 1, :, cols_a] = (
                part[k, 1, :, cols_a].astype(F32) + rs1[k, 0].astype(F32)
            ).astype(BF)
            rs_near_left(k, cols_a, 2).start()
            rs_far_right(k).wait_recv()
            part[k, 2, :, cols_b] = (
                part[k, 2, :, cols_b].astype(F32) + rs1[k, 1].astype(F32)
            ).astype(BF)
            rs_near_right(k, cols_b, 5).start()

        @pl.when((step >= 3) & (step < nz + 3))
        def _():
            pass_on(step - 3)

        @pl.when(step == nz + 1)
        def _():
            part[nz] = project()
            rs_start(nz)

        @pl.when((step >= 1) & (step < nz // 2))
        def _():
            below, above = 2 * step - 1, 2 * step
            kv_z_up(0, below).wait_recv()
            kv_z_down(0, above).wait_recv()

            @pl.when(step < nz // 2 - 1)
            def _():
                kv_z_up(below, below + 2).start()
                kv_z_down(above, above + 2).start()

            @pl.when(step == nz // 2 - 1)
            def _():
                k_z_far.start()
                v_z_far.start()

            for j in (below, above):
                kv_up(j).start()
                kv_down(j).start()

        @pl.when(step == nz // 2)
        def _():
            k_z_far.wait_recv()
            v_z_far.wait_recv()
            kv_up(last).start()
            kv_down(last).start()

        for at, chunks in LATER.items():

            @pl.when(step == at)
            def _(chunks=chunks):
                for i in chunks:
                    to_plane(jnp.int32(MIRROR[i]), dispatch)

        @pl.when((step >= 1) & (step <= nz // 2 + 1))
        def _():
            def forward(j):
                kv_up(j).wait_recv()
                k_far(j).start()
                kv_down(j).wait_recv()
                v_far(j).start()

            each_plane(step - 1, forward)

        @pl.when((step >= 2) & (step <= nz // 2 + 2))
        def _():
            def across(j):
                k_far(j).wait_recv()
                v_far(j).wait_recv()
                kv_across(j).start()

            each_plane(step - 2, across)

        @pl.when((step >= 3) & (step <= nz // 2 + 3))
        def _():
            def attend_to(j):
                kv_across(j).wait_recv()
                attend(j)

            each_plane(step - 3, attend_to)

        @pl.when(step >= 4)
        def _():
            k = step - 4
            ret_out[k] = to_blocks(rs_total(k).astype(BF))

            @pl.when(k == 0)
            def _():
                ret_in[0, p_me] = ret_out[0, p_me]

            to_plane(k, give_back)

        @pl.when(step == nz + 2)
        def _():
            pass_on(nz)

        @pl.when(step >= nz - 1)
        def _():
            take_back(step - (nz - 1))

    mix_ref[...] = rms_scale(rs_total(nz), mg_ref[...]).astype(BF)

    for j in (5, 6, 7):
        take_back(jnp.int32(j))

    columns_of = side[...].T
    at0, at1, weight0, weight1 = (columns_of[:, c : c + 1] for c in range(4))
    lanes = lax.broadcasted_iota(jnp.int32, (tok, nz * ROWS), 1).astype(F32)
    take = jnp.concatenate([one_hot(lanes == at0), one_hot(lanes == at1)], axis=0)
    square = jnp.zeros((tok, 1), F32)
    block = min(512, width)
    for c in range(width // block):
        columns = slice(c * block, (c + 1) * block)
        both = dot(take, ret_rows[:, :, columns].reshape(nz * ROWS, block))
        mixed = weight0 * both[:tok] + weight1 * both[tok:]
        combined[:, columns] = mixed
        square = square + jnp.sum(mixed * mixed, axis=1, keepdims=True)
    scale = lax.rsqrt(square / width + norm_eps)
    out_ref[...] = (combined[...] * scale * fg_ref[...]).astype(BF)

    @pl.loop(0, nz)
    def _(k):
        wait_plane(k, outgoing, d_send)
        wait_plane(k, ret_out, r_send)
        ag_right(k).wait_send()
        ag_left(k).wait_send()
        fwd_right(k).wait_send()
        fwd_left(k).wait_send()
        kv_up(k).wait_send()
        kv_down(k).wait_send()
        k_far(k).wait_send()
        v_far(k).wait_send()
        kv_across(k).wait_send()

        @pl.when((k > 0) & (k < last))
        def _():
            kv_z_up(0, k).wait_send()

    k_z_far.wait_send()
    v_z_far.wait_send()

    @pl.loop(0, nz + 1)
    def _(k):
        for copy in rs_copies(k):
            copy.wait_send()


def permutation():
    source, piece, rank = np.meshgrid(
        np.arange(PL), np.arange(SUB), np.arange(CAP), indexing="ij"
    )
    travel = (source * SUB + piece) * CAP + rank
    rowwise = (piece * PL + source) * CAP + rank
    matrix = np.zeros((PL * ROWS, PL * ROWS), np.float32)
    matrix[rowwise.reshape(-1), travel.reshape(-1)] = 1.0
    return matrix


def turn_tables(rows):
    quarter = HEAD // 4
    inverse = rope_base ** (-np.arange(quarter, dtype=np.float64) / quarter)

    def table(count, make, at):
        angle = np.arange(count, dtype=np.float64)[:, None] * inverse[None, :]
        out = np.zeros((count, HEAD), np.float32)
        out[:, at : at + 2 * quarter] = make(angle)
        return jnp.asarray(out)

    def cosines(angle):
        return np.concatenate([np.cos(angle), np.cos(angle)], axis=1)

    def sines(angle):
        return np.concatenate([-np.sin(angle), np.sin(angle)], axis=1)

    return (
        table(rows, cosines, 0),
        table(rows, sines, 0),
        table(GRID_W, cosines, HEAD // 2),
        table(GRID_W, sines, HEAD // 2),
    )


def local(
    queries,
    keys,
    values,
    query_gain,
    key_gain,
    out_weight,
    mixer_gain,
    expert_in,
    routes,
    route_weights,
    expert_gain,
    gate_w,
    up_w,
    down_w,
    ffn_out_gain,
):
    nz = lax.axis_size("ep_0")
    assert nz == NZ
    tok, width = expert_in.shape
    ff = gate_w.shape[2]
    seq = queries.shape[0]
    tables = turn_tables(nz * PL * seq // GRID_W)
    matrix = permutation()
    pin = jnp.asarray(matrix, BF)
    pout = jnp.asarray(matrix.T, BF)
    vmem = pl.BlockSpec(memory_space=pltpu.VMEM)
    hbm = pl.BlockSpec(memory_space=pl.ANY)
    travel = (nz, PL, ROWS, width // SUB)
    dma = pltpu.SemaphoreType.DMA
    operands = (
        expert_in,
        routes.T,
        route_weights.T,
        expert_gain[None, :],
        ffn_out_gain[None, :],
        pin,
        pout,
        queries,
        keys,
        values,
        query_gain[None, :],
        key_gain[None, :],
        mixer_gain[None, :],
        *tables,
    )
    assert len(operands) == OPERANDS
    return pl.pallas_call(
        functools.partial(layer_kernel, nz),
        out_shape=(
            jax.ShapeDtypeStruct((seq // TP, width), BF),
            jax.ShapeDtypeStruct((tok, width), BF),
        ),
        in_specs=[hbm] * (OPERANDS + 4),
        out_specs=(vmem, vmem),
        scratch_shapes=[pltpu.VMEM(a.shape, a.dtype) for a in operands]
        + [
            pltpu.VMEM((tok, width), BF),
            pltpu.VMEM(travel, BF),
            pltpu.VMEM(travel, BF),
            pltpu.VMEM((nz, 4, ROWS, width), BF),
            pltpu.VMEM((nz + 1, 4, ROWS, width), BF),
            pltpu.VMEM((nz + 1, 2, ROWS, width // 2), BF),
            pltpu.VMEM((nz + 1, 2, ROWS, width), BF),
            pltpu.VMEM(travel, BF),
            pltpu.VMEM(travel, BF),
            pltpu.VMEM((nz, ROWS, width), BF),
            pltpu.VMEM((width, 2 * ff), BF),
            pltpu.VMEM((ff, width), BF),
            pltpu.VMEM((tok, width), F32),
            pltpu.VMEM(out_weight.shape, BF),
            pltpu.VMEM((nz, 2, 4, 2, seq, HEAD), BF),
            pltpu.VMEM((8, tok), F32),
            pltpu.VMEM((HEADS, seq, HEAD), BF),
            pltpu.VMEM((HEADS, seq, HEAD), F32),
            pltpu.VMEM((HEADS, seq, HEAD), F32),
            pltpu.VMEM((HEADS, seq, HEAD), F32),
            pltpu.VMEM((seq, HEADS * HEAD), BF),
            dma((4,)),
            dma((nz,)),
            dma((nz,)),
            dma((nz, 4)),
            dma((nz, 4)),
            dma((nz + 1, 6)),
            dma((nz + 1, 2)),
            dma((nz + 1, 4)),
            dma((nz,)),
            dma((nz,)),
            dma((nz, 2)),
            dma((nz, 2)),
            dma((nz, 4)),
            dma((nz, 4)),
            dma((nz,)),
            dma((nz,)),
            dma((OPERANDS,)),
        ],
        compiler_params=pltpu.CompilerParams(
            collective_id=0, has_side_effects=True, vmem_limit_bytes=62 * 2**20
        ),
        name="layer",
    )(
        *operands,
        gate_w,
        up_w,
        down_w,
        out_weight,
    )


def solution(mesh):
    split = Mesh(
        mesh.devices.reshape(mesh.shape["ep"] // 8, 4, 2, mesh.shape["tp"]),
        ("ep_0", "ep_1", "ep_2", "tp"),
    )
    return jax.shard_map(
        local,
        mesh=split,
        in_specs=(
            P(EP, "tp"),
            P(EP, "tp"),
            P(EP, "tp"),
            P(),
            P(),
            P("tp", None),
            P(),
            P(EP_TP, None),
            P(EP_TP, None),
            P(EP_TP, None),
            P(),
            P(EP, None, "tp"),
            P(EP, None, "tp"),
            P(EP, "tp", None),
            P(),
        ),
        out_specs=(P(EP_TP, None), P(EP_TP, None)),
        check_vma=False,
    )
```

```python
import functools

import jax
import jax.numpy as jnp
import numpy as np
from jax import lax
from jax.experimental import pallas as pl
from jax.experimental.pallas import tpu as pltpu
from jax.sharding import Mesh
from jax.sharding import PartitionSpec as P

HEAD = 128
HEADS = 4
GRID_W = 64
TP = 4
OPERANDS = 17
EP = ("ep_0", "ep_1", "ep_2")
EP_TP = ("ep_0", "ep_1", "ep_2", "tp")
MESH = pl.DeviceIdType.MESH
BF = jnp.bfloat16
F32 = jnp.float32

norm_eps = 1e-06
rope_base = 10000.0
clamp_limit = 7.0
sigmoid_slope = 1.702

PL = 8
CAP = 6
SUB = 8
ROWS = PL * CAP
AWAY = (0, 1, -3, 3, -2, 4, 2, -1)
NZ = len(AWAY)
FIRST = (1, 2)
LATER = {0: (3,), 1: (4,), 2: (5, 7), 3: (6,)}
INDEX = [[a % NZ for a in AWAY].index(d) for d in range(NZ)]
MIRROR = [INDEX[-a % NZ] for a in AWAY]


def rms_scale(values_in, gain):
    return (
        values_in
        * lax.rsqrt(jnp.mean(values_in * values_in, axis=-1, keepdims=True) + norm_eps)
        * gain
    )


def dot(a, b):
    return jnp.dot(a, b, preferred_element_type=F32)


def one_hot(cond):
    return jnp.where(cond, 1.0, 0.0).astype(BF)


def layer_kernel(nz, *refs):
    ours = refs[:OPERANDS]
    held = refs[OPERANDS + 6 : 2 * OPERANDS + 6]
    sems = refs[-1]
    copies = [
        pltpu.make_async_copy(src, dst, sems.at[i])
        for i, (src, dst) in enumerate(zip(ours, held))
    ]
    for copy in copies:
        copy.start()

    def operands_here():
        for copy in copies:
            copy.wait()

    layer(nz, operands_here, *held, *refs[OPERANDS : OPERANDS + 6], *refs[2 * OPERANDS + 6 : -1])


def layer(
    nz,
    operands_here,
    x_ref,
    routes_t_ref,
    rw_t_ref,
    eg_ref,
    fg_ref,
    pin_ref,
    pout_ref,
    q_ref,
    k_ref,
    v_ref,
    qg_ref,
    kg_ref,
    mg_ref,
    cos_row_ref,
    sin_row_ref,
    cos_col_ref,
    sin_col_ref,
    gate_hbm,
    up_hbm,
    down_hbm,
    ow_hbm,
    mix_ref,
    out_ref,
    normed,
    outgoing,
    arr,
    xall,
    part,
    rs1,
    rs2,
    ret_out,
    ret_in,
    ret_rows,
    wgu,
    wd,
    combined,
    ow,
    kv,
    side,
    q_s,
    m_s,
    l_s,
    acc_s,
    att_s,
    w_sem,
    d_send,
    d_recv,
    ag_send,
    ag_recv,
    rs_send,
    rs1_recv,
    rs2_recv,
    r_send,
    r_recv,
    kz_send,
    kz_recv,
    ky_send,
    ky_recv,
    kc_send,
    kc_recv,
):
    z = lax.axis_index("ep_0")
    p_me = lax.axis_index("ep_1") * 2 + lax.axis_index("ep_2")
    x_me = lax.axis_index("tp")
    right = {"tp": lax.rem(x_me + 1, 4)}
    left = {"tp": lax.rem(x_me + 3, 4)}
    y_me = lax.axis_index("ep_1")
    y_up = {"ep_1": lax.rem(y_me + 1, 4)}
    y_down = {"ep_1": lax.rem(y_me + 3, 4)}
    other_core = {"ep_2": 1 - lax.axis_index("ep_2")}
    tok, width = x_ref.shape
    half = width // 2
    sub_w = width // SUB
    ff = wd.shape[0]
    n_exp = nz * PL

    def peer(zz, p):
        return {"ep_0": zz, "ep_1": lax.div(p, 2), "ep_2": lax.rem(p, 2)}

    def entry(values, i):
        found = jnp.full(jnp.shape(i), values[0], jnp.int32)
        for j in range(1, nz):
            found = jnp.where(i == j, values[j], found)
        return found

    def plane(i):
        return lax.rem(z + entry([a % nz for a in AWAY], i), nz)

    def mirror(i):
        return entry(MIRROR, i)

    barrier = pltpu.get_barrier_semaphore()

    def greet(device):
        pl.semaphore_signal(barrier, inc=1, device_id=device, device_id_type=MESH)

    greet(left)
    greet(right)
    for j in range(1, PL):
        greet(peer(z, lax.rem(p_me + j, PL)))

    @pl.loop(1, nz)
    def _(d):
        zz = lax.rem(z + d, nz)
        for j in range(PL):
            greet(peer(zz, lax.rem(p_me + j, PL)))

    w_copies = [
        pltpu.make_async_copy(gate_hbm.at[0], wgu.at[:, pl.ds(0, ff)], w_sem.at[0]),
        pltpu.make_async_copy(up_hbm.at[0], wgu.at[:, pl.ds(ff, ff)], w_sem.at[1]),
        pltpu.make_async_copy(down_hbm.at[0], wd, w_sem.at[2]),
        pltpu.make_async_copy(ow_hbm, ow, w_sem.at[3]),
    ]
    for copy in w_copies:
        copy.start()

    operands_here()
    xf = x_ref[...].astype(F32)
    normed[...] = rms_scale(xf, eg_ref[...]).astype(BF)

    def base_of(e):
        o = (lax.shift_right_logical(e, 3) - z + nz) & (nz - 1)
        return entry(INDEX, o) * ROWS + (e & 7) * CAP

    e_rows = lax.broadcasted_iota(jnp.int32, (n_exp, tok), 0)
    t_a = lax.broadcasted_iota(jnp.int32, (tok, tok), 0)
    t_b = lax.broadcasted_iota(jnp.int32, (tok, tok), 1)
    before_t = one_hot(t_a < t_b)
    oh0 = e_rows == routes_t_ref[0:1, :]
    oh1 = e_rows == routes_t_ref[1:2, :]
    rank0 = dot(one_hot(oh0), before_t)
    rank1 = dot(one_hot(oh1), before_t) + jnp.sum(
        jnp.where(oh0, 1.0, 0.0), axis=1, keepdims=True
    )
    base = base_of(e_rows).astype(F32)
    place0 = jnp.sum(jnp.where(oh0, base + rank0, 0.0), axis=0, keepdims=True)
    place1 = jnp.sum(jnp.where(oh1, base + rank1, 0.0), axis=0, keepdims=True)
    slots = lax.broadcasted_iota(jnp.int32, (nz * ROWS, tok), 0).astype(F32)
    pick = one_hot((slots == place0) | (slots == place1))
    side[...] = jnp.concatenate(
        [place0, place1, rw_t_ref[...], jnp.zeros((4, tok), F32)], axis=0
    )

    def stack_pieces(rows):
        return jnp.concatenate(
            [rows[:, q * sub_w : (q + 1) * sub_w] for q in range(SUB)], axis=0
        )

    def join_pieces(stacked):
        return jnp.concatenate(
            [stacked[q * ROWS : (q + 1) * ROWS, :] for q in range(SUB)], axis=1
        )

    def to_blocks(rows):
        blocks = dot(pout_ref[...], stack_pieces(rows)).astype(BF)
        return blocks.reshape(PL, ROWS, sub_w)

    def to_rows(blocks):
        flat = blocks.reshape(PL * ROWS, sub_w)
        return join_pieces(dot(pin_ref[...], flat).astype(BF))

    def dispatch(i, p):
        return pltpu.make_async_remote_copy(
            src_ref=outgoing.at[i, p],
            dst_ref=arr.at[mirror(i), p_me],
            send_sem=d_send.at[jnp.minimum(i, 1)],
            recv_sem=d_recv.at[mirror(i)],
            device_id=peer(plane(i), p),
            device_id_type=MESH,
        )

    def give_back(i, p):
        return pltpu.make_async_remote_copy(
            src_ref=ret_out.at[i, p],
            dst_ref=ret_in.at[mirror(i), p_me],
            send_sem=r_send.at[jnp.minimum(i, 1)],
            recv_sem=r_recv.at[mirror(i)],
            device_id=peer(plane(i), p),
            device_id_type=MESH,
        )

    def x_copy(src, dst, send, recv, to):
        return pltpu.make_async_remote_copy(
            src_ref=src, dst_ref=dst, send_sem=send, recv_sem=recv, device_id=to,
            device_id_type=MESH,
        )

    z_up = {"ep_0": lax.rem(z + 1, nz)}
    z_down = {"ep_0": lax.rem(z + nz - 1, nz)}

    def kv_z_up(k, to):
        return x_copy(kv.at[k, 0, 0], kv.at[to, 0, 0], kz_send.at[0], kz_recv.at[to, 0], z_up)

    def kv_z_down(k, to):
        return x_copy(
            kv.at[k, 0, 0], kv.at[to, 0, 0], kz_send.at[0], kz_recv.at[to, 0], z_down
        )

    last = nz - 1
    k_z_far = x_copy(
        kv.at[last - 2, 0, 0, 0], kv.at[last, 0, 0, 0], kz_send.at[0], kz_recv.at[last, 0],
        z_up,
    )
    v_z_far = x_copy(
        kv.at[last - 1, 0, 0, 1], kv.at[last, 0, 0, 1], kz_send.at[0], kz_recv.at[last, 1],
        z_down,
    )

    def each_plane(group, act):
        act(jnp.maximum(2 * group - 1, 0))

        @pl.when((group >= 1) & (group < nz // 2))
        def _():
            act(2 * group)

    def kv_up(k):
        return x_copy(kv.at[k, 0, 0], kv.at[k, 0, 1], ky_send.at[0], ky_recv.at[k, 0], y_up)

    def kv_down(k):
        return x_copy(kv.at[k, 0, 0], kv.at[k, 0, 2], ky_send.at[0], ky_recv.at[k, 1], y_down)

    def k_far(k):
        return x_copy(
            kv.at[k, 0, 1, 0], kv.at[k, 0, 3, 0], ky_send.at[0], ky_recv.at[k, 2], y_up
        )

    def v_far(k):
        return x_copy(
            kv.at[k, 0, 2, 1], kv.at[k, 0, 3, 1], ky_send.at[0], ky_recv.at[k, 3], y_down
        )

    def kv_across(k):
        return x_copy(kv.at[k, 0], kv.at[k, 1], kc_send.at[0], kc_recv.at[k], other_core)

    def attend(k):
        keys = kv[k, :, :, 0].reshape(-1, HEAD)
        vals = kv[k, :, :, 1].reshape(-1, HEAD)

        @pl.loop(0, HEADS)
        def _(h):
            scores = lax.dot_general(
                q_s[h], keys, (((1,), (1,)), ((), ())), preferred_element_type=F32
            ) * HEAD ** (-0.5)
            peak = jnp.maximum(m_s[h], jnp.max(scores, axis=1, keepdims=True))
            fade = jnp.exp(m_s[h] - peak)
            expo = jnp.exp(scores - peak[:, :1])
            m_s[h] = peak
            sums = l_s[h] * fade
            for c in range(expo.shape[1] // HEAD):
                sums = sums + expo[:, c * HEAD : (c + 1) * HEAD]
            l_s[h] = sums
            acc_s[h] = acc_s[h] * fade + dot(expo.astype(BF), vals)

    def project():
        for h in range(HEADS):
            total = jnp.sum(l_s[h], axis=1, keepdims=True)
            att_s[:, h * HEAD : (h + 1) * HEAD] = (acc_s[h] / total).astype(BF)
        share = att_s.shape[0] // TP
        ours = jnp.concatenate(
            [
                att_s[pl.ds(pl.multiple_of(lax.rem(x_me + o, TP) * share, share), share), :]
                for o in (0, 3, 1, 2)
            ],
            axis=0,
        )
        return dot(ours, ow[...]).astype(BF).reshape(TP, share, width)

    def to_plane(i, make):
        @pl.when(i == 0)
        def _():
            @pl.loop(1, PL)
            def _(j):
                make(i, lax.rem(p_me + j, PL)).start()

        @pl.when(i > 0)
        def _():
            @pl.loop(0, PL)
            def _(j):
                make(i, lax.rem(p_me + j, PL)).start()

    def wait_bytes(ref, sem):
        pltpu.make_async_copy(ref, ref, sem).wait()

    def wait_plane(i, ref, sem):
        @pl.when(i == 0)
        def _():
            wait_bytes(ref.at[0, pl.ds(0, PL - 1)], sem.at[0])

        @pl.when(i > 0)
        def _():
            wait_bytes(ref.at[i], sem.at[i])

    def gather(i):
        rows = dot(pick[i * ROWS : (i + 1) * ROWS, :], normed[...]).astype(BF)
        outgoing[i] = to_blocks(rows)

    gather(0)
    pl.semaphore_wait(barrier, n_exp - 1 + 2)
    to_plane(jnp.int32(0), dispatch)
    arr[0, p_me] = outgoing[0, p_me]

    for c in FIRST:
        gather(MIRROR[c])
        to_plane(jnp.int32(MIRROR[c]), dispatch)

    grid_rows = k_ref.shape[0] // GRID_W
    first_row = (z * PL + p_me) * grid_rows
    cosine = jnp.concatenate(
        [cos_row_ref[pl.ds(first_row + g, 1), :] + cos_col_ref[...] for g in range(grid_rows)],
        axis=0,
    )
    sine = jnp.concatenate(
        [sin_row_ref[pl.ds(first_row + g, 1), :] + sin_col_ref[...] for g in range(grid_rows)],
        axis=0,
    )
    lane = lax.broadcasted_iota(jnp.int32, cosine.shape, 1)
    first_of_pair = (lane & 32) == 0

    def normed_and_turned(head, gain):
        field = rms_scale(head.astype(F32), gain)
        swapped = jnp.where(
            first_of_pair, pltpu.roll(field, HEAD - 32, 1), pltpu.roll(field, 32, 1)
        )
        return (field * cosine + swapped * sine).astype(BF)

    kv[0, 0, 0, 0] = normed_and_turned(k_ref[...], kg_ref[...])
    kv[0, 0, 0, 1] = v_ref[...]
    kv_z_up(0, 1).start()
    kv_z_down(0, 2).start()
    kv_up(0).start()
    kv_down(0).start()

    for c in range(1, nz):
        if c not in FIRST:
            gather(MIRROR[c])

    for h in range(HEADS):
        q_s[h] = normed_and_turned(q_ref[:, h * HEAD : (h + 1) * HEAD], qg_ref[...])
    m_s[...] = jnp.full(m_s.shape, -1e30, F32)
    l_s[...] = jnp.zeros(l_s.shape, F32)
    acc_s[...] = jnp.zeros(acc_s.shape, F32)

    cols_a, cols_b = pl.ds(0, half), pl.ds(half, half)

    def ag_right(k):
        return x_copy(xall.at[k, 0], xall.at[k, 1], ag_send.at[0], ag_recv.at[k, 0], right)

    def ag_left(k):
        return x_copy(xall.at[k, 0], xall.at[k, 2], ag_send.at[0], ag_recv.at[k, 1], left)

    def fwd_right(k):
        return x_copy(
            xall.at[k, 1, :, cols_a], xall.at[k, 3, :, cols_a],
            ag_send.at[0], ag_recv.at[k, 2], right,
        )

    def fwd_left(k):
        return x_copy(
            xall.at[k, 2, :, cols_b], xall.at[k, 3, :, cols_b],
            ag_send.at[0], ag_recv.at[k, 3], left,
        )

    def rs_far_left(k):
        return x_copy(
            part.at[k, 3, :, cols_a], rs1.at[k, 0], rs_send.at[0], rs1_recv.at[k, 0], left
        )

    def rs_far_right(k):
        return x_copy(
            part.at[k, 3, :, cols_b], rs1.at[k, 1], rs_send.at[0], rs1_recv.at[k, 1], right
        )

    def rs_near_left(k, c, s):
        return x_copy(
            part.at[k, 1, :, c], rs2.at[k, 1, :, c], rs_send.at[0], rs2_recv.at[k, s - 2], left
        )

    def rs_near_right(k, c, s):
        return x_copy(
            part.at[k, 2, :, c], rs2.at[k, 0, :, c], rs_send.at[0], rs2_recv.at[k, s - 2], right
        )

    def rs_copies(k):
        return (
            rs_far_left(k),
            rs_far_right(k),
            rs_near_left(k, cols_a, 2),
            rs_near_left(k, cols_b, 3),
            rs_near_right(k, cols_a, 4),
            rs_near_right(k, cols_b, 5),
        )

    def rs_far(k):
        rs_far_left(k).start()
        rs_far_right(k).start()

    def rs_near(k):
        rs_near_left(k, cols_b, 3).start()
        rs_near_right(k, cols_a, 4).start()

    def rs_total(k):
        for copy in rs_copies(k)[2:]:
            copy.wait_recv()
        return part[k, 0].astype(F32) + rs2[k, 0].astype(F32) + rs2[k, 1].astype(F32)

    def take_back(j):
        kk = mirror(j)
        wait_plane(kk, ret_in, r_recv)
        ret_rows[kk] = to_rows(ret_in[kk])

    @pl.loop(0, nz + 4)
    def _(step):
        @pl.when(step < nz)
        def _():
            k = step
            wait_plane(k, arr, d_recv)
            xall[k, 0] = to_rows(arr[k])
            ag_right(k).start()
            ag_left(k).start()
        @pl.when((step >= 1) & (step < nz + 1))
        def _():
            k = step - 1
            ag_right(k).wait_recv()
            fwd_right(k).start()
            ag_left(k).wait_recv()
            fwd_left(k).start()

        @pl.when((step >= 2) & (step < nz + 2))
        def _():
            k = step - 2
            fwd_right(k).wait_recv()
            fwd_left(k).wait_recv()

            @pl.when(step == 2)
            def _():
                for copy in w_copies:
                    copy.wait()

            rows = xall[k].reshape(4 * ROWS, width)
            pre = dot(rows, wgu[...])
            gate_cut = jnp.minimum(pre[:, :ff], clamp_limit)
            up_cut = jnp.clip(pre[:, ff:], -clamp_limit, clamp_limit)
            hidden = (
                (up_cut + 1.0) * gate_cut * (1.0 / (1.0 + jnp.exp(-sigmoid_slope * gate_cut)))
            ).astype(BF)
            part[k] = dot(hidden, wd[...]).astype(BF).reshape(4, ROWS, width)
            rs_far(k)

        def pass_on(k):
            rs_far_left(k).wait_recv()
            part[k, 1, :, cols_a] = (
                part[k, 1, :, cols_a].astype(F32) + rs1[k, 0].astype(F32)
            ).astype(BF)
            rs_near_left(k, cols_a, 2).start()
            rs_far_right(k).wait_recv()
            part[k, 2, :, cols_b] = (
                part[k, 2, :, cols_b].astype(F32) + rs1[k, 1].astype(F32)
            ).astype(BF)
            rs_near_right(k, cols_b, 5).start()

        @pl.when((step >= 3) & (step < nz + 3))
        def _():
            pass_on(step - 3)

        @pl.when((step >= 2) & (step < nz + 2))
        def _():
            rs_near(step - 2)

        @pl.when(step == nz + 2)
        def _():
            rs_far(nz)
            rs_near(nz)

        @pl.when((step >= 2) & (step <= nz // 2))
        def _():
            below, above = 2 * step - 3, 2 * step - 2
            kv_z_up(0, below).wait_recv()
            kv_z_down(0, above).wait_recv()

            @pl.when(step < nz // 2)
            def _():
                kv_z_up(below, below + 2).start()
                kv_z_down(above, above + 2).start()

            @pl.when(step == nz // 2)
            def _():
                k_z_far.start()
                v_z_far.start()

            for j in (below, above):
                kv_up(j).start()
                kv_down(j).start()

        @pl.when(step == nz // 2 + 1)
        def _():
            k_z_far.wait_recv()
            v_z_far.wait_recv()
            kv_up(last).start()
            kv_down(last).start()

        for at, chunks in LATER.items():

            @pl.when(step == at)
            def _(chunks=chunks):
                for i in chunks:
                    to_plane(jnp.int32(MIRROR[i]), dispatch)

        @pl.when((step >= 2) & (step <= nz // 2 + 2))
        def _():
            def forward(j):
                kv_up(j).wait_recv()
                k_far(j).start()
                kv_down(j).wait_recv()
                v_far(j).start()

            each_plane(step - 2, forward)

        @pl.when((step >= 3) & (step <= nz // 2 + 3))
        def _():
            def across(j):
                k_far(j).wait_recv()
                v_far(j).wait_recv()
                kv_across(j).start()

            each_plane(step - 3, across)

        @pl.when((step >= 4) & (step <= nz // 2 + 4))
        def _():
            def attend_to(j):
                kv_across(j).wait_recv()
                attend(j)

            each_plane(step - 4, attend_to)

        @pl.when(step >= 4)
        def _():
            k = step - 4
            ret_out[k] = to_blocks(rs_total(k).astype(BF))

            @pl.when(k == 0)
            def _():
                ret_in[0, p_me] = ret_out[0, p_me]

            to_plane(k, give_back)

        @pl.when(step == nz)
        def _():
            part[nz] = project()

        @pl.when(step == nz + 3)
        def _():
            pass_on(nz)

        @pl.when(step >= nz - 1)
        def _():
            take_back(step - (nz - 1))

    mix_ref[...] = rms_scale(rs_total(nz), mg_ref[...]).astype(BF)

    for j in (5, 6, 7):
        take_back(jnp.int32(j))

    columns_of = side[...].T
    at0, at1, weight0, weight1 = (columns_of[:, c : c + 1] for c in range(4))
    lanes = lax.broadcasted_iota(jnp.int32, (tok, nz * ROWS), 1).astype(F32)
    take = jnp.concatenate([one_hot(lanes == at0), one_hot(lanes == at1)], axis=0)
    square = jnp.zeros((tok, 1), F32)
    block = min(512, width)
    for c in range(width // block):
        columns = slice(c * block, (c + 1) * block)
        both = dot(take, ret_rows[:, :, columns].reshape(nz * ROWS, block))
        mixed = weight0 * both[:tok] + weight1 * both[tok:]
        combined[:, columns] = mixed
        square = square + jnp.sum(mixed * mixed, axis=1, keepdims=True)
    scale = lax.rsqrt(square / width + norm_eps)
    out_ref[...] = (combined[...] * scale * fg_ref[...]).astype(BF)

    for blocks, sems in ((outgoing, d_send), (ret_out, r_send)):
        wait_bytes(blocks.at[0, pl.ds(0, PL - 1)], sems.at[0])
        wait_bytes(blocks.at[pl.ds(1, nz - 1)], sems.at[1])
    wait_bytes(xall.at[:, pl.ds(0, 3)], ag_send.at[0])
    wait_bytes(part.at[:, pl.ds(0, 3)], rs_send.at[0])
    wait_bytes(kv.at[pl.ds(0, nz - 1), 0, 0], kz_send.at[0])
    wait_bytes(kv.at[:, 0, pl.ds(0, 3)], ky_send.at[0])
    wait_bytes(kv.at[:, 0], kc_send.at[0])


def hand_over(mix_hbm, rows_hbm, mix_out, rows_out, mix_v, rows_v, sems):
    taken = [
        pltpu.make_async_copy(mix_hbm, mix_v, sems.at[0]),
        pltpu.make_async_copy(rows_hbm, rows_v, sems.at[1]),
    ]
    given = [
        pltpu.make_async_copy(mix_v, mix_out, sems.at[2]),
        pltpu.make_async_copy(rows_v, rows_out, sems.at[3]),
    ]
    for copy in taken:
        copy.start()
    for here, there in zip(taken, given):
        here.wait()
        there.start()
    for copy in given:
        copy.wait()


def permutation():
    source, piece, rank = np.meshgrid(
        np.arange(PL), np.arange(SUB), np.arange(CAP), indexing="ij"
    )
    travel = (source * SUB + piece) * CAP + rank
    rowwise = (piece * PL + source) * CAP + rank
    matrix = np.zeros((PL * ROWS, PL * ROWS), np.float32)
    matrix[rowwise.reshape(-1), travel.reshape(-1)] = 1.0
    return matrix


def turn_tables(rows):
    quarter = HEAD // 4
    inverse = rope_base ** (-np.arange(quarter, dtype=np.float64) / quarter)

    def table(count, make, at):
        angle = np.arange(count, dtype=np.float64)[:, None] * inverse[None, :]
        out = np.zeros((count, HEAD), np.float32)
        out[:, at : at + 2 * quarter] = make(angle)
        return jnp.asarray(out)

    def cosines(angle):
        return np.concatenate([np.cos(angle), np.cos(angle)], axis=1)

    def sines(angle):
        return np.concatenate([-np.sin(angle), np.sin(angle)], axis=1)

    return (
        table(rows, cosines, 0),
        table(rows, sines, 0),
        table(GRID_W, cosines, HEAD // 2),
        table(GRID_W, sines, HEAD // 2),
    )


def local(
    queries,
    keys,
    values,
    query_gain,
    key_gain,
    out_weight,
    mixer_gain,
    expert_in,
    routes,
    route_weights,
    expert_gain,
    gate_w,
    up_w,
    down_w,
    ffn_out_gain,
):
    nz = lax.axis_size("ep_0")
    assert nz == NZ
    tok, width = expert_in.shape
    ff = gate_w.shape[2]
    seq = queries.shape[0]
    tables = turn_tables(nz * PL * seq // GRID_W)
    matrix = permutation()
    pin = jnp.asarray(matrix, BF)
    pout = jnp.asarray(matrix.T, BF)
    vmem = pl.BlockSpec(memory_space=pltpu.VMEM)
    hbm = pl.BlockSpec(memory_space=pl.ANY)
    travel = (nz, PL, ROWS, width // SUB)
    dma = pltpu.SemaphoreType.DMA
    operands = (
        expert_in,
        routes.T,
        route_weights.T,
        expert_gain[None, :],
        ffn_out_gain[None, :],
        pin,
        pout,
        queries,
        keys,
        values,
        query_gain[None, :],
        key_gain[None, :],
        mixer_gain[None, :],
        *tables,
    )
    assert len(operands) == OPERANDS
    made = pl.pallas_call(
        functools.partial(layer_kernel, nz),
        out_shape=(
            jax.ShapeDtypeStruct((seq // TP, width), BF),
            jax.ShapeDtypeStruct((tok, width), BF),
        ),
        in_specs=[hbm] * (OPERANDS + 4),
        out_specs=(vmem, vmem),
        scratch_shapes=[pltpu.VMEM(a.shape, a.dtype) for a in operands]
        + [
            pltpu.VMEM((tok, width), BF),
            pltpu.VMEM(travel, BF),
            pltpu.VMEM(travel, BF),
            pltpu.VMEM((nz, 4, ROWS, width), BF),
            pltpu.VMEM((nz + 1, 4, ROWS, width), BF),
            pltpu.VMEM((nz + 1, 2, ROWS, width // 2), BF),
            pltpu.VMEM((nz + 1, 2, ROWS, width), BF),
            pltpu.VMEM(travel, BF),
            pltpu.VMEM(travel, BF),
            pltpu.VMEM((nz, ROWS, width), BF),
            pltpu.VMEM((width, 2 * ff), BF),
            pltpu.VMEM((ff, width), BF),
            pltpu.VMEM((tok, width), F32),
            pltpu.VMEM(out_weight.shape, BF),
            pltpu.VMEM((nz, 2, 4, 2, seq, HEAD), BF),
            pltpu.VMEM((8, tok), F32),
            pltpu.VMEM((HEADS, seq, HEAD), BF),
            pltpu.VMEM((HEADS, seq, HEAD), F32),
            pltpu.VMEM((HEADS, seq, HEAD), F32),
            pltpu.VMEM((HEADS, seq, HEAD), F32),
            pltpu.VMEM((seq, HEADS * HEAD), BF),
            dma((4,)),
            dma((2,)),
            dma((nz,)),
            dma((1,)),
            dma((nz, 4)),
            dma((1,)),
            dma((nz + 1, 2)),
            dma((nz + 1, 4)),
            dma((2,)),
            dma((nz,)),
            dma((1,)),
            dma((nz, 2)),
            dma((1,)),
            dma((nz, 4)),
            dma((1,)),
            dma((nz,)),
            dma((OPERANDS,)),
        ],
        compiler_params=pltpu.CompilerParams(
            collective_id=0, has_side_effects=True, vmem_limit_bytes=62 * 2**20
        ),
        name="layer",
    )(
        *operands,
        gate_w,
        up_w,
        down_w,
        out_weight,
    )
    return tuple(
        pl.pallas_call(
            hand_over,
            out_shape=tuple(jax.ShapeDtypeStruct(a.shape, a.dtype) for a in made),
            in_specs=[hbm] * 2,
            out_specs=(hbm, hbm),
            scratch_shapes=[pltpu.VMEM(a.shape, a.dtype) for a in made] + [dma((4,))],
            name="hand_over",
        )(*made)
    )


def solution(mesh):
    split = Mesh(
        mesh.devices.reshape(mesh.shape["ep"] // 8, 4, 2, mesh.shape["tp"]),
        ("ep_0", "ep_1", "ep_2", "tp"),
    )
    return jax.shard_map(
        local,
        mesh=split,
        in_specs=(
            P(EP, "tp"),
            P(EP, "tp"),
            P(EP, "tp"),
            P(),
            P(),
            P("tp", None),
            P(),
            P(EP_TP, None),
            P(EP_TP, None),
            P(EP_TP, None),
            P(),
            P(EP, None, "tp"),
            P(EP, None, "tp"),
            P(EP, "tp", None),
            P(),
        ),
        out_specs=(P(EP_TP, None), P(EP_TP, None)),
        check_vma=False,
    )
```

```python
import functools

import jax
import jax.numpy as jnp
import numpy as np
from jax import lax
from jax.experimental import pallas as pl
from jax.experimental.pallas import tpu as pltpu
from jax.sharding import Mesh
from jax.sharding import PartitionSpec as P

HEAD = 128
HEADS = 4
GRID_W = 64
TP = 4
OPERANDS = 17
EP = ("ep_0", "ep_1", "ep_2")
EP_TP = ("ep_0", "ep_1", "ep_2", "tp")
MESH = pl.DeviceIdType.MESH
BF = jnp.bfloat16
F32 = jnp.float32

norm_eps = 1e-06
rope_base = 10000.0
clamp_limit = 7.0
sigmoid_slope = 1.702

PL = 8
CAP = 6
SUB = 8
ROWS = PL * CAP
AWAY = (0, 1, -2, 3, 4, -3, 2, -1)
NZ = len(AWAY)
FIRST = (1, 2, 3)
LATER = {0: (4,), 2: (5,), 3: (6, 7)}
INDEX = [[a % NZ for a in AWAY].index(d) for d in range(NZ)]
MIRROR = [INDEX[-a % NZ] for a in AWAY]


def rms_scale(values_in, gain):
    return (
        values_in
        * lax.rsqrt(jnp.mean(values_in * values_in, axis=-1, keepdims=True) + norm_eps)
        * gain
    )


def dot(a, b):
    return jnp.dot(a, b, preferred_element_type=F32)


def one_hot(cond):
    return jnp.where(cond, 1.0, 0.0).astype(BF)


def layer_kernel(nz, *refs):
    ours = refs[:OPERANDS]
    held = refs[OPERANDS + 6 : 2 * OPERANDS + 6]
    sems = refs[-1]
    copies = [
        pltpu.make_async_copy(src, dst, sems.at[i])
        for i, (src, dst) in enumerate(zip(ours, held))
    ]
    for copy in copies:
        copy.start()

    def operands_here():
        for copy in copies:
            copy.wait()

    layer(nz, operands_here, *held, *refs[OPERANDS : OPERANDS + 6], *refs[2 * OPERANDS + 6 : -1])


def layer(
    nz,
    operands_here,
    x_ref,
    routes_t_ref,
    rw_t_ref,
    eg_ref,
    fg_ref,
    pin_ref,
    pout_ref,
    q_ref,
    k_ref,
    v_ref,
    qg_ref,
    kg_ref,
    mg_ref,
    cos_row_ref,
    sin_row_ref,
    cos_col_ref,
    sin_col_ref,
    gate_hbm,
    up_hbm,
    down_hbm,
    ow_hbm,
    mix_ref,
    out_ref,
    normed,
    outgoing,
    arr,
    xall,
    part,
    rs1,
    rs2,
    ret_out,
    ret_in,
    ret_rows,
    wgu,
    wd,
    combined,
    ow,
    kv,
    side,
    q_s,
    m_s,
    l_s,
    acc_s,
    att_s,
    w_sem,
    d_send,
    d_recv,
    ag_send,
    ag_recv,
    rs_send,
    rs1_recv,
    rs2_recv,
    r_send,
    r_recv,
    kz_send,
    kz_recv,
    ky_send,
    ky_recv,
    kc_send,
    kc_recv,
):
    z = lax.axis_index("ep_0")
    p_me = lax.axis_index("ep_1") * 2 + lax.axis_index("ep_2")
    x_me = lax.axis_index("tp")
    right = {"tp": lax.rem(x_me + 1, 4)}
    left = {"tp": lax.rem(x_me + 3, 4)}
    y_me = lax.axis_index("ep_1")
    y_up = {"ep_1": lax.rem(y_me + 1, 4)}
    y_down = {"ep_1": lax.rem(y_me + 3, 4)}
    other_core = {"ep_2": 1 - lax.axis_index("ep_2")}
    tok, width = x_ref.shape
    half = width // 2
    sub_w = width // SUB
    ff = wd.shape[0]
    n_exp = nz * PL

    def peer(zz, p):
        return {"ep_0": zz, "ep_1": lax.div(p, 2), "ep_2": lax.rem(p, 2)}

    def entry(values, i):
        found = jnp.full(jnp.shape(i), values[0], jnp.int32)
        for j in range(1, nz):
            found = jnp.where(i == j, values[j], found)
        return found

    def plane(i):
        return lax.rem(z + entry([a % nz for a in AWAY], i), nz)

    def mirror(i):
        return entry(MIRROR, i)

    barrier = pltpu.get_barrier_semaphore()

    def greet(device):
        pl.semaphore_signal(barrier, inc=1, device_id=device, device_id_type=MESH)

    greet(left)
    greet(right)
    for j in range(1, PL):
        greet(peer(z, lax.rem(p_me + j, PL)))

    @pl.loop(1, nz)
    def _(d):
        zz = lax.rem(z + d, nz)
        for j in range(PL):
            greet(peer(zz, lax.rem(p_me + j, PL)))

    w_copies = [
        pltpu.make_async_copy(gate_hbm.at[0], wgu.at[:, pl.ds(0, ff)], w_sem.at[0]),
        pltpu.make_async_copy(up_hbm.at[0], wgu.at[:, pl.ds(ff, ff)], w_sem.at[1]),
        pltpu.make_async_copy(down_hbm.at[0], wd, w_sem.at[2]),
        pltpu.make_async_copy(ow_hbm, ow, w_sem.at[3]),
    ]
    for copy in w_copies:
        copy.start()

    operands_here()
    xf = x_ref[...].astype(F32)
    normed[...] = rms_scale(xf, eg_ref[...]).astype(BF)

    def base_of(e):
        o = (lax.shift_right_logical(e, 3) - z + nz) & (nz - 1)
        return entry(INDEX, o) * ROWS + (e & 7) * CAP

    e_rows = lax.broadcasted_iota(jnp.int32, (n_exp, tok), 0)
    t_a = lax.broadcasted_iota(jnp.int32, (tok, tok), 0)
    t_b = lax.broadcasted_iota(jnp.int32, (tok, tok), 1)
    before_t = one_hot(t_a < t_b)
    oh0 = e_rows == routes_t_ref[0:1, :]
    oh1 = e_rows == routes_t_ref[1:2, :]
    rank0 = dot(one_hot(oh0), before_t)
    rank1 = dot(one_hot(oh1), before_t) + jnp.sum(
        jnp.where(oh0, 1.0, 0.0), axis=1, keepdims=True
    )
    base = base_of(e_rows).astype(F32)
    place0 = jnp.sum(jnp.where(oh0, base + rank0, 0.0), axis=0, keepdims=True)
    place1 = jnp.sum(jnp.where(oh1, base + rank1, 0.0), axis=0, keepdims=True)
    slots = lax.broadcasted_iota(jnp.int32, (nz * ROWS, tok), 0).astype(F32)
    pick = one_hot((slots == place0) | (slots == place1))
    side[...] = jnp.concatenate(
        [place0, place1, rw_t_ref[...], jnp.zeros((4, tok), F32)], axis=0
    )

    def stack_pieces(rows):
        return jnp.concatenate(
            [rows[:, q * sub_w : (q + 1) * sub_w] for q in range(SUB)], axis=0
        )

    def join_pieces(stacked):
        return jnp.concatenate(
            [stacked[q * ROWS : (q + 1) * ROWS, :] for q in range(SUB)], axis=1
        )

    def to_blocks(rows):
        blocks = dot(pout_ref[...], stack_pieces(rows)).astype(BF)
        return blocks.reshape(PL, ROWS, sub_w)

    def to_rows(blocks):
        flat = blocks.reshape(PL * ROWS, sub_w)
        return join_pieces(dot(pin_ref[...], flat).astype(BF))

    def dispatch(i, p):
        return pltpu.make_async_remote_copy(
            src_ref=outgoing.at[i, p],
            dst_ref=arr.at[mirror(i), p_me],
            send_sem=d_send.at[jnp.minimum(i, 1)],
            recv_sem=d_recv.at[mirror(i)],
            device_id=peer(plane(i), p),
            device_id_type=MESH,
        )

    def give_back(i, p):
        return pltpu.make_async_remote_copy(
            src_ref=ret_out.at[i, p],
            dst_ref=ret_in.at[mirror(i), p_me],
            send_sem=r_send.at[jnp.minimum(i, 1)],
            recv_sem=r_recv.at[mirror(i)],
            device_id=peer(plane(i), p),
            device_id_type=MESH,
        )

    def x_copy(src, dst, send, recv, to):
        return pltpu.make_async_remote_copy(
            src_ref=src, dst_ref=dst, send_sem=send, recv_sem=recv, device_id=to,
            device_id_type=MESH,
        )

    z_up = {"ep_0": lax.rem(z + 1, nz)}
    z_down = {"ep_0": lax.rem(z + nz - 1, nz)}

    def kv_z_up(k, to):
        return x_copy(kv.at[k, 0, 0], kv.at[to, 0, 0], kz_send.at[0], kz_recv.at[to, 0], z_up)

    def kv_z_down(k, to):
        return x_copy(
            kv.at[k, 0, 0], kv.at[to, 0, 0], kz_send.at[0], kz_recv.at[to, 0], z_down
        )

    last = nz - 1
    k_z_far = x_copy(
        kv.at[last - 2, 0, 0, 0], kv.at[last, 0, 0, 0], kz_send.at[0], kz_recv.at[last, 0],
        z_up,
    )
    v_z_far = x_copy(
        kv.at[last - 1, 0, 0, 1], kv.at[last, 0, 0, 1], kz_send.at[0], kz_recv.at[last, 1],
        z_down,
    )

    def each_plane(group, act):
        act(jnp.maximum(2 * group - 1, 0))

        @pl.when((group >= 1) & (group < nz // 2))
        def _():
            act(2 * group)

    def kv_up(k):
        return x_copy(kv.at[k, 0, 0], kv.at[k, 0, 1], ky_send.at[0], ky_recv.at[k, 0], y_up)

    def kv_down(k):
        return x_copy(kv.at[k, 0, 0], kv.at[k, 0, 2], ky_send.at[0], ky_recv.at[k, 1], y_down)

    def k_far(k):
        return x_copy(
            kv.at[k, 0, 1, 0], kv.at[k, 0, 3, 0], ky_send.at[0], ky_recv.at[k, 2], y_up
        )

    def v_far(k):
        return x_copy(
            kv.at[k, 0, 2, 1], kv.at[k, 0, 3, 1], ky_send.at[0], ky_recv.at[k, 3], y_down
        )

    def kv_across(k):
        return x_copy(kv.at[k, 0], kv.at[k, 1], kc_send.at[0], kc_recv.at[k], other_core)

    def attend(k):
        keys = kv[k, :, :, 0].reshape(-1, HEAD)
        vals = kv[k, :, :, 1].reshape(-1, HEAD)

        @pl.loop(0, HEADS)
        def _(h):
            scores = lax.dot_general(
                q_s[h], keys, (((1,), (1,)), ((), ())), preferred_element_type=F32
            ) * HEAD ** (-0.5)
            peak = jnp.maximum(m_s[h], jnp.max(scores, axis=1, keepdims=True))
            fade = jnp.exp(m_s[h] - peak)
            expo = jnp.exp(scores - peak[:, :1])
            m_s[h] = peak
            sums = l_s[h] * fade
            for c in range(expo.shape[1] // HEAD):
                sums = sums + expo[:, c * HEAD : (c + 1) * HEAD]
            l_s[h] = sums
            acc_s[h] = acc_s[h] * fade + dot(expo.astype(BF), vals)

    def project():
        for h in range(HEADS):
            total = jnp.sum(l_s[h], axis=1, keepdims=True)
            att_s[:, h * HEAD : (h + 1) * HEAD] = (acc_s[h] / total).astype(BF)
        share = att_s.shape[0] // TP
        ours = jnp.concatenate(
            [
                att_s[pl.ds(pl.multiple_of(lax.rem(x_me + o, TP) * share, share), share), :]
                for o in (0, 3, 1, 2)
            ],
            axis=0,
        )
        return dot(ours, ow[...]).astype(BF).reshape(TP, share, width)

    def to_plane(i, make):
        @pl.when(i == 0)
        def _():
            @pl.loop(1, PL)
            def _(j):
                make(i, lax.rem(p_me + j, PL)).start()

        @pl.when(i > 0)
        def _():
            @pl.loop(0, PL)
            def _(j):
                make(i, lax.rem(p_me + j, PL)).start()

    def wait_bytes(ref, sem):
        pltpu.make_async_copy(ref, ref, sem).wait()

    def wait_plane(i, ref, sem):
        @pl.when(i == 0)
        def _():
            wait_bytes(ref.at[0, pl.ds(0, PL - 1)], sem.at[0])

        @pl.when(i > 0)
        def _():
            wait_bytes(ref.at[i], sem.at[i])

    def gather(i):
        rows = dot(pick[i * ROWS : (i + 1) * ROWS, :], normed[...]).astype(BF)
        outgoing[i] = to_blocks(rows)

    gather(0)
    pl.semaphore_wait(barrier, n_exp - 1 + 2)
    to_plane(jnp.int32(0), dispatch)
    arr[0, p_me] = outgoing[0, p_me]

    for c in FIRST:
        gather(MIRROR[c])
        to_plane(jnp.int32(MIRROR[c]), dispatch)

    grid_rows = k_ref.shape[0] // GRID_W
    first_row = (z * PL + p_me) * grid_rows
    cosine = jnp.concatenate(
        [cos_row_ref[pl.ds(first_row + g, 1), :] + cos_col_ref[...] for g in range(grid_rows)],
        axis=0,
    )
    sine = jnp.concatenate(
        [sin_row_ref[pl.ds(first_row + g, 1), :] + sin_col_ref[...] for g in range(grid_rows)],
        axis=0,
    )
    lane = lax.broadcasted_iota(jnp.int32, cosine.shape, 1)
    first_of_pair = (lane & 32) == 0

    def normed_and_turned(head, gain):
        field = rms_scale(head.astype(F32), gain)
        swapped = jnp.where(
            first_of_pair, pltpu.roll(field, HEAD - 32, 1), pltpu.roll(field, 32, 1)
        )
        return (field * cosine + swapped * sine).astype(BF)

    kv[0, 0, 0, 0] = normed_and_turned(k_ref[...], kg_ref[...])
    kv[0, 0, 0, 1] = v_ref[...]
    kv_z_up(0, 1).start()
    kv_z_down(0, 2).start()
    kv_up(0).start()
    kv_down(0).start()

    for c in range(1, nz):
        if c not in FIRST:
            gather(MIRROR[c])

    for h in range(HEADS):
        q_s[h] = normed_and_turned(q_ref[:, h * HEAD : (h + 1) * HEAD], qg_ref[...])
    m_s[...] = jnp.full(m_s.shape, -1e30, F32)
    l_s[...] = jnp.zeros(l_s.shape, F32)
    acc_s[...] = jnp.zeros(acc_s.shape, F32)

    cols_a, cols_b = pl.ds(0, half), pl.ds(half, half)

    def ag_right(k):
        return x_copy(xall.at[k, 0], xall.at[k, 1], ag_send.at[0], ag_recv.at[k, 0], right)

    def ag_left(k):
        return x_copy(xall.at[k, 0], xall.at[k, 2], ag_send.at[0], ag_recv.at[k, 1], left)

    def fwd_right(k):
        return x_copy(
            xall.at[k, 1, :, cols_a], xall.at[k, 3, :, cols_a],
            ag_send.at[0], ag_recv.at[k, 2], right,
        )

    def fwd_left(k):
        return x_copy(
            xall.at[k, 2, :, cols_b], xall.at[k, 3, :, cols_b],
            ag_send.at[0], ag_recv.at[k, 3], left,
        )

    def rs_far_left(k):
        return x_copy(
            part.at[k, 3, :, cols_a], rs1.at[k, 0], rs_send.at[0], rs1_recv.at[k, 0], left
        )

    def rs_far_right(k):
        return x_copy(
            part.at[k, 3, :, cols_b], rs1.at[k, 1], rs_send.at[0], rs1_recv.at[k, 1], right
        )

    def rs_near_left(k, c, s):
        return x_copy(
            part.at[k, 1, :, c], rs2.at[k, 1, :, c], rs_send.at[0], rs2_recv.at[k, s - 2], left
        )

    def rs_near_right(k, c, s):
        return x_copy(
            part.at[k, 2, :, c], rs2.at[k, 0, :, c], rs_send.at[0], rs2_recv.at[k, s - 2], right
        )

    def rs_copies(k):
        return (
            rs_far_left(k),
            rs_far_right(k),
            rs_near_left(k, cols_a, 2),
            rs_near_left(k, cols_b, 3),
            rs_near_right(k, cols_a, 4),
            rs_near_right(k, cols_b, 5),
        )

    def rs_far(k):
        rs_far_left(k).start()
        rs_far_right(k).start()

    def rs_near(k):
        rs_near_left(k, cols_b, 3).start()
        rs_near_right(k, cols_a, 4).start()

    def rs_total(k):
        for copy in rs_copies(k)[2:]:
            copy.wait_recv()
        return part[k, 0].astype(F32) + rs2[k, 0].astype(F32) + rs2[k, 1].astype(F32)

    def experts(k):
        fwd_right(k).wait_recv()
        fwd_left(k).wait_recv()

        rows = xall[k].reshape(4 * ROWS, width)
        pre = dot(rows, wgu[...])
        gate_cut = jnp.minimum(pre[:, :ff], clamp_limit)
        up_cut = jnp.clip(pre[:, ff:], -clamp_limit, clamp_limit)
        hidden = (
            (up_cut + 1.0) * gate_cut * (1.0 / (1.0 + jnp.exp(-sigmoid_slope * gate_cut)))
        ).astype(BF)
        part[k] = dot(hidden, wd[...]).astype(BF).reshape(4, ROWS, width)
        rs_far(k)

    def pass_on(k):
        rs_far_left(k).wait_recv()
        part[k, 1, :, cols_a] = (
            part[k, 1, :, cols_a].astype(F32) + rs1[k, 0].astype(F32)
        ).astype(BF)
        rs_near_left(k, cols_a, 2).start()
        rs_far_right(k).wait_recv()
        part[k, 2, :, cols_b] = (
            part[k, 2, :, cols_b].astype(F32) + rs1[k, 1].astype(F32)
        ).astype(BF)
        rs_near_right(k, cols_b, 5).start()

    def finish(k):
        ret_out[k] = to_blocks(rs_total(k).astype(BF))
        to_plane(k, give_back)

    def take_back(j):
        kk = mirror(j)
        wait_plane(kk, ret_in, r_recv)
        ret_rows[kk] = to_rows(ret_in[kk])

    @pl.loop(0, nz + 4)
    def _(step):
        @pl.when(step < nz)
        def _():
            k = step
            wait_plane(k, arr, d_recv)
            xall[k, 0] = to_rows(arr[k])
            ag_right(k).start()
            ag_left(k).start()
        @pl.when((step >= 1) & (step < nz + 1))
        def _():
            k = step - 1
            ag_right(k).wait_recv()
            fwd_right(k).start()
            ag_left(k).wait_recv()
            fwd_left(k).start()

        @pl.when(step == 2)
        def _():
            for copy in w_copies:
                copy.wait()

        @pl.when((step >= 3) & (step < nz + 2))
        def _():
            experts(step - 2)

        @pl.when((step >= 4) & (step < nz + 3))
        def _():
            pass_on(step - 3)

        @pl.when((step >= 3) & (step < nz + 2))
        def _():
            rs_near(step - 2)

        @pl.when(step == nz + 1)
        def _():
            experts(0)

        @pl.when(step == nz + 2)
        def _():
            rs_near(0)

        @pl.when((step >= 2) & (step <= nz // 2))
        def _():
            below, above = 2 * step - 3, 2 * step - 2
            kv_z_up(0, below).wait_recv()
            kv_z_down(0, above).wait_recv()

            @pl.when(step < nz // 2)
            def _():
                kv_z_up(below, below + 2).start()
                kv_z_down(above, above + 2).start()

            @pl.when(step == nz // 2)
            def _():
                k_z_far.start()
                v_z_far.start()

            for j in (below, above):
                kv_up(j).start()
                kv_down(j).start()

        @pl.when(step == nz // 2 + 1)
        def _():
            k_z_far.wait_recv()
            v_z_far.wait_recv()
            kv_up(last).start()
            kv_down(last).start()

        for at, chunks in LATER.items():

            @pl.when(step == at)
            def _(chunks=chunks):
                for i in chunks:
                    to_plane(jnp.int32(MIRROR[i]), dispatch)

        @pl.when((step >= 2) & (step <= nz // 2 + 2))
        def _():
            def forward(j):
                kv_up(j).wait_recv()
                k_far(j).start()
                kv_down(j).wait_recv()
                v_far(j).start()

            each_plane(step - 2, forward)

        @pl.when((step >= 3) & (step <= nz // 2 + 3))
        def _():
            def across(j):
                k_far(j).wait_recv()
                v_far(j).wait_recv()
                kv_across(j).start()

            each_plane(step - 3, across)

        @pl.when((step >= 4) & (step <= nz // 2 + 4))
        def _():
            def attend_to(j):
                kv_across(j).wait_recv()
                attend(j)

            each_plane(step - 4, attend_to)

        @pl.when(step >= 5)
        def _():
            finish(step - 4)

        @pl.when(step == nz)
        def _():
            part[nz] = project()

        @pl.when(step == nz + 2)
        def _():
            pass_on(0)
            rs_far(nz)
            rs_near(nz)

        @pl.when(step == nz + 3)
        def _():
            finish(jnp.int32(0))
            ret_in[0, p_me] = ret_out[0, p_me]
            pass_on(nz)

        @pl.when(step >= nz)
        def _():
            take_back(step - (nz - 1))

    for j in (5, 6, 7):
        take_back(jnp.int32(j))

    mix_ref[...] = rms_scale(rs_total(nz), mg_ref[...]).astype(BF)
    take_back(jnp.int32(0))

    columns_of = side[...].T
    at0, at1, weight0, weight1 = (columns_of[:, c : c + 1] for c in range(4))
    lanes = lax.broadcasted_iota(jnp.int32, (tok, nz * ROWS), 1).astype(F32)
    take = jnp.concatenate([one_hot(lanes == at0), one_hot(lanes == at1)], axis=0)
    square = jnp.zeros((tok, 1), F32)
    block = min(512, width)
    for c in range(width // block):
        columns = slice(c * block, (c + 1) * block)
        both = dot(take, ret_rows[:, :, columns].reshape(nz * ROWS, block))
        mixed = weight0 * both[:tok] + weight1 * both[tok:]
        combined[:, columns] = mixed
        square = square + jnp.sum(mixed * mixed, axis=1, keepdims=True)
    scale = lax.rsqrt(square / width + norm_eps)
    out_ref[...] = (combined[...] * scale * fg_ref[...]).astype(BF)

    for blocks, sems in ((outgoing, d_send), (ret_out, r_send)):
        wait_bytes(blocks.at[0, pl.ds(0, PL - 1)], sems.at[0])
        wait_bytes(blocks.at[pl.ds(1, nz - 1)], sems.at[1])
    wait_bytes(xall.at[:, pl.ds(0, 3)], ag_send.at[0])
    wait_bytes(part.at[:, pl.ds(0, 3)], rs_send.at[0])
    wait_bytes(kv.at[pl.ds(0, nz - 1), 0, 0], kz_send.at[0])
    wait_bytes(kv.at[:, 0, pl.ds(0, 3)], ky_send.at[0])
    wait_bytes(kv.at[:, 0], kc_send.at[0])


def permutation():
    source, piece, rank = np.meshgrid(
        np.arange(PL), np.arange(SUB), np.arange(CAP), indexing="ij"
    )
    travel = (source * SUB + piece) * CAP + rank
    rowwise = (piece * PL + source) * CAP + rank
    matrix = np.zeros((PL * ROWS, PL * ROWS), np.float32)
    matrix[rowwise.reshape(-1), travel.reshape(-1)] = 1.0
    return matrix


def turn_tables(rows):
    quarter = HEAD // 4
    inverse = rope_base ** (-np.arange(quarter, dtype=np.float64) / quarter)

    def table(count, make, at):
        angle = np.arange(count, dtype=np.float64)[:, None] * inverse[None, :]
        out = np.zeros((count, HEAD), np.float32)
        out[:, at : at + 2 * quarter] = make(angle)
        return jnp.asarray(out)

    def cosines(angle):
        return np.concatenate([np.cos(angle), np.cos(angle)], axis=1)

    def sines(angle):
        return np.concatenate([-np.sin(angle), np.sin(angle)], axis=1)

    return (
        table(rows, cosines, 0),
        table(rows, sines, 0),
        table(GRID_W, cosines, HEAD // 2),
        table(GRID_W, sines, HEAD // 2),
    )


def local(
    queries,
    keys,
    values,
    query_gain,
    key_gain,
    out_weight,
    mixer_gain,
    expert_in,
    routes,
    route_weights,
    expert_gain,
    gate_w,
    up_w,
    down_w,
    ffn_out_gain,
):
    nz = lax.axis_size("ep_0")
    assert nz == NZ
    tok, width = expert_in.shape
    ff = gate_w.shape[2]
    seq = queries.shape[0]
    tables = turn_tables(nz * PL * seq // GRID_W)
    matrix = permutation()
    pin = jnp.asarray(matrix, BF)
    pout = jnp.asarray(matrix.T, BF)
    hbm = pl.BlockSpec(memory_space=pltpu.HBM)
    vmem = pl.BlockSpec(memory_space=pltpu.VMEM)
    travel = (nz, PL, ROWS, width // SUB)
    dma = pltpu.SemaphoreType.DMA
    operands = (
        expert_in,
        routes.T,
        route_weights.T,
        expert_gain[None, :],
        ffn_out_gain[None, :],
        pin,
        pout,
        queries,
        keys,
        values,
        query_gain[None, :],
        key_gain[None, :],
        mixer_gain[None, :],
        *tables,
    )
    assert len(operands) == OPERANDS
    made = pl.pallas_call(
        functools.partial(layer_kernel, nz),
        out_shape=(
            pltpu.VMEM((seq // TP, width), BF),
            pltpu.VMEM((tok, width), BF),
        ),
        in_specs=[hbm] * (OPERANDS + 4),
        out_specs=(vmem, vmem),
        scratch_shapes=[pltpu.VMEM(a.shape, a.dtype) for a in operands]
        + [
            pltpu.VMEM((tok, width), BF),
            pltpu.VMEM(travel, BF),
            pltpu.VMEM(travel, BF),
            pltpu.VMEM((nz, 4, ROWS, width), BF),
            pltpu.VMEM((nz + 1, 4, ROWS, width), BF),
            pltpu.VMEM((nz + 1, 2, ROWS, width // 2), BF),
            pltpu.VMEM((nz + 1, 2, ROWS, width), BF),
            pltpu.VMEM(travel, BF),
            pltpu.VMEM(travel, BF),
            pltpu.VMEM((nz, ROWS, width), BF),
            pltpu.VMEM((width, 2 * ff), BF),
            pltpu.VMEM((ff, width), BF),
            pltpu.VMEM((tok, width), F32),
            pltpu.VMEM(out_weight.shape, BF),
            pltpu.VMEM((nz, 2, 4, 2, seq, HEAD), BF),
            pltpu.VMEM((8, tok), F32),
            pltpu.VMEM((HEADS, seq, HEAD), BF),
            pltpu.VMEM((HEADS, seq, HEAD), F32),
            pltpu.VMEM((HEADS, seq, HEAD), F32),
            pltpu.VMEM((HEADS, seq, HEAD), F32),
            pltpu.VMEM((seq, HEADS * HEAD), BF),
            dma((4,)),
            dma((2,)),
            dma((nz,)),
            dma((1,)),
            dma((nz, 4)),
            dma((1,)),
            dma((nz + 1, 2)),
            dma((nz + 1, 4)),
            dma((2,)),
            dma((nz,)),
            dma((1,)),
            dma((nz, 2)),
            dma((1,)),
            dma((nz, 4)),
            dma((1,)),
            dma((nz,)),
            dma((OPERANDS,)),
        ],
        compiler_params=pltpu.CompilerParams(
            collective_id=0, has_side_effects=True, vmem_limit_bytes=58 * 2**20
        ),
        name="layer",
    )(
        *operands,
        gate_w,
        up_w,
        down_w,
        out_weight,
    )
    return made


def solution(mesh):
    split = Mesh(
        mesh.devices.reshape(mesh.shape["ep"] // 8, 4, 2, mesh.shape["tp"]),
        ("ep_0", "ep_1", "ep_2", "tp"),
    )
    return jax.shard_map(
        local,
        mesh=split,
        in_specs=(
            P(EP, "tp"),
            P(EP, "tp"),
            P(EP, "tp"),
            P(),
            P(),
            P("tp", None),
            P(),
            P(EP_TP, None),
            P(EP_TP, None),
            P(EP_TP, None),
            P(),
            P(EP, None, "tp"),
            P(EP, None, "tp"),
            P(EP, "tp", None),
            P(),
        ),
        out_specs=(P(EP_TP, None), P(EP_TP, None)),
        check_vma=False,
    )
```

```python
import functools

import jax
import jax.numpy as jnp
import numpy as np
from jax import lax
from jax.experimental import pallas as pl
from jax.experimental.pallas import tpu as pltpu
from jax.sharding import Mesh
from jax.sharding import PartitionSpec as P

HEAD = 128
HEADS = 4
GRID_W = 64
TP = 4
OPERANDS = 17
EP = ("ep_0", "ep_1", "ep_2")
EP_TP = ("ep_0", "ep_1", "ep_2", "tp")
MESH = pl.DeviceIdType.MESH
BF = jnp.bfloat16
F32 = jnp.float32

norm_eps = 1e-06
rope_base = 10000.0
clamp_limit = 7.0
sigmoid_slope = 1.702

PL = 8
CAP = 6
SUB = 8
ROWS = PL * CAP
AWAY = (0, 1, -2, 3, 4, -3, 2, -1)
NZ = len(AWAY)
FIRST = (1, 2, 3)
LATER = {0: (4,), 2: (5,), 3: (6, 7)}
INDEX = [[a % NZ for a in AWAY].index(d) for d in range(NZ)]
MIRROR = [INDEX[-a % NZ] for a in AWAY]


def rms_scale(values_in, gain):
    return (
        values_in
        * lax.rsqrt(jnp.mean(values_in * values_in, axis=-1, keepdims=True) + norm_eps)
        * gain
    )


def dot(a, b):
    return jnp.dot(a, b, preferred_element_type=F32)


def one_hot(cond):
    return jnp.where(cond, 1.0, 0.0).astype(BF)


def layer_kernel(nz, *refs):
    ours = refs[:OPERANDS]
    held = refs[OPERANDS + 6 : 2 * OPERANDS + 6]
    sems = refs[-1]
    copies = [
        pltpu.make_async_copy(src, dst, sems.at[i])
        for i, (src, dst) in enumerate(zip(ours, held))
    ]
    for copy in copies:
        copy.start()

    def operands_here(first, end):
        for copy in copies[first:end]:
            copy.wait()

    layer(nz, operands_here, *held, *refs[OPERANDS : OPERANDS + 6], *refs[2 * OPERANDS + 6 : -1])


def layer(
    nz,
    operands_here,
    x_ref,
    routes_t_ref,
    rw_t_ref,
    eg_ref,
    fg_ref,
    pin_ref,
    pout_ref,
    q_ref,
    k_ref,
    v_ref,
    qg_ref,
    kg_ref,
    mg_ref,
    cos_row_ref,
    sin_row_ref,
    cos_col_ref,
    sin_col_ref,
    gate_hbm,
    up_hbm,
    down_hbm,
    ow_hbm,
    mix_ref,
    out_ref,
    normed,
    outgoing,
    arr,
    xall,
    part,
    rs1,
    rs2,
    ret_out,
    ret_in,
    ret_rows,
    wgu,
    wd,
    combined,
    ow,
    kv,
    side,
    both,
    q_s,
    m_s,
    l_s,
    acc_s,
    att_s,
    w_sem,
    d_send,
    d_recv,
    ag_send,
    ag_recv,
    rs_send,
    rs1_recv,
    rs2_recv,
    r_send,
    r_recv,
    kz_send,
    kz_recv,
    ky_send,
    ky_recv,
    kc_send,
    kc_recv,
):
    z = lax.axis_index("ep_0")
    p_me = lax.axis_index("ep_1") * 2 + lax.axis_index("ep_2")
    x_me = lax.axis_index("tp")
    right = {"tp": lax.rem(x_me + 1, 4)}
    left = {"tp": lax.rem(x_me + 3, 4)}
    y_me = lax.axis_index("ep_1")
    y_up = {"ep_1": lax.rem(y_me + 1, 4)}
    y_down = {"ep_1": lax.rem(y_me + 3, 4)}
    other_core = {"ep_2": 1 - lax.axis_index("ep_2")}
    tok, width = x_ref.shape
    half = width // 2
    sub_w = width // SUB
    ff = wd.shape[0]
    n_exp = nz * PL

    def peer(zz, p):
        return {"ep_0": zz, "ep_1": lax.div(p, 2), "ep_2": lax.rem(p, 2)}

    def entry(values, i):
        found = jnp.full(jnp.shape(i), values[0], jnp.int32)
        for j in range(1, nz):
            found = jnp.where(i == j, values[j], found)
        return found

    def plane(i):
        return lax.rem(z + entry([a % nz for a in AWAY], i), nz)

    def mirror(i):
        return entry(MIRROR, i)

    barrier = pltpu.get_barrier_semaphore()

    def greet(device):
        pl.semaphore_signal(barrier, inc=1, device_id=device, device_id_type=MESH)

    greet(left)
    greet(right)
    for j in range(1, PL):
        greet(peer(z, lax.rem(p_me + j, PL)))

    @pl.loop(1, nz)
    def _(d):
        zz = lax.rem(z + d, nz)
        for j in range(PL):
            greet(peer(zz, lax.rem(p_me + j, PL)))

    w_copies = [
        pltpu.make_async_copy(gate_hbm.at[0], wgu.at[:, pl.ds(0, ff)], w_sem.at[0]),
        pltpu.make_async_copy(up_hbm.at[0], wgu.at[:, pl.ds(ff, ff)], w_sem.at[1]),
        pltpu.make_async_copy(down_hbm.at[0], wd, w_sem.at[2]),
        pltpu.make_async_copy(ow_hbm, ow, w_sem.at[3]),
    ]
    for copy in w_copies:
        copy.start()

    operands_here(0, 7)
    xf = x_ref[...].astype(F32)
    normed[...] = rms_scale(xf, eg_ref[...]).astype(BF)

    def base_of(e):
        o = (lax.shift_right_logical(e, 3) - z + nz) & (nz - 1)
        return entry(INDEX, o) * ROWS + (e & 7) * CAP

    e_rows = lax.broadcasted_iota(jnp.int32, (n_exp, tok), 0)
    t_a = lax.broadcasted_iota(jnp.int32, (tok, tok), 0)
    t_b = lax.broadcasted_iota(jnp.int32, (tok, tok), 1)
    before_t = one_hot(t_a < t_b)
    oh0 = e_rows == routes_t_ref[0:1, :]
    oh1 = e_rows == routes_t_ref[1:2, :]
    rank0 = dot(one_hot(oh0), before_t)
    rank1 = dot(one_hot(oh1), before_t) + jnp.sum(
        jnp.where(oh0, 1.0, 0.0), axis=1, keepdims=True
    )
    base = base_of(e_rows).astype(F32)
    place0 = jnp.sum(jnp.where(oh0, base + rank0, 0.0), axis=0, keepdims=True)
    place1 = jnp.sum(jnp.where(oh1, base + rank1, 0.0), axis=0, keepdims=True)
    slots = lax.broadcasted_iota(jnp.int32, (nz * ROWS, tok), 0).astype(F32)
    pick = one_hot((slots == place0) | (slots == place1))
    side[...] = jnp.concatenate(
        [place0, place1, rw_t_ref[...], jnp.zeros((4, tok), F32)], axis=0
    )

    def stack_pieces(rows):
        return jnp.concatenate(
            [rows[:, q * sub_w : (q + 1) * sub_w] for q in range(SUB)], axis=0
        )

    def join_pieces(stacked):
        return jnp.concatenate(
            [stacked[q * ROWS : (q + 1) * ROWS, :] for q in range(SUB)], axis=1
        )

    def to_blocks(rows):
        blocks = dot(pout_ref[...], stack_pieces(rows)).astype(BF)
        return blocks.reshape(PL, ROWS, sub_w)

    def to_rows(blocks):
        flat = blocks.reshape(PL * ROWS, sub_w)
        return join_pieces(dot(pin_ref[...], flat).astype(BF))

    def dispatch(i, p):
        return pltpu.make_async_remote_copy(
            src_ref=outgoing.at[i, p],
            dst_ref=arr.at[mirror(i), p_me],
            send_sem=d_send.at[jnp.minimum(i, 1)],
            recv_sem=d_recv.at[mirror(i)],
            device_id=peer(plane(i), p),
            device_id_type=MESH,
        )

    def give_back(i, p):
        return pltpu.make_async_remote_copy(
            src_ref=ret_out.at[i, p],
            dst_ref=ret_in.at[mirror(i), p_me],
            send_sem=r_send.at[jnp.minimum(i, 1)],
            recv_sem=r_recv.at[mirror(i)],
            device_id=peer(plane(i), p),
            device_id_type=MESH,
        )

    def x_copy(src, dst, send, recv, to):
        return pltpu.make_async_remote_copy(
            src_ref=src, dst_ref=dst, send_sem=send, recv_sem=recv, device_id=to,
            device_id_type=MESH,
        )

    z_up = {"ep_0": lax.rem(z + 1, nz)}
    z_down = {"ep_0": lax.rem(z + nz - 1, nz)}

    def kv_z_up(k, to):
        return x_copy(kv.at[k, 0, 0], kv.at[to, 0, 0], kz_send.at[0], kz_recv.at[to, 0], z_up)

    def kv_z_down(k, to):
        return x_copy(
            kv.at[k, 0, 0], kv.at[to, 0, 0], kz_send.at[0], kz_recv.at[to, 0], z_down
        )

    last = nz - 1
    k_z_far = x_copy(
        kv.at[last - 2, 0, 0, 0], kv.at[last, 0, 0, 0], kz_send.at[0], kz_recv.at[last, 0],
        z_up,
    )
    v_z_far = x_copy(
        kv.at[last - 1, 0, 0, 1], kv.at[last, 0, 0, 1], kz_send.at[0], kz_recv.at[last, 1],
        z_down,
    )

    def each_plane(group, act):
        act(jnp.maximum(2 * group - 1, 0))

        @pl.when((group >= 1) & (group < nz // 2))
        def _():
            act(2 * group)

    def kv_up(k):
        return x_copy(kv.at[k, 0, 0], kv.at[k, 0, 1], ky_send.at[0], ky_recv.at[k, 0], y_up)

    def kv_down(k):
        return x_copy(kv.at[k, 0, 0], kv.at[k, 0, 2], ky_send.at[0], ky_recv.at[k, 1], y_down)

    def k_far(k):
        return x_copy(
            kv.at[k, 0, 1, 0], kv.at[k, 0, 3, 0], ky_send.at[0], ky_recv.at[k, 2], y_up
        )

    def v_far(k):
        return x_copy(
            kv.at[k, 0, 2, 1], kv.at[k, 0, 3, 1], ky_send.at[0], ky_recv.at[k, 3], y_down
        )

    def kv_across(k):
        return x_copy(kv.at[k, 0], kv.at[k, 1], kc_send.at[0], kc_recv.at[k], other_core)

    def attend(k):
        keys = kv[k, :, :, 0].reshape(-1, HEAD)
        vals = kv[k, :, :, 1].reshape(-1, HEAD)

        @pl.loop(0, HEADS)
        def _(h):
            scores = lax.dot_general(
                q_s[h], keys, (((1,), (1,)), ((), ())), preferred_element_type=F32
            ) * HEAD ** (-0.5)
            peak = jnp.maximum(m_s[h], jnp.max(scores, axis=1, keepdims=True))
            fade = jnp.exp(m_s[h] - peak)
            expo = jnp.exp(scores - peak[:, :1])
            m_s[h] = peak
            sums = l_s[h] * fade
            for c in range(expo.shape[1] // HEAD):
                sums = sums + expo[:, c * HEAD : (c + 1) * HEAD]
            l_s[h] = sums
            acc_s[h] = acc_s[h] * fade + dot(expo.astype(BF), vals)

    def project():
        for h in range(HEADS):
            total = jnp.sum(l_s[h], axis=1, keepdims=True)
            att_s[:, h * HEAD : (h + 1) * HEAD] = (acc_s[h] / total).astype(BF)
        share = att_s.shape[0] // TP
        ours = jnp.concatenate(
            [
                att_s[pl.ds(pl.multiple_of(lax.rem(x_me + o, TP) * share, share), share), :]
                for o in (0, 3, 1, 2)
            ],
            axis=0,
        )
        return dot(ours, ow[...]).astype(BF).reshape(TP, share, width)

    def to_plane(i, make):
        @pl.when(i == 0)
        def _():
            @pl.loop(1, PL)
            def _(j):
                make(i, lax.rem(p_me + j, PL)).start()

        @pl.when(i > 0)
        def _():
            @pl.loop(0, PL)
            def _(j):
                make(i, lax.rem(p_me + j, PL)).start()

    def wait_bytes(ref, sem):
        pltpu.make_async_copy(ref, ref, sem).wait()

    def wait_plane(i, ref, sem):
        @pl.when(i == 0)
        def _():
            wait_bytes(ref.at[0, pl.ds(0, PL - 1)], sem.at[0])

        @pl.when(i > 0)
        def _():
            wait_bytes(ref.at[i], sem.at[i])

    def gather(i):
        rows = dot(pick[i * ROWS : (i + 1) * ROWS, :], normed[...]).astype(BF)
        outgoing[i] = to_blocks(rows)

    gather(0)
    pl.semaphore_wait(barrier, n_exp - 1 + 2)
    to_plane(jnp.int32(0), dispatch)
    arr[0, p_me] = outgoing[0, p_me]

    for c in FIRST:
        gather(MIRROR[c])
        to_plane(jnp.int32(MIRROR[c]), dispatch)

    operands_here(7, OPERANDS)
    grid_rows = k_ref.shape[0] // GRID_W
    first_row = (z * PL + p_me) * grid_rows
    cosine = jnp.concatenate(
        [cos_row_ref[pl.ds(first_row + g, 1), :] + cos_col_ref[...] for g in range(grid_rows)],
        axis=0,
    )
    sine = jnp.concatenate(
        [sin_row_ref[pl.ds(first_row + g, 1), :] + sin_col_ref[...] for g in range(grid_rows)],
        axis=0,
    )
    lane = lax.broadcasted_iota(jnp.int32, cosine.shape, 1)
    first_of_pair = (lane & 32) == 0

    def normed_and_turned(head, gain):
        field = rms_scale(head.astype(F32), gain)
        swapped = jnp.where(
            first_of_pair, pltpu.roll(field, HEAD - 32, 1), pltpu.roll(field, 32, 1)
        )
        return (field * cosine + swapped * sine).astype(BF)

    kv[0, 0, 0, 0] = normed_and_turned(k_ref[...], kg_ref[...])
    kv[0, 0, 0, 1] = v_ref[...]
    kv_z_up(0, 1).start()
    kv_z_down(0, 2).start()
    kv_up(0).start()
    kv_down(0).start()

    for c in range(1, nz):
        if c not in FIRST:
            gather(MIRROR[c])

    for h in range(HEADS):
        q_s[h] = normed_and_turned(q_ref[:, h * HEAD : (h + 1) * HEAD], qg_ref[...])
    ret_rows[0] = jnp.zeros(ret_rows.shape[1:], BF)
    m_s[...] = jnp.full(m_s.shape, -1e30, F32)
    l_s[...] = jnp.zeros(l_s.shape, F32)
    acc_s[...] = jnp.zeros(acc_s.shape, F32)

    cols_a, cols_b = pl.ds(0, half), pl.ds(half, half)

    def ag_right(k):
        return x_copy(xall.at[k, 0], xall.at[k, 1], ag_send.at[0], ag_recv.at[k, 0], right)

    def ag_left(k):
        return x_copy(xall.at[k, 0], xall.at[k, 2], ag_send.at[0], ag_recv.at[k, 1], left)

    def fwd_right(k):
        return x_copy(
            xall.at[k, 1, :, cols_a], xall.at[k, 3, :, cols_a],
            ag_send.at[0], ag_recv.at[k, 2], right,
        )

    def fwd_left(k):
        return x_copy(
            xall.at[k, 2, :, cols_b], xall.at[k, 3, :, cols_b],
            ag_send.at[0], ag_recv.at[k, 3], left,
        )

    def rs_far_left(k):
        return x_copy(
            part.at[k, 3, :, cols_a], rs1.at[k, 0], rs_send.at[0], rs1_recv.at[k, 0], left
        )

    def rs_far_right(k):
        return x_copy(
            part.at[k, 3, :, cols_b], rs1.at[k, 1], rs_send.at[0], rs1_recv.at[k, 1], right
        )

    def rs_near_left(k, c, s):
        return x_copy(
            part.at[k, 1, :, c], rs2.at[k, 1, :, c], rs_send.at[0], rs2_recv.at[k, s - 2], left
        )

    def rs_near_right(k, c, s):
        return x_copy(
            part.at[k, 2, :, c], rs2.at[k, 0, :, c], rs_send.at[0], rs2_recv.at[k, s - 2], right
        )

    def rs_copies(k):
        return (
            rs_far_left(k),
            rs_far_right(k),
            rs_near_left(k, cols_a, 2),
            rs_near_left(k, cols_b, 3),
            rs_near_right(k, cols_a, 4),
            rs_near_right(k, cols_b, 5),
        )

    def rs_far(k):
        rs_far_left(k).start()
        rs_far_right(k).start()

    def rs_near(k):
        rs_near_left(k, cols_b, 3).start()
        rs_near_right(k, cols_a, 4).start()

    def rs_total(k):
        for copy in rs_copies(k)[2:]:
            copy.wait_recv()
        return part[k, 0].astype(F32) + rs2[k, 0].astype(F32) + rs2[k, 1].astype(F32)

    def experts(k):
        fwd_right(k).wait_recv()
        fwd_left(k).wait_recv()

        rows = xall[k].reshape(4 * ROWS, width)
        pre = dot(rows, wgu[...])
        gate_cut = jnp.minimum(pre[:, :ff], clamp_limit)
        up_cut = jnp.clip(pre[:, ff:], -clamp_limit, clamp_limit)
        hidden = (
            (up_cut + 1.0) * gate_cut * (1.0 / (1.0 + jnp.exp(-sigmoid_slope * gate_cut)))
        ).astype(BF)
        part[k] = dot(hidden, wd[...]).astype(BF).reshape(4, ROWS, width)
        rs_far(k)

    def pass_on(k):
        rs_far_left(k).wait_recv()
        part[k, 1, :, cols_a] = (
            part[k, 1, :, cols_a].astype(F32) + rs1[k, 0].astype(F32)
        ).astype(BF)
        rs_near_left(k, cols_a, 2).start()
        rs_far_right(k).wait_recv()
        part[k, 2, :, cols_b] = (
            part[k, 2, :, cols_b].astype(F32) + rs1[k, 1].astype(F32)
        ).astype(BF)
        rs_near_right(k, cols_b, 5).start()

    def finish(k):
        ret_out[k] = to_blocks(rs_total(k).astype(BF))
        to_plane(k, give_back)

    def take_back(j):
        kk = mirror(j)
        wait_plane(kk, ret_in, r_recv)
        ret_rows[kk] = to_rows(ret_in[kk])

    @pl.loop(0, nz + 4)
    def _(step):
        @pl.when(step < nz)
        def _():
            k = step
            wait_plane(k, arr, d_recv)
            xall[k, 0] = to_rows(arr[k])
            ag_right(k).start()
            ag_left(k).start()
        @pl.when((step >= 1) & (step < nz + 1))
        def _():
            k = step - 1
            ag_right(k).wait_recv()
            fwd_right(k).start()
            ag_left(k).wait_recv()
            fwd_left(k).start()

        @pl.when(step == 2)
        def _():
            for copy in w_copies:
                copy.wait()

        @pl.when((step >= 3) & (step < nz + 2))
        def _():
            experts(step - 2)

        @pl.when((step >= 4) & (step < nz + 3))
        def _():
            pass_on(step - 3)

        @pl.when((step >= 3) & (step < nz + 2))
        def _():
            rs_near(step - 2)

        @pl.when(step == nz + 1)
        def _():
            experts(0)

        @pl.when(step == nz + 2)
        def _():
            rs_near(0)

        @pl.when((step >= 4) & (step <= nz // 2 + 4))
        def _():
            def attend_to(j):
                kv_across(j).wait_recv()
                attend(j)

            each_plane(step - 4, attend_to)

        @pl.when((step >= 2) & (step <= nz // 2))
        def _():
            below, above = 2 * step - 3, 2 * step - 2
            kv_z_up(0, below).wait_recv()
            kv_z_down(0, above).wait_recv()

            @pl.when(step < nz // 2)
            def _():
                kv_z_up(below, below + 2).start()
                kv_z_down(above, above + 2).start()

            @pl.when(step == nz // 2)
            def _():
                k_z_far.start()
                v_z_far.start()

            for j in (below, above):
                kv_up(j).start()
                kv_down(j).start()

        @pl.when(step == nz // 2 + 1)
        def _():
            k_z_far.wait_recv()
            v_z_far.wait_recv()
            kv_up(last).start()
            kv_down(last).start()

        for at, chunks in LATER.items():

            @pl.when(step == at)
            def _(chunks=chunks):
                for i in chunks:
                    to_plane(jnp.int32(MIRROR[i]), dispatch)

        @pl.when((step >= 2) & (step <= nz // 2 + 2))
        def _():
            def forward(j):
                kv_up(j).wait_recv()
                k_far(j).start()
                kv_down(j).wait_recv()
                v_far(j).start()

            each_plane(step - 2, forward)

        @pl.when((step >= 3) & (step <= nz // 2 + 3))
        def _():
            def across(j):
                k_far(j).wait_recv()
                v_far(j).wait_recv()
                kv_across(j).start()

            each_plane(step - 3, across)

        @pl.when(step >= 5)
        def _():
            finish(step - 4)

        @pl.when(step == nz)
        def _():
            part[nz] = project()

        @pl.when(step == nz + 2)
        def _():
            pass_on(0)
            rs_far(nz)
            rs_near(nz)

        @pl.when(step == nz + 3)
        def _():
            finish(jnp.int32(0))
            ret_in[0, p_me] = ret_out[0, p_me]
            pass_on(nz)

        @pl.when(step >= nz)
        def _():
            take_back(step - (nz - 1))

    for j in (5, 6, 7):
        take_back(jnp.int32(j))

    columns_of = side[...].T
    at0, at1, weight0, weight1 = (columns_of[:, c : c + 1] for c in range(4))
    lanes = lax.broadcasted_iota(jnp.int32, (tok, nz * ROWS), 1).astype(F32)
    take = jnp.concatenate([one_hot(lanes == at0), one_hot(lanes == at1)], axis=0)
    block = min(512, width)
    blocks = [slice(c * block, (c + 1) * block) for c in range(width // block)]
    for columns in blocks:
        both[:, columns] = dot(take, ret_rows[:, :, columns].reshape(nz * ROWS, block))

    mix_ref[...] = rms_scale(rs_total(nz), mg_ref[...]).astype(BF)

    take_back(jnp.int32(0))
    square = jnp.zeros((tok, 1), F32)
    for columns in blocks:
        results = both[:, columns] + dot(take[:, :ROWS], ret_rows[0, :, columns])
        mixed = weight0 * results[:tok] + weight1 * results[tok:]
        combined[:, columns] = mixed
        square = square + jnp.sum(mixed * mixed, axis=1, keepdims=True)
    scale = lax.rsqrt(square / width + norm_eps)
    out_ref[...] = (combined[...] * scale * fg_ref[...]).astype(BF)

    for blocks, sems in ((outgoing, d_send), (ret_out, r_send)):
        wait_bytes(blocks.at[0, pl.ds(0, PL - 1)], sems.at[0])
        wait_bytes(blocks.at[pl.ds(1, nz - 1)], sems.at[1])
    wait_bytes(xall.at[:, pl.ds(0, 3)], ag_send.at[0])
    wait_bytes(part.at[:, pl.ds(0, 3)], rs_send.at[0])
    wait_bytes(kv.at[pl.ds(0, nz - 1), 0, 0], kz_send.at[0])
    wait_bytes(kv.at[:, 0, pl.ds(0, 3)], ky_send.at[0])
    wait_bytes(kv.at[:, 0], kc_send.at[0])


def permutation():
    source, piece, rank = np.meshgrid(
        np.arange(PL), np.arange(SUB), np.arange(CAP), indexing="ij"
    )
    travel = (source * SUB + piece) * CAP + rank
    rowwise = (piece * PL + source) * CAP + rank
    matrix = np.zeros((PL * ROWS, PL * ROWS), np.float32)
    matrix[rowwise.reshape(-1), travel.reshape(-1)] = 1.0
    return matrix


def turn_tables(rows):
    quarter = HEAD // 4
    inverse = rope_base ** (-np.arange(quarter, dtype=np.float64) / quarter)

    def table(count, make, at):
        angle = np.arange(count, dtype=np.float64)[:, None] * inverse[None, :]
        out = np.zeros((count, HEAD), np.float32)
        out[:, at : at + 2 * quarter] = make(angle)
        return jnp.asarray(out)

    def cosines(angle):
        return np.concatenate([np.cos(angle), np.cos(angle)], axis=1)

    def sines(angle):
        return np.concatenate([-np.sin(angle), np.sin(angle)], axis=1)

    return (
        table(rows, cosines, 0),
        table(rows, sines, 0),
        table(GRID_W, cosines, HEAD // 2),
        table(GRID_W, sines, HEAD // 2),
    )


def local(
    queries,
    keys,
    values,
    query_gain,
    key_gain,
    out_weight,
    mixer_gain,
    expert_in,
    routes,
    route_weights,
    expert_gain,
    gate_w,
    up_w,
    down_w,
    ffn_out_gain,
):
    nz = lax.axis_size("ep_0")
    assert nz == NZ
    tok, width = expert_in.shape
    ff = gate_w.shape[2]
    seq = queries.shape[0]
    tables = turn_tables(nz * PL * seq // GRID_W)
    matrix = permutation()
    pin = jnp.asarray(matrix, BF)
    pout = jnp.asarray(matrix.T, BF)
    hbm = pl.BlockSpec(memory_space=pltpu.HBM)
    vmem = pl.BlockSpec(memory_space=pltpu.VMEM)
    travel = (nz, PL, ROWS, width // SUB)
    dma = pltpu.SemaphoreType.DMA
    operands = (
        expert_in,
        routes.T,
        route_weights.T,
        expert_gain[None, :],
        ffn_out_gain[None, :],
        pin,
        pout,
        queries,
        keys,
        values,
        query_gain[None, :],
        key_gain[None, :],
        mixer_gain[None, :],
        *tables,
    )
    assert len(operands) == OPERANDS
    made = pl.pallas_call(
        functools.partial(layer_kernel, nz),
        out_shape=(
            pltpu.VMEM((seq // TP, width), BF),
            pltpu.VMEM((tok, width), BF),
        ),
        in_specs=[hbm] * (OPERANDS + 4),
        out_specs=(vmem, vmem),
        scratch_shapes=[pltpu.VMEM(a.shape, a.dtype) for a in operands]
        + [
            pltpu.VMEM((tok, width), BF),
            pltpu.VMEM(travel, BF),
            pltpu.VMEM(travel, BF),
            pltpu.VMEM((nz, 4, ROWS, width), BF),
            pltpu.VMEM((nz + 1, 4, ROWS, width), BF),
            pltpu.VMEM((nz + 1, 2, ROWS, width // 2), BF),
            pltpu.VMEM((nz + 1, 2, ROWS, width), BF),
            pltpu.VMEM(travel, BF),
            pltpu.VMEM(travel, BF),
            pltpu.VMEM((nz, ROWS, width), BF),
            pltpu.VMEM((width, 2 * ff), BF),
            pltpu.VMEM((ff, width), BF),
            pltpu.VMEM((tok, width), F32),
            pltpu.VMEM(out_weight.shape, BF),
            pltpu.VMEM((nz, 2, 4, 2, seq, HEAD), BF),
            pltpu.VMEM((8, tok), F32),
            pltpu.VMEM((2 * tok, width), F32),
            pltpu.VMEM((HEADS, seq, HEAD), BF),
            pltpu.VMEM((HEADS, seq, HEAD), F32),
            pltpu.VMEM((HEADS, seq, HEAD), F32),
            pltpu.VMEM((HEADS, seq, HEAD), F32),
            pltpu.VMEM((seq, HEADS * HEAD), BF),
            dma((4,)),
            dma((2,)),
            dma((nz,)),
            dma((1,)),
            dma((nz, 4)),
            dma((1,)),
            dma((nz + 1, 2)),
            dma((nz + 1, 4)),
            dma((2,)),
            dma((nz,)),
            dma((1,)),
            dma((nz, 2)),
            dma((1,)),
            dma((nz, 4)),
            dma((1,)),
            dma((nz,)),
            dma((OPERANDS,)),
        ],
        compiler_params=pltpu.CompilerParams(
            collective_id=0, has_side_effects=True, vmem_limit_bytes=58 * 2**20
        ),
        name="layer",
    )(
        *operands,
        gate_w,
        up_w,
        down_w,
        out_weight,
    )
    return made


def solution(mesh):
    split = Mesh(
        mesh.devices.reshape(mesh.shape["ep"] // 8, 4, 2, mesh.shape["tp"]),
        ("ep_0", "ep_1", "ep_2", "tp"),
    )
    return jax.shard_map(
        local,
        mesh=split,
        in_specs=(
            P(EP, "tp"),
            P(EP, "tp"),
            P(EP, "tp"),
            P(),
            P(),
            P("tp", None),
            P(),
            P(EP_TP, None),
            P(EP_TP, None),
            P(EP_TP, None),
            P(),
            P(EP, None, "tp"),
            P(EP, None, "tp"),
            P(EP, "tp", None),
            P(),
        ),
        out_specs=(P(EP_TP, None), P(EP_TP, None)),
        check_vma=False,
    )
```

```python
import functools

import jax
import jax.numpy as jnp
import numpy as np
from jax import lax
from jax.experimental import pallas as pl
from jax.experimental.pallas import tpu as pltpu
from jax.sharding import Mesh
from jax.sharding import PartitionSpec as P

HEAD = 128
HEADS = 4
GRID_W = 64
TP = 4
OPERANDS = 17
EP = ("ep_0", "ep_1", "ep_2")
EP_TP = ("ep_0", "ep_1", "ep_2", "tp")
MESH = pl.DeviceIdType.MESH
BF = jnp.bfloat16
F32 = jnp.float32

norm_eps = 1e-06
rope_base = 10000.0
clamp_limit = 7.0
sigmoid_slope = 1.702

PL = 8
CAP = 6
SUB = 8
ROWS = PL * CAP
AWAY = (0, 1, -2, 3, 4, -3, 2, -1)
NZ = len(AWAY)
FIRST = (1, 2, 3)
LATER = {0: (4,), 2: (5,), 3: (6, 7)}
INDEX = [[a % NZ for a in AWAY].index(d) for d in range(NZ)]
MIRROR = [INDEX[-a % NZ] for a in AWAY]


def rms_scale(values_in, gain):
    return (
        values_in
        * lax.rsqrt(jnp.mean(values_in * values_in, axis=-1, keepdims=True) + norm_eps)
        * gain
    )


def dot(a, b):
    return jnp.dot(a, b, preferred_element_type=F32)


def one_hot(cond):
    return jnp.where(cond, 1.0, 0.0).astype(BF)


def layer_kernel(nz, *refs):
    ours = refs[:OPERANDS]
    held = refs[OPERANDS + 6 : 2 * OPERANDS + 6]
    sems = refs[-1]
    copies = [
        pltpu.make_async_copy(src, dst, sems.at[i])
        for i, (src, dst) in enumerate(zip(ours, held))
    ]
    for copy in copies:
        copy.start()

    def operands_here():
        for copy in copies:
            copy.wait()

    layer(nz, operands_here, *held, *refs[OPERANDS : OPERANDS + 6], *refs[2 * OPERANDS + 6 : -1])


def layer(
    nz,
    operands_here,
    x_ref,
    routes_t_ref,
    rw_t_ref,
    eg_ref,
    fg_ref,
    pin_ref,
    pout_ref,
    q_ref,
    k_ref,
    v_ref,
    qg_ref,
    kg_ref,
    mg_ref,
    cos_row_ref,
    sin_row_ref,
    cos_col_ref,
    sin_col_ref,
    gate_hbm,
    up_hbm,
    down_hbm,
    ow_hbm,
    mix_ref,
    out_ref,
    normed,
    outgoing,
    arr,
    xall,
    part,
    rs1,
    rs2,
    ret_out,
    ret_in,
    ret_rows,
    wgu,
    wd,
    combined,
    ow,
    kv,
    side,
    both,
    q_s,
    m_s,
    l_s,
    acc_s,
    att_s,
    w_sem,
    d_send,
    d_recv,
    ag_send,
    ag_recv,
    rs_send,
    rs1_recv,
    rs2_recv,
    r_send,
    r_recv,
    kz_send,
    kz_recv,
    ky_send,
    ky_recv,
    kc_send,
    kc_recv,
):
    z = lax.axis_index("ep_0")
    p_me = lax.axis_index("ep_1") * 2 + lax.axis_index("ep_2")
    x_me = lax.axis_index("tp")
    right = {"tp": lax.rem(x_me + 1, 4)}
    left = {"tp": lax.rem(x_me + 3, 4)}
    y_me = lax.axis_index("ep_1")
    y_up = {"ep_1": lax.rem(y_me + 1, 4)}
    y_down = {"ep_1": lax.rem(y_me + 3, 4)}
    other_core = {"ep_2": 1 - lax.axis_index("ep_2")}
    tok, width = x_ref.shape
    half = width // 2
    sub_w = width // SUB
    ff = wd.shape[0]
    n_exp = nz * PL

    def peer(zz, p):
        return {"ep_0": zz, "ep_1": lax.div(p, 2), "ep_2": lax.rem(p, 2)}

    def entry(values, i):
        found = jnp.full(jnp.shape(i), values[0], jnp.int32)
        for j in range(1, nz):
            found = jnp.where(i == j, values[j], found)
        return found

    def plane(i):
        return lax.rem(z + entry([a % nz for a in AWAY], i), nz)

    def mirror(i):
        return entry(MIRROR, i)

    barrier = pltpu.get_barrier_semaphore()

    def greet(device):
        pl.semaphore_signal(barrier, inc=1, device_id=device, device_id_type=MESH)

    greet(left)
    greet(right)
    for j in range(1, PL):
        greet(peer(z, lax.rem(p_me + j, PL)))

    @pl.loop(1, nz)
    def _(d):
        zz = lax.rem(z + d, nz)
        for j in range(PL):
            greet(peer(zz, lax.rem(p_me + j, PL)))

    w_copies = [
        pltpu.make_async_copy(gate_hbm.at[0], wgu.at[:, pl.ds(0, ff)], w_sem.at[0]),
        pltpu.make_async_copy(up_hbm.at[0], wgu.at[:, pl.ds(ff, ff)], w_sem.at[1]),
        pltpu.make_async_copy(down_hbm.at[0], wd, w_sem.at[2]),
        pltpu.make_async_copy(ow_hbm, ow, w_sem.at[3]),
    ]
    for copy in w_copies:
        copy.start()

    operands_here()
    xf = x_ref[...].astype(F32)
    normed[...] = rms_scale(xf, eg_ref[...]).astype(BF)

    def base_of(e):
        o = (lax.shift_right_logical(e, 3) - z + nz) & (nz - 1)
        return entry(INDEX, o) * ROWS + (e & 7) * CAP

    e_rows = lax.broadcasted_iota(jnp.int32, (n_exp, tok), 0)
    t_a = lax.broadcasted_iota(jnp.int32, (tok, tok), 0)
    t_b = lax.broadcasted_iota(jnp.int32, (tok, tok), 1)
    before_t = one_hot(t_a < t_b)
    oh0 = e_rows == routes_t_ref[0:1, :]
    oh1 = e_rows == routes_t_ref[1:2, :]
    rank0 = dot(one_hot(oh0), before_t)
    rank1 = dot(one_hot(oh1), before_t) + jnp.sum(
        jnp.where(oh0, 1.0, 0.0), axis=1, keepdims=True
    )
    base = base_of(e_rows).astype(F32)
    place0 = jnp.sum(jnp.where(oh0, base + rank0, 0.0), axis=0, keepdims=True)
    place1 = jnp.sum(jnp.where(oh1, base + rank1, 0.0), axis=0, keepdims=True)
    slots = lax.broadcasted_iota(jnp.int32, (nz * ROWS, tok), 0).astype(F32)
    pick = one_hot((slots == place0) | (slots == place1))
    side[...] = jnp.concatenate(
        [place0, place1, rw_t_ref[...], jnp.zeros((4, tok), F32)], axis=0
    )

    def stack_pieces(rows):
        return jnp.concatenate(
            [rows[:, q * sub_w : (q + 1) * sub_w] for q in range(SUB)], axis=0
        )

    def join_pieces(stacked):
        return jnp.concatenate(
            [stacked[q * ROWS : (q + 1) * ROWS, :] for q in range(SUB)], axis=1
        )

    def to_blocks(rows):
        blocks = dot(pout_ref[...], stack_pieces(rows)).astype(BF)
        return blocks.reshape(PL, ROWS, sub_w)

    def to_rows(blocks):
        flat = blocks.reshape(PL * ROWS, sub_w)
        return join_pieces(dot(pin_ref[...], flat).astype(BF))

    def dispatch(i, p):
        return pltpu.make_async_remote_copy(
            src_ref=outgoing.at[i, p],
            dst_ref=arr.at[mirror(i), p_me],
            send_sem=d_send.at[jnp.minimum(i, 1)],
            recv_sem=d_recv.at[mirror(i)],
            device_id=peer(plane(i), p),
            device_id_type=MESH,
        )

    def give_back(i, p):
        return pltpu.make_async_remote_copy(
            src_ref=ret_out.at[i, p],
            dst_ref=ret_in.at[mirror(i), p_me],
            send_sem=r_send.at[jnp.minimum(i, 1)],
            recv_sem=r_recv.at[mirror(i)],
            device_id=peer(plane(i), p),
            device_id_type=MESH,
        )

    def x_copy(src, dst, send, recv, to):
        return pltpu.make_async_remote_copy(
            src_ref=src, dst_ref=dst, send_sem=send, recv_sem=recv, device_id=to,
            device_id_type=MESH,
        )

    z_up = {"ep_0": lax.rem(z + 1, nz)}
    z_down = {"ep_0": lax.rem(z + nz - 1, nz)}

    def kv_z_up(k, to):
        return x_copy(kv.at[k, 0, 0], kv.at[to, 0, 0], kz_send.at[0], kz_recv.at[to, 0], z_up)

    def kv_z_down(k, to):
        return x_copy(
            kv.at[k, 0, 0], kv.at[to, 0, 0], kz_send.at[0], kz_recv.at[to, 0], z_down
        )

    last = nz - 1
    k_z_far = x_copy(
        kv.at[last - 2, 0, 0, 0], kv.at[last, 0, 0, 0], kz_send.at[0], kz_recv.at[last, 0],
        z_up,
    )
    v_z_far = x_copy(
        kv.at[last - 1, 0, 0, 1], kv.at[last, 0, 0, 1], kz_send.at[0], kz_recv.at[last, 1],
        z_down,
    )

    def each_plane(group, act):
        act(jnp.maximum(2 * group - 1, 0))

        @pl.when((group >= 1) & (group < nz // 2))
        def _():
            act(2 * group)

    def kv_up(k):
        return x_copy(kv.at[k, 0, 0], kv.at[k, 0, 1], ky_send.at[0], ky_recv.at[k, 0], y_up)

    def kv_down(k):
        return x_copy(kv.at[k, 0, 0], kv.at[k, 0, 2], ky_send.at[0], ky_recv.at[k, 1], y_down)

    def k_far(k):
        return x_copy(
            kv.at[k, 0, 1, 0], kv.at[k, 0, 3, 0], ky_send.at[0], ky_recv.at[k, 2], y_up
        )

    def v_far(k):
        return x_copy(
            kv.at[k, 0, 2, 1], kv.at[k, 0, 3, 1], ky_send.at[0], ky_recv.at[k, 3], y_down
        )

    def kv_across(k):
        return x_copy(kv.at[k, 0], kv.at[k, 1], kc_send.at[0], kc_recv.at[k], other_core)

    def attend(k):
        keys = kv[k, :, :, 0].reshape(-1, HEAD)
        vals = kv[k, :, :, 1].reshape(-1, HEAD)

        @pl.loop(0, HEADS)
        def _(h):
            scores = lax.dot_general(
                q_s[h], keys, (((1,), (1,)), ((), ())), preferred_element_type=F32
            ) * HEAD ** (-0.5)
            peak = jnp.maximum(m_s[h], jnp.max(scores, axis=1, keepdims=True))
            fade = jnp.exp(m_s[h] - peak)
            expo = jnp.exp(scores - peak[:, :1])
            m_s[h] = peak
            sums = l_s[h] * fade
            for c in range(expo.shape[1] // HEAD):
                sums = sums + expo[:, c * HEAD : (c + 1) * HEAD]
            l_s[h] = sums
            acc_s[h] = acc_s[h] * fade + dot(expo.astype(BF), vals)

    def project():
        for h in range(HEADS):
            total = jnp.sum(l_s[h], axis=1, keepdims=True)
            att_s[:, h * HEAD : (h + 1) * HEAD] = (acc_s[h] / total).astype(BF)
        share = att_s.shape[0] // TP
        ours = jnp.concatenate(
            [
                att_s[pl.ds(pl.multiple_of(lax.rem(x_me + o, TP) * share, share), share), :]
                for o in (0, 3, 1, 2)
            ],
            axis=0,
        )
        return dot(ours, ow[...]).astype(BF).reshape(TP, share, width)

    def to_plane(i, make):
        @pl.when(i == 0)
        def _():
            @pl.loop(1, PL)
            def _(j):
                make(i, lax.rem(p_me + j, PL)).start()

        @pl.when(i > 0)
        def _():
            @pl.loop(0, PL)
            def _(j):
                make(i, lax.rem(p_me + j, PL)).start()

    def wait_bytes(ref, sem):
        pltpu.make_async_copy(ref, ref, sem).wait()

    def wait_plane(i, ref, sem):
        @pl.when(i == 0)
        def _():
            wait_bytes(ref.at[0, pl.ds(0, PL - 1)], sem.at[0])

        @pl.when(i > 0)
        def _():
            wait_bytes(ref.at[i], sem.at[i])

    def gather(i):
        rows = dot(pick[i * ROWS : (i + 1) * ROWS, :], normed[...]).astype(BF)
        outgoing[i] = to_blocks(rows)

    gather(0)
    pl.semaphore_wait(barrier, n_exp - 1 + 2)
    to_plane(jnp.int32(0), dispatch)
    arr[0, p_me] = outgoing[0, p_me]

    for c in FIRST:
        gather(MIRROR[c])
        to_plane(jnp.int32(MIRROR[c]), dispatch)

    grid_rows = k_ref.shape[0] // GRID_W
    first_row = (z * PL + p_me) * grid_rows
    cosine = jnp.concatenate(
        [cos_row_ref[pl.ds(first_row + g, 1), :] + cos_col_ref[...] for g in range(grid_rows)],
        axis=0,
    )
    sine = jnp.concatenate(
        [sin_row_ref[pl.ds(first_row + g, 1), :] + sin_col_ref[...] for g in range(grid_rows)],
        axis=0,
    )
    lane = lax.broadcasted_iota(jnp.int32, cosine.shape, 1)
    first_of_pair = (lane & 32) == 0

    def normed_and_turned(head, gain):
        field = rms_scale(head.astype(F32), gain)
        swapped = jnp.where(
            first_of_pair, pltpu.roll(field, HEAD - 32, 1), pltpu.roll(field, 32, 1)
        )
        return (field * cosine + swapped * sine).astype(BF)

    kv[0, 0, 0, 0] = normed_and_turned(k_ref[...], kg_ref[...])
    kv[0, 0, 0, 1] = v_ref[...]
    kv_z_up(0, 1).start()
    kv_z_down(0, 2).start()
    kv_up(0).start()
    kv_down(0).start()

    for c in range(1, nz):
        if c not in FIRST:
            gather(MIRROR[c])

    for h in range(HEADS):
        q_s[h] = normed_and_turned(q_ref[:, h * HEAD : (h + 1) * HEAD], qg_ref[...])
    ret_rows[0] = jnp.zeros(ret_rows.shape[1:], BF)
    m_s[...] = jnp.full(m_s.shape, -1e30, F32)
    l_s[...] = jnp.zeros(l_s.shape, F32)
    acc_s[...] = jnp.zeros(acc_s.shape, F32)

    cols_a, cols_b = pl.ds(0, half), pl.ds(half, half)

    def ag_right(k):
        return x_copy(xall.at[k, 0], xall.at[k, 1], ag_send.at[0], ag_recv.at[k, 0], right)

    def ag_left(k):
        return x_copy(xall.at[k, 0], xall.at[k, 2], ag_send.at[0], ag_recv.at[k, 1], left)

    def fwd_right(k):
        return x_copy(
            xall.at[k, 1, :, cols_a], xall.at[k, 3, :, cols_a],
            ag_send.at[0], ag_recv.at[k, 2], right,
        )

    def fwd_left(k):
        return x_copy(
            xall.at[k, 2, :, cols_b], xall.at[k, 3, :, cols_b],
            ag_send.at[0], ag_recv.at[k, 3], left,
        )

    def rs_far_left(k):
        return x_copy(
            part.at[k, 3, :, cols_a], rs1.at[k, 0], rs_send.at[0], rs1_recv.at[k, 0], left
        )

    def rs_far_right(k):
        return x_copy(
            part.at[k, 3, :, cols_b], rs1.at[k, 1], rs_send.at[0], rs1_recv.at[k, 1], right
        )

    def rs_near_left(k, c, s):
        return x_copy(
            part.at[k, 1, :, c], rs2.at[k, 1, :, c], rs_send.at[0], rs2_recv.at[k, s - 2], left
        )

    def rs_near_right(k, c, s):
        return x_copy(
            part.at[k, 2, :, c], rs2.at[k, 0, :, c], rs_send.at[0], rs2_recv.at[k, s - 2], right
        )

    def rs_copies(k):
        return (
            rs_far_left(k),
            rs_far_right(k),
            rs_near_left(k, cols_a, 2),
            rs_near_left(k, cols_b, 3),
            rs_near_right(k, cols_a, 4),
            rs_near_right(k, cols_b, 5),
        )

    def rs_far(k):
        rs_far_left(k).start()
        rs_far_right(k).start()

    def rs_near(k):
        rs_near_left(k, cols_b, 3).start()
        rs_near_right(k, cols_a, 4).start()

    def rs_total(k):
        for copy in rs_copies(k)[2:]:
            copy.wait_recv()
        return part[k, 0].astype(F32) + rs2[k, 0].astype(F32) + rs2[k, 1].astype(F32)

    def experts(k):
        fwd_right(k).wait_recv()
        fwd_left(k).wait_recv()

        rows = xall[k].reshape(4 * ROWS, width)
        pre = dot(rows, wgu[...])
        gate_cut = jnp.minimum(pre[:, :ff], clamp_limit)
        up_cut = jnp.clip(pre[:, ff:], -clamp_limit, clamp_limit)
        hidden = (
            (up_cut + 1.0) * gate_cut * (1.0 / (1.0 + jnp.exp(-sigmoid_slope * gate_cut)))
        ).astype(BF)
        part[k] = dot(hidden, wd[...]).astype(BF).reshape(4, ROWS, width)
        rs_far(k)

    def pass_on(k):
        rs_far_left(k).wait_recv()
        part[k, 1, :, cols_a] = (
            part[k, 1, :, cols_a].astype(F32) + rs1[k, 0].astype(F32)
        ).astype(BF)
        rs_near_left(k, cols_a, 2).start()
        rs_far_right(k).wait_recv()
        part[k, 2, :, cols_b] = (
            part[k, 2, :, cols_b].astype(F32) + rs1[k, 1].astype(F32)
        ).astype(BF)
        rs_near_right(k, cols_b, 5).start()

    def finish(k):
        ret_out[k] = to_blocks(rs_total(k).astype(BF))
        to_plane(k, give_back)

    def take_back(j):
        kk = mirror(j)
        wait_plane(kk, ret_in, r_recv)
        ret_rows[kk] = to_rows(ret_in[kk])

    @pl.loop(0, nz + 4)
    def _(step):
        @pl.when(step < nz)
        def _():
            k = step
            wait_plane(k, arr, d_recv)
            xall[k, 0] = to_rows(arr[k])
            ag_right(k).start()
            ag_left(k).start()
        @pl.when((step >= 1) & (step < nz + 1))
        def _():
            k = step - 1
            ag_right(k).wait_recv()
            fwd_right(k).start()
            ag_left(k).wait_recv()
            fwd_left(k).start()

        @pl.when(step == 2)
        def _():
            for copy in w_copies:
                copy.wait()

        @pl.when((step >= 3) & (step < nz + 2))
        def _():
            experts(step - 2)

        @pl.when((step >= 4) & (step < nz + 3))
        def _():
            pass_on(step - 3)

        @pl.when((step >= 3) & (step < nz + 2))
        def _():
            rs_near(step - 2)

        @pl.when(step == nz + 1)
        def _():
            experts(0)

        @pl.when(step == nz + 2)
        def _():
            rs_near(0)

        @pl.when((step >= 2) & (step <= nz // 2))
        def _():
            below, above = 2 * step - 3, 2 * step - 2
            kv_z_up(0, below).wait_recv()
            kv_z_down(0, above).wait_recv()

            @pl.when(step < nz // 2)
            def _():
                kv_z_up(below, below + 2).start()
                kv_z_down(above, above + 2).start()

            @pl.when(step == nz // 2)
            def _():
                k_z_far.start()
                v_z_far.start()

            for j in (below, above):
                kv_up(j).start()
                kv_down(j).start()

        @pl.when(step == nz // 2 + 1)
        def _():
            k_z_far.wait_recv()
            v_z_far.wait_recv()
            kv_up(last).start()
            kv_down(last).start()

        for at, chunks in LATER.items():

            @pl.when(step == at)
            def _(chunks=chunks):
                for i in chunks:
                    to_plane(jnp.int32(MIRROR[i]), dispatch)

        @pl.when((step >= 2) & (step <= nz // 2 + 2))
        def _():
            def forward(j):
                kv_up(j).wait_recv()
                k_far(j).start()
                kv_down(j).wait_recv()
                v_far(j).start()

            each_plane(step - 2, forward)

        @pl.when((step >= 3) & (step <= nz // 2 + 3))
        def _():
            def across(j):
                k_far(j).wait_recv()
                v_far(j).wait_recv()
                kv_across(j).start()

            each_plane(step - 3, across)

        @pl.when((step >= 4) & (step <= nz // 2 + 4))
        def _():
            def attend_to(j):
                kv_across(j).wait_recv()
                attend(j)

            each_plane(step - 4, attend_to)

        @pl.when(step >= 5)
        def _():
            finish(step - 4)

        @pl.when(step == nz)
        def _():
            part[nz] = project()

        @pl.when(step == nz + 2)
        def _():
            pass_on(0)
            rs_far(nz)
            rs_near(nz)

        @pl.when(step == nz + 3)
        def _():
            finish(jnp.int32(0))
            ret_in[0, p_me] = ret_out[0, p_me]
            pass_on(nz)

        @pl.when(step >= nz)
        def _():
            take_back(step - (nz - 1))

    for j in (5, 6, 7):
        take_back(jnp.int32(j))

    columns_of = side[...].T
    at0, at1, weight0, weight1 = (columns_of[:, c : c + 1] for c in range(4))
    lanes = lax.broadcasted_iota(jnp.int32, (tok, nz * ROWS), 1).astype(F32)
    take = jnp.concatenate([one_hot(lanes == at0), one_hot(lanes == at1)], axis=0)
    block = min(512, width)
    blocks = [slice(c * block, (c + 1) * block) for c in range(width // block)]
    for columns in blocks:
        both[:, columns] = dot(take, ret_rows[:, :, columns].reshape(nz * ROWS, block))

    mix_ref[...] = rms_scale(rs_total(nz), mg_ref[...]).astype(BF)

    take_back(jnp.int32(0))
    square = jnp.zeros((tok, 1), F32)
    for columns in blocks:
        results = both[:, columns] + dot(take[:, :ROWS], ret_rows[0, :, columns])
        mixed = weight0 * results[:tok] + weight1 * results[tok:]
        combined[:, columns] = mixed
        square = square + jnp.sum(mixed * mixed, axis=1, keepdims=True)
    scale = lax.rsqrt(square / width + norm_eps)
    out_ref[...] = (combined[...] * scale * fg_ref[...]).astype(BF)

    for blocks, sems in ((outgoing, d_send), (ret_out, r_send)):
        wait_bytes(blocks.at[0, pl.ds(0, PL - 1)], sems.at[0])
        wait_bytes(blocks.at[pl.ds(1, nz - 1)], sems.at[1])
    wait_bytes(xall.at[:, pl.ds(0, 3)], ag_send.at[0])
    wait_bytes(part.at[:, pl.ds(0, 3)], rs_send.at[0])
    wait_bytes(kv.at[pl.ds(0, nz - 1), 0, 0], kz_send.at[0])
    wait_bytes(kv.at[:, 0, pl.ds(0, 3)], ky_send.at[0])
    wait_bytes(kv.at[:, 0], kc_send.at[0])


def permutation():
    source, piece, rank = np.meshgrid(
        np.arange(PL), np.arange(SUB), np.arange(CAP), indexing="ij"
    )
    travel = (source * SUB + piece) * CAP + rank
    rowwise = (piece * PL + source) * CAP + rank
    matrix = np.zeros((PL * ROWS, PL * ROWS), np.float32)
    matrix[rowwise.reshape(-1), travel.reshape(-1)] = 1.0
    return matrix


def turn_tables(rows):
    quarter = HEAD // 4
    inverse = rope_base ** (-np.arange(quarter, dtype=np.float64) / quarter)

    def table(count, make, at):
        angle = np.arange(count, dtype=np.float64)[:, None] * inverse[None, :]
        out = np.zeros((count, HEAD), np.float32)
        out[:, at : at + 2 * quarter] = make(angle)
        return jnp.asarray(out)

    def cosines(angle):
        return np.concatenate([np.cos(angle), np.cos(angle)], axis=1)

    def sines(angle):
        return np.concatenate([-np.sin(angle), np.sin(angle)], axis=1)

    return (
        table(rows, cosines, 0),
        table(rows, sines, 0),
        table(GRID_W, cosines, HEAD // 2),
        table(GRID_W, sines, HEAD // 2),
    )


def local(
    queries,
    keys,
    values,
    query_gain,
    key_gain,
    out_weight,
    mixer_gain,
    expert_in,
    routes,
    route_weights,
    expert_gain,
    gate_w,
    up_w,
    down_w,
    ffn_out_gain,
):
    nz = lax.axis_size("ep_0")
    assert nz == NZ
    tok, width = expert_in.shape
    ff = gate_w.shape[2]
    seq = queries.shape[0]
    tables = turn_tables(nz * PL * seq // GRID_W)
    matrix = permutation()
    pin = jnp.asarray(matrix, BF)
    pout = jnp.asarray(matrix.T, BF)
    hbm = pl.BlockSpec(memory_space=pltpu.HBM)
    vmem = pl.BlockSpec(memory_space=pltpu.VMEM)
    travel = (nz, PL, ROWS, width // SUB)
    dma = pltpu.SemaphoreType.DMA
    operands = (
        expert_in,
        routes.T,
        route_weights.T,
        expert_gain[None, :],
        ffn_out_gain[None, :],
        pin,
        pout,
        queries,
        keys,
        values,
        query_gain[None, :],
        key_gain[None, :],
        mixer_gain[None, :],
        *tables,
    )
    assert len(operands) == OPERANDS
    made = pl.pallas_call(
        functools.partial(layer_kernel, nz),
        out_shape=(
            pltpu.VMEM((seq // TP, width), BF),
            pltpu.VMEM((tok, width), BF),
        ),
        in_specs=[hbm] * (OPERANDS + 4),
        out_specs=(vmem, vmem),
        scratch_shapes=[pltpu.VMEM(a.shape, a.dtype) for a in operands]
        + [
            pltpu.VMEM((tok, width), BF),
            pltpu.VMEM(travel, BF),
            pltpu.VMEM(travel, BF),
            pltpu.VMEM((nz, 4, ROWS, width), BF),
            pltpu.VMEM((nz + 1, 4, ROWS, width), BF),
            pltpu.VMEM((nz + 1, 2, ROWS, width // 2), BF),
            pltpu.VMEM((nz + 1, 2, ROWS, width), BF),
            pltpu.VMEM(travel, BF),
            pltpu.VMEM(travel, BF),
            pltpu.VMEM((nz, ROWS, width), BF),
            pltpu.VMEM((width, 2 * ff), BF),
            pltpu.VMEM((ff, width), BF),
            pltpu.VMEM((tok, width), F32),
            pltpu.VMEM(out_weight.shape, BF),
            pltpu.VMEM((nz, 2, 4, 2, seq, HEAD), BF),
            pltpu.VMEM((8, tok), F32),
            pltpu.VMEM((2 * tok, width), F32),
            pltpu.VMEM((HEADS, seq, HEAD), BF),
            pltpu.VMEM((HEADS, seq, HEAD), F32),
            pltpu.VMEM((HEADS, seq, HEAD), F32),
            pltpu.VMEM((HEADS, seq, HEAD), F32),
            pltpu.VMEM((seq, HEADS * HEAD), BF),
            dma((4,)),
            dma((2,)),
            dma((nz,)),
            dma((1,)),
            dma((nz, 4)),
            dma((1,)),
            dma((nz + 1, 2)),
            dma((nz + 1, 4)),
            dma((2,)),
            dma((nz,)),
            dma((1,)),
            dma((nz, 2)),
            dma((1,)),
            dma((nz, 4)),
            dma((1,)),
            dma((nz,)),
            dma((OPERANDS,)),
        ],
        compiler_params=pltpu.CompilerParams(
            collective_id=0, has_side_effects=True, vmem_limit_bytes=58 * 2**20
        ),
        name="layer",
    )(
        *operands,
        gate_w,
        up_w,
        down_w,
        out_weight,
    )
    return made


def solution(mesh):
    split = Mesh(
        mesh.devices.reshape(mesh.shape["ep"] // 8, 4, 2, mesh.shape["tp"]),
        ("ep_0", "ep_1", "ep_2", "tp"),
    )
    return jax.shard_map(
        local,
        mesh=split,
        in_specs=(
            P(EP, "tp"),
            P(EP, "tp"),
            P(EP, "tp"),
            P(),
            P(),
            P("tp", None),
            P(),
            P(EP_TP, None),
            P(EP_TP, None),
            P(EP_TP, None),
            P(),
            P(EP, None, "tp"),
            P(EP, None, "tp"),
            P(EP, "tp", None),
            P(),
        ),
        out_specs=(P(EP_TP, None), P(EP_TP, None)),
        check_vma=False,
    )
```
